32 devices in a mesh: sp: 8 (over z, y), tp: 4 (over x, core).
Axes of the slice: x: 2, y: 2, z: 4, core: 2. Of those that a mesh axis runs over, the one named last changes fastest.
Arguments:
- latent: bfloat16 [2048, 2048], P('sp'), may hold values from -6 to 6
- context: bfloat16 [512, 2048], P('sp'), may hold values from -6 to 6
- condition: float32 [2048], P('sp'), may hold values from -6 to 6
- ctx_condition: float32 [2048], P('sp'), may hold values from -6 to 6
- shift_weight: bfloat16 [2048, 2048], P('sp', 'tp'), may hold values from -0.125 to 0.125
- scale_weight: bfloat16 [2048, 2048], P('sp', 'tp'), may hold values from -0.125 to 0.125
- gate_weight: bfloat16 [2048, 2048], P('sp', 'tp'), may hold values from -0.125 to 0.125
- norm_gain: float32 [2048], replicated, may hold values from 0.1 to 1.9
- query_weight: bfloat16 [2048, 1024], P(None, 'tp'), may hold values from -0.125 to 0.125
- key_weight: bfloat16 [2048, 1024], P(None, 'tp'), may hold values from -0.125 to 0.125
- value_weight: bfloat16 [2048, 1024], P(None, 'tp'), may hold values from -0.125 to 0.125
- query_gain: float32 [64], replicated, may hold values from 0.6 to 6.5
- key_gain: float32 [64], replicated, may hold values from 0.6 to 6.5
- offset_bias: float32 [16, 15, 31], P('tp'), may hold values from 1 to 3
- out_weight: bfloat16 [1024, 2048], P('tp'), may hold values from -0.75 to 0.75
Outputs:
- mixed_rows: bfloat16 [2048, 2048], P('sp')
The draws below stay inside these ranges and needn't reach their ends.
All inputs are finite; a program needn't handle non-finite values.
Results may differ from the reference program's by a relative error of at most 0.01405.
The reference program's roundings to bfloat16 on the way count: a program that leaves them out, or rounds other values in their place, can miss the bound.
Values may be sent and summed in bfloat16 or wider, within the bound.
A program may use at most 64 MiB of HBM per device.

```python
import jax
import jax.numpy as jnp
from jax import lax

D = 2048
HEADS = 16
HEAD_DIM = 64
GRID_W = 64
WIN_ROWS = 8
WIN_COLS = 16
CTX = 512
TOKENS = 2048
ATT_W = 1024
N_TP = 4


def gain_draw(base_key):
    return jax.random.uniform(base_key, (HEAD_DIM,), jnp.float32, 0.6, 2.0)


def draw_query_gain(key, part):
    return gain_draw(jax.random.fold_in(key, 11))


def draw_key_gain(key, part):
    return gain_draw(jax.random.fold_in(key, 23))


def level_of(stream_key, dims, cuts, smallest, largest):
    gain = 1.0
    for dim, shards_of in cuts:
        heights = jax.random.uniform(jax.random.fold_in(jax.random.fold_in(stream_key, 6), dim), (shards_of,), jnp.float32, smallest / len(cuts), largest / len(cuts))
        gain = gain * jnp.repeat(jnp.exp(heights), dims[dim] // shards_of).reshape((-1,) + (1,) * (len(dims) - 1 - dim))
    return gain


def gaussian(rng, extent, width, most, cuts=(), kind=jnp.bfloat16):
    values = width * jax.random.normal(rng, extent, jnp.float32)
    if cuts:
        values = values * level_of(rng, extent, cuts, -0.22, 0.18)
    return jnp.clip(values, -most, most).astype(kind)


def setup_inputs(seed: int = 0) -> dict:
    streams_of = jax.random.split(jax.random.key(seed), 16)
    latent = gaussian(streams_of[0], (TOKENS, D), 1.0, 6.0, ((0, 8),))
    context = gaussian(streams_of[1], (CTX, D), 1.0, 6.0, ((0, 8),))
    condition = gaussian(streams_of[2], (D,), 1.0, 6.0, ((0, 8),), jnp.float32)
    ctx_condition = gaussian(streams_of[3], (D,), 1.0, 6.0, ((0, 8),), jnp.float32)
    shift_weight = gaussian(streams_of[4], (D, D), D ** -0.5, 0.125, ((0, 8), (1, 4)))
    scale_weight = gaussian(streams_of[5], (D, D), D ** -0.5, 0.125, ((0, 8), (1, 4)))
    gate_weight = gaussian(streams_of[6], (D, D), D ** -0.5, 0.125, ((0, 8), (1, 4)))
    norm_gain = jnp.clip(1.0 + 0.18 * jax.random.normal(streams_of[7], (D,), jnp.float32), 0.1, 1.9)
    query_weight = gaussian(streams_of[8], (D, ATT_W), D ** -0.5, 0.125, ((1, 4),))
    key_weight = gaussian(streams_of[9], (D, ATT_W), D ** -0.5, 0.125, ((1, 4),))
    value_weight = gaussian(streams_of[10], (D, ATT_W), D ** -0.5, 0.125, ((1, 4),))
    query_gain = draw_query_gain(jax.random.fold_in(streams_of[15], 71), 0)
    key_gain = draw_key_gain(jax.random.fold_in(streams_of[15], 71), 0)
    offset_bias = jnp.clip(1.0 + 2.0 * jax.random.uniform(streams_of[13], (HEADS, 2 * WIN_ROWS - 1, 2 * WIN_COLS - 1), jnp.float32) ** level_of(streams_of[13], (HEADS, 2 * WIN_ROWS - 1, 2 * WIN_COLS - 1), ((0, 4),), -0.2, 0.2), 1.0, 3.0)
    out_weight = gaussian(streams_of[14], (ATT_W, D), (ATT_W // 16) ** -0.5, 0.75, ((0, 4),))
    return dict(latent=latent, context=context, condition=condition, ctx_condition=ctx_condition, shift_weight=shift_weight, scale_weight=scale_weight, gate_weight=gate_weight, norm_gain=norm_gain, query_weight=query_weight, key_weight=key_weight, value_weight=value_weight, query_gain=query_gain, key_gain=key_gain, offset_bias=offset_bias, out_weight=out_weight)


EPS = 1e-06

def modulate(rows_in, norm_gain, shift_vec, scale_vec):
    values = rows_in.astype(jnp.float32)
    normed = values * lax.rsqrt(lax.optimization_barrier(jnp.mean(values * values, axis=-1, keepdims=True)) + EPS)
    return (normed * norm_gain * (1.0 + scale_vec) + shift_vec).astype(jnp.bfloat16)

def head_norm(projected, head_gain):
    row_count = projected.shape[0]
    split_heads = projected.reshape(row_count, -1, head_gain.shape[0])
    normed = split_heads * lax.rsqrt(lax.optimization_barrier(jnp.mean(split_heads * split_heads, axis=-1, keepdims=True)) + EPS)
    return (normed * head_gain).astype(jnp.bfloat16).reshape(row_count, -1)

def per_head(matrix, row_count):
    return matrix.reshape(row_count, HEADS, HEAD_DIM).transpose(1, 0, 2)

def reference(latent, context, condition, ctx_condition, shift_weight, scale_weight, gate_weight, norm_gain, query_weight, key_weight, value_weight, query_gain, key_gain, offset_bias, out_weight):
    activations = jax.nn.silu(jnp.stack([condition, ctx_condition])).astype(jnp.bfloat16)
    shift_vec = jnp.dot(activations, shift_weight, preferred_element_type=jnp.float32)
    scale_vec = jnp.dot(activations, scale_weight, preferred_element_type=jnp.float32)
    gate_vec = jnp.dot(activations[:1], gate_weight, preferred_element_type=jnp.float32)
    hidden = modulate(latent, norm_gain, shift_vec[0], scale_vec[0])
    ctx_hidden = modulate(context, norm_gain, shift_vec[1], scale_vec[1])
    queries = head_norm(jnp.dot(hidden, query_weight, preferred_element_type=jnp.float32), query_gain)
    keys_lat = head_norm(jnp.dot(hidden, key_weight, preferred_element_type=jnp.float32), key_gain)
    values_lat = jnp.dot(hidden, value_weight, preferred_element_type=jnp.float32).astype(jnp.bfloat16)
    ctx_keys = head_norm(jnp.dot(ctx_hidden, key_weight, preferred_element_type=jnp.float32), key_gain)
    ctx_values = jnp.dot(ctx_hidden, value_weight, preferred_element_type=jnp.float32).astype(jnp.bfloat16)
    grid_rows = TOKENS // GRID_W
    score_scale = HEAD_DIM ** (-0.5)
    row_ids = jnp.arange(grid_rows, dtype=jnp.int32)
    band_start = jnp.clip(row_ids - WIN_ROWS // 2, 0, grid_rows - WIN_ROWS)
    band_rows = band_start[:, None] + jnp.arange(WIN_ROWS, dtype=jnp.int32)[None, :]
    row_steps = band_rows - row_ids[:, None] + WIN_ROWS - 1
    column_ids = jnp.arange(GRID_W, dtype=jnp.int32)
    col_start = jnp.clip(column_ids - WIN_COLS // 2, 0, GRID_W - WIN_COLS)
    col_open = (column_ids[None, :] >= col_start[:, None]) & (column_ids[None, :] < col_start[:, None] + WIN_COLS)
    col_steps = jnp.clip(column_ids[None, :] - column_ids[:, None], 1 - WIN_COLS, WIN_COLS - 1) + WIN_COLS - 1

    def one_head(operands):
        q_head, k_head, v_head, kc_head, vc_head, table = operands
        q_grid = q_head.reshape(grid_rows, GRID_W, HEAD_DIM).astype(jnp.float32)
        k_grid = k_head.reshape(grid_rows, GRID_W, HEAD_DIM).astype(jnp.float32)
        v_grid = v_head.reshape(grid_rows, GRID_W, HEAD_DIM).astype(jnp.float32)
        k_band = k_grid[band_rows]
        v_band = v_grid[band_rows]
        offsets = table[row_steps[:, None, :, None], col_steps[None, :, None, :]]
        local_scores = jnp.einsum('rqd,rjkd->rqjk', q_grid, k_band) * score_scale + offsets
        local_scores = jnp.where(col_open[None, :, None, :], local_scores, -jnp.inf)
        ctx_scores = jnp.einsum('rqd,nd->rqn', q_grid, kc_head.astype(jnp.float32)) * score_scale
        row_max = jnp.maximum(lax.optimization_barrier(jnp.max(local_scores, axis=(2, 3))), lax.optimization_barrier(jnp.max(ctx_scores, axis=2)))
        local_exp = jnp.exp(local_scores - row_max[..., None, None])
        ctx_exp = jnp.exp(ctx_scores - row_max[..., None])
        denominator = lax.optimization_barrier(jnp.sum(local_exp, axis=(2, 3))) + lax.optimization_barrier(jnp.sum(ctx_exp, axis=2))
        local_weights = (local_exp / denominator[..., None, None]).astype(jnp.bfloat16)
        ctx_weights = (ctx_exp / denominator[..., None]).astype(jnp.bfloat16)
        result = jnp.einsum('rqjk,rjkd->rqd', local_weights.astype(jnp.float32), v_band) + jnp.einsum('rqn,nd->rqd', ctx_weights.astype(jnp.float32), vc_head.astype(jnp.float32))
        return result.astype(jnp.bfloat16)
    attended = lax.map(one_head, (per_head(queries, TOKENS), per_head(keys_lat, TOKENS), per_head(values_lat, TOKENS), per_head(ctx_keys, CTX), per_head(ctx_values, CTX), offset_bias))
    attended = attended.transpose(1, 2, 0, 3).reshape(TOKENS, ATT_W)
    group_cols = ATT_W // N_TP
    branch = jnp.zeros((TOKENS, D), jnp.float32)
    for group in range(N_TP):
        partial_value = jnp.dot(attended[:, group * group_cols:(group + 1) * group_cols], out_weight[group * group_cols:(group + 1) * group_cols], preferred_element_type=jnp.float32)
        rounded = lax.optimization_barrier(partial_value.astype(jnp.bfloat16))
        branch = branch + rounded.astype(jnp.float32)
    return (latent.astype(jnp.float32) + gate_vec[0] * branch).astype(jnp.bfloat16)
```

```python
import functools

import jax
import jax.numpy as jnp
from jax import lax
from jax.experimental import pallas as pl
from jax.experimental.pallas import tpu as pltpu
from jax.sharding import PartitionSpec as P

HEAD_DIM = 64
GRID_W = 64
WIN_ROWS = 8
WIN_COLS = 16


EPS = 1e-06


def extended(x, sides, width):
    for axis, dim in sides:
        count, length = (lax.axis_size(axis), x.shape[dim])
        up = [(i, (i + 1) % count) for i in range(count - 1)]
        down = [(j, i) for i, j in up]
        last = lax.slice_in_dim(x, length - width, length, axis=dim)
        initial = lax.slice_in_dim(x, 0, width, axis=dim)
        before = lax.ppermute(last, axis, up)
        after = lax.ppermute(initial, axis, down)
        x = jnp.concatenate([before, x, after], axis=dim)
    return x


def modulate(rows_in, norm_gain, shift_vec, scale_vec):
    values = rows_in.astype(jnp.float32)
    normed = values * lax.rsqrt(jnp.mean(values * values, axis=-1, keepdims=True) + EPS)
    return (normed * norm_gain * (1.0 + scale_vec) + shift_vec).astype(jnp.bfloat16)


def head_norm(projected, head_gain):
    row_count = projected.shape[0]
    split_heads = projected.reshape(row_count, -1, head_gain.shape[0])
    normed = split_heads * lax.rsqrt(
        jnp.mean(split_heads * split_heads, axis=-1, keepdims=True) + EPS
    )
    return (normed * head_gain).astype(jnp.bfloat16).reshape(row_count, -1)


def per_device_plain(
    latent,
    context,
    condition,
    ctx_condition,
    shift_weight,
    scale_weight,
    gate_weight,
    norm_gain,
    query_weight,
    key_weight,
    value_weight,
    query_gain,
    key_gain,
    offset_bias,
    out_weight,
):
    activations = jax.nn.silu(jnp.stack([condition, ctx_condition])).astype(jnp.bfloat16)
    part_shift = jnp.dot(activations, shift_weight, preferred_element_type=jnp.float32)
    part_scale = jnp.dot(activations, scale_weight, preferred_element_type=jnp.float32)
    part_gate = jnp.dot(activations[:1], gate_weight, preferred_element_type=jnp.float32)
    block_cols = shift_weight.shape[1]
    first_col = lax.axis_index("tp") * block_cols

    def spread(piece_part):
        padded_vec = jnp.zeros((piece_part.shape[0], block_cols * lax.axis_size("tp")), jnp.float32)
        return lax.dynamic_update_slice_in_dim(padded_vec, piece_part, first_col, 1)

    shift_vec, scale_vec, gate_vec = lax.psum(
        (spread(part_shift), spread(part_scale), spread(part_gate)), ("sp", "tp")
    )
    hidden = modulate(latent, norm_gain, shift_vec[0], scale_vec[0])
    queries = head_norm(
        jnp.dot(hidden, query_weight, preferred_element_type=jnp.float32), query_gain
    )
    keys_lat = head_norm(jnp.dot(hidden, key_weight, preferred_element_type=jnp.float32), key_gain)
    values_lat = jnp.dot(hidden, value_weight, preferred_element_type=jnp.float32).astype(
        jnp.bfloat16
    )
    ctx_hidden = modulate(
        lax.all_gather(context, "sp", axis=0, tiled=True), norm_gain, shift_vec[1], scale_vec[1]
    )
    ctx_keys = head_norm(
        jnp.dot(ctx_hidden, key_weight, preferred_element_type=jnp.float32), key_gain
    )
    ctx_values = jnp.dot(ctx_hidden, value_weight, preferred_element_type=jnp.float32).astype(
        jnp.bfloat16
    )
    ctx_pairs = jnp.concatenate([ctx_keys, ctx_values], axis=1)
    col_width = keys_lat.shape[1]
    heads_dev = col_width // HEAD_DIM
    local_rows = keys_lat.shape[0] // GRID_W
    halo_rows = WIN_ROWS // 2
    window_keys = WIN_ROWS * GRID_W
    key_value = jnp.concatenate([keys_lat, values_lat], axis=1).reshape(
        local_rows, GRID_W, 2 * col_width
    )
    padded = extended(key_value, (("sp", 0),), halo_rows)
    first_row = lax.axis_index("sp") * local_rows
    total_rows = local_rows * lax.axis_size("sp")
    global_rows = first_row + jnp.arange(local_rows, dtype=jnp.int32)
    band_start = jnp.clip(global_rows - halo_rows, 0, total_rows - WIN_ROWS)
    band_global = band_start[:, None] + jnp.arange(WIN_ROWS, dtype=jnp.int32)[None, :]
    banded = jnp.take(padded, band_global - first_row + halo_rows, axis=0)
    key_band = banded[..., :col_width].reshape(local_rows, window_keys, heads_dev, HEAD_DIM)
    value_band = banded[..., col_width:].reshape(local_rows, window_keys, heads_dev, HEAD_DIM)
    row_steps = band_global - global_rows[:, None] + WIN_ROWS - 1
    row_hot = (
        row_steps[:, :, None] == jnp.arange(2 * WIN_ROWS - 1, dtype=jnp.int32)[None, None, :]
    ).astype(jnp.float32)
    column_ids = jnp.arange(GRID_W, dtype=jnp.int32)
    col_steps = (
        jnp.clip(column_ids[None, :] - column_ids[:, None], 1 - WIN_COLS, WIN_COLS - 1)
        + WIN_COLS
        - 1
    )
    col_hot = (
        col_steps[:, :, None] == jnp.arange(2 * WIN_COLS - 1, dtype=jnp.int32)[None, None, :]
    ).astype(jnp.float32)
    col_start = jnp.clip(column_ids - WIN_COLS // 2, 0, GRID_W - WIN_COLS)
    col_open = (column_ids[None, :] >= col_start[:, None]) & (
        column_ids[None, :] < col_start[:, None] + WIN_COLS
    )
    col_table = jnp.einsum("hab,qkb->haqk", offset_bias, col_hot, precision=lax.Precision.HIGHEST)
    col_table = jnp.where(col_open[None, None, :, :], col_table, -jnp.inf)
    offset_terms = jnp.einsum(
        "rja,haqk->hrqjk",
        row_hot,
        jnp.where(col_open[None, None], col_table, 0.0),
        precision=lax.Precision.HIGHEST,
    )
    offset_terms = jnp.where(col_open[None, None, :, None, :], offset_terms, -jnp.inf)
    offset_terms = offset_terms.reshape(heads_dev, local_rows, GRID_W, window_keys)
    score_scale = HEAD_DIM ** (-0.5)
    q_grid = queries.reshape(local_rows, GRID_W, heads_dev, HEAD_DIM)
    scores = (
        jnp.einsum("rqhd,rnhd->hrqn", q_grid, key_band, preferred_element_type=jnp.float32)
        * score_scale
        + offset_terms
    )
    ctx_count = ctx_pairs.shape[0]
    ctx_keys_all = ctx_pairs[:, :col_width].reshape(ctx_count, heads_dev, HEAD_DIM)
    ctx_values_all = ctx_pairs[:, col_width:].reshape(ctx_count, heads_dev, HEAD_DIM)
    ctx_scores = (
        jnp.einsum("rqhd,nhd->hrqn", q_grid, ctx_keys_all, preferred_element_type=jnp.float32)
        * score_scale
    )
    row_max = jnp.maximum(jnp.max(scores, axis=3), jnp.max(ctx_scores, axis=3))
    local_exp = jnp.exp(scores - row_max[..., None])
    ctx_exp = jnp.exp(ctx_scores - row_max[..., None])
    denominator = jnp.sum(local_exp, axis=3) + jnp.sum(ctx_exp, axis=3)
    local_weights = (local_exp / denominator[..., None]).astype(jnp.bfloat16)
    ctx_weights = (ctx_exp / denominator[..., None]).astype(jnp.bfloat16)
    combined = jnp.einsum(
        "hrqn,rnhd->rqhd", local_weights, value_band, preferred_element_type=jnp.float32
    ) + jnp.einsum(
        "hrqn,nhd->rqhd", ctx_weights, ctx_values_all, preferred_element_type=jnp.float32
    )
    attended = combined.astype(jnp.bfloat16).reshape(local_rows * GRID_W, col_width)
    partial_value = jnp.dot(attended, out_weight, preferred_element_type=jnp.float32)
    branch = lax.psum(partial_value.astype(jnp.bfloat16), "tp").astype(jnp.float32)
    return (latent.astype(jnp.float32) + gate_vec[0] * branch).astype(jnp.bfloat16)


MESH = pl.DeviceIdType.MESH
MASKED = -1e30
F32 = jnp.float32
BF16 = jnp.bfloat16


def fused_kernel(
    n_sp,
    n_tp,
    latent,
    context,
    shift_w,
    scale_w,
    gate_w,
    query_w,
    key_w,
    value_w,
    out_w,
    cond,
    ctx_cond,
    norm_gain,
    query_gain,
    key_gain,
    bias_in,
    out,
    cond_v,
    ctx_cond_v,
    norm_gain_v,
    query_gain_v,
    key_gain_v,
    bias_v,
    x_in,
    x_norm,
    hid,
    w_mod,
    w_qkv,
    w_out,
    mod_sp,
    mod_tp,
    gate_sp,
    gate_tp,
    acc,
    q_stage,
    k_stage,
    v_stage,
    ck_stage,
    cv_stage,
    q_all,
    k_all,
    v_all,
    ctx_k,
    ctx_v,
    bias_pad,
    bias_lines,
    table,
    att_slab,
    att,
    local_sem,
    mod_send,
    mod_recv,
    modt_send,
    modt_recv,
    gate_send,
    gate_recv,
    gatet_send,
    gatet_recv,
    pair_send,
    pair_recv,
    halo_send,
    halo_recv,
    ctx_send,
    ctx_recv,
    wo_send,
    wo_recv,
    att_send,
    att_recv,
):
    me_s, me_t = lax.axis_index("sp"), lax.axis_index("tp")
    rows, d = latent.shape
    c_rows = context.shape[0]
    width = key_w.shape[1]
    heads = width // HEAD_DIM
    block = shift_w.shape[1]
    blocks = block // 128
    l_rows = rows // GRID_W
    halo = WIN_ROWS // 2
    win = WIN_ROWS * GRID_W
    core = lax.rem(me_t, 2)
    chip = lax.div(me_t, 2)
    partner = me_t + 1 - 2 * core
    n_x = n_tp // 2
    side = lax.rem(me_s, 2)
    slab = lax.div(me_s, 2)
    mate = me_s + 1 - 2 * side
    last_slab = n_sp // 2 - 1
    half = width // 2
    half_heads = heads // 2

    def remote(src, dst, send, recv, s, t):
        return pltpu.make_async_remote_copy(
            src_ref=src, dst_ref=dst, send_sem=send, recv_sem=recv,
            device_id=(s, t), device_id_type=MESH,
        )

    loads = [
        (shift_w, w_mod.at[0]),
        (scale_w, w_mod.at[1]),
        (gate_w, w_mod.at[2]),
        (context, x_in.at[pl.ds(0, c_rows)]),
        (latent, x_in.at[pl.ds(c_rows, rows)]),
        (key_w, w_qkv.at[0]),
        (value_w, w_qkv.at[1]),
        (query_w, w_qkv.at[2]),
        (out_w, w_out.at[me_t]),
        (cond, cond_v),
        (ctx_cond, ctx_cond_v),
        (norm_gain, norm_gain_v),
        (query_gain, query_gain_v),
        (key_gain, key_gain_v),
        (bias_in, bias_v),
    ]
    copies = [pltpu.make_async_copy(a, b, local_sem.at[i]) for i, (a, b) in enumerate(loads)]
    for i in (9, 10, 0, 1, 2, 11, 12, 13, 14, 3, 4):
        copies[i].start()

    barrier = pltpu.get_barrier_semaphore()
    for k in range(1, n_sp):
        pl.semaphore_signal(
            barrier, inc=1, device_id=(lax.rem(me_s + k, n_sp), me_t), device_id_type=MESH
        )
    for k in range(1, n_tp):
        pl.semaphore_signal(
            barrier, inc=1, device_id=(me_s, lax.rem(me_t + k, n_tp)), device_id_type=MESH
        )

    def silu(v):
        return v / (1.0 + jnp.exp(-v))

    two = (16, cond.shape[1])
    row_id = lax.broadcasted_iota(jnp.int32, two, 0)
    copies[9].wait()
    copies[10].wait()
    act0 = jnp.broadcast_to(silu(cond_v[...]), two)
    act1 = jnp.broadcast_to(silu(ctx_cond_v[...]), two)

    def placed(first, second):
        picked = jnp.where(row_id == first, act0, 0.0)
        if second is not None:
            picked = jnp.where(row_id == second, act1, picked)
        return picked.astype(BF16)

    part = jnp.zeros((16, block), F32)
    for i, (first, second) in enumerate(((0, 1), (2, 3), (4, None))):
        copies[i].wait()
        part += jnp.dot(placed(first, second), w_mod[i], preferred_element_type=F32)
    for b in range(blocks):
        mod_sp[me_s, 4 * b : 4 * b + 4, :] = part[:4, b * 128 : (b + 1) * 128]
        gate_sp[me_s, b : b + 1, :] = part[4:5, b * 128 : (b + 1) * 128]
    pl.semaphore_wait(barrier, n_sp + n_tp - 2)
    sends = []

    def share_sp(buf, send, recv):
        for k in range(1, n_sp):
            peer = lax.rem(me_s + k, n_sp)
            c = remote(buf.at[me_s], buf.at[me_s], send.at[k], recv.at[me_s], peer, me_t)
            c.start()
            sends.append(c)

    def sum_sp(buf, send, recv):
        for k in range(1, n_sp):
            peer = lax.rem(me_s + k, n_sp)
            remote(buf.at[peer], buf.at[peer], send.at[k], recv.at[peer], peer, me_t).wait_recv()
        total = buf[0]
        for k in range(1, n_sp):
            total = total + buf[k]
        return total

    def share_tp(buf, send, recv):
        for k in range(1, n_tp):
            peer = lax.rem(me_t + k, n_tp)
            c = remote(buf.at[me_t], buf.at[me_t], send.at[k], recv.at[me_t], me_s, peer)
            c.start()
            sends.append(c)

    def wait_tp(buf, send, recv):
        for k in range(1, n_tp):
            peer = lax.rem(me_t + k, n_tp)
            remote(buf.at[peer], buf.at[peer], send.at[k], recv.at[peer], me_s, peer).wait_recv()

    share_sp(mod_sp, mod_send, mod_recv)
    for i in (5, 6, 7, 8):
        copies[i].start()

    def gather_start(view, sems, source=None):
        send, recv = sems
        mine = view(me_t) if source is None else source
        started = [remote(mine, view(me_t), send(0), recv(me_t), me_s, partner)]
        for k in range(1, n_x):
            far = 2 * lax.rem(chip + k, n_x) + core
            started.append(remote(mine, view(me_t), send(k), recv(me_t), me_s, far))
        for c in reversed(started):
            c.start()
        sends.extend(started)

    def gather_forward(view, sems):
        send, recv = sems
        for k in range(1, n_x):
            came = 2 * lax.rem(chip + n_x - k, n_x) + core
            c = remote(view(came), view(came), send(n_x + k), recv(came), me_s, partner)
            c.wait_recv()
            c.start()
            sends.append(c)

    far = 2 * (1 - chip) + core
    far_partner = 2 * (1 - chip) + 1 - core
    piece = width // 8
    y_pieces = 2
    direct = width - 2 * y_pieces * piece

    def wo_rows(c, at_side):
        if c < y_pieces:
            start = direct + at_side * y_pieces * piece + c * piece
        else:
            start = (c - y_pieces) * piece
        return pl.ds(pl.multiple_of(start, piece), piece)

    n_pieces = direct // piece + y_pieces

    def wo_copy(kind, c, source, shard, rows_at, s, t):
        return remote(
            source.at[rows_at], w_out.at[shard, rows_at],
            wo_send.at[kind, c], wo_recv.at[kind, c], s, t,
        )

    def begin(c):
        c.start()
        sends.append(c)

    def wo_far(c):
        return wo_copy(0, c, out_w, me_t, wo_rows(c, side), me_s, far)

    def wo_forward(c):
        at_rows = wo_rows(c, side)
        came = w_out.at[far]
        wo_copy(0, c, came, far, at_rows, me_s, far).wait_recv()
        begin(wo_copy(1, c, came, far, at_rows, me_s, partner))
        if c < y_pieces:
            begin(wo_copy(2, c, came, far, at_rows, mate, me_t))

    def wo_cross(c):
        at_rows = wo_rows(c, 1 - side)
        came = w_out.at[far]
        wo_copy(2, c, came, far, at_rows, mate, me_t).wait_recv()
        begin(wo_copy(3, c, came, far, at_rows, me_s, partner))

    def wo_finish_far():
        for c in range(n_pieces):
            wo_copy(
                1, c, w_out.at[far_partner], far_partner, wo_rows(c, side), me_s, partner
            ).wait_recv()
        for c in range(y_pieces):
            wo_copy(
                3, c, w_out.at[far_partner], far_partner, wo_rows(c, 1 - side), me_s, partner
            ).wait_recv()

    def wo_partner():
        return remote(
            out_w, w_out.at[me_t], wo_send.at[4, 0], wo_recv.at[4, 0], me_s, partner
        )

    def att_view(h):
        return lambda j: att.at[j, h]

    def att_sems(n):
        return (lambda k: att_send.at[n, k]), (lambda k: att_recv.at[n, k])

    begin(wo_far(0))

    copies[3].wait()
    copies[4].wait()
    copies[11].wait()
    step = 32

    def norm_rows(i, carry):
        at = pl.ds(pl.multiple_of(i * step, step), step)
        v = x_in[at, :].astype(F32)
        r = lax.rsqrt(jnp.mean(v * v, axis=-1, keepdims=True) + EPS)
        x_norm[at, :] = v * r * norm_gain_v[...]
        return carry

    lax.fori_loop(0, (rows + c_rows) // step, norm_rows, 0)

    pair = 2 * GRID_W
    q_col = lax.broadcasted_iota(jnp.int32, (GRID_W, pair), 0)
    k_col = lax.broadcasted_iota(jnp.int32, (GRID_W, pair), 1) % GRID_W
    col0 = jnp.clip(q_col - WIN_COLS // 2, 0, GRID_W - WIN_COLS)
    col_open = (k_col >= col0) & (k_col < col0 + WIN_COLS)
    n_pairs = 2 * WIN_ROWS - 2
    copies[14].wait()
    bias_pad[...] = jnp.zeros_like(bias_pad)
    for h in range(heads):
        bias_pad[h, : 2 * WIN_ROWS - 1, : 2 * WIN_COLS - 1] = bias_v[:, h, :]
    for h in range(half_heads):
        head = side * half_heads + h
        upper = pltpu.roll(bias_pad[head, 1 : n_pairs + 1, :], GRID_W, 1)
        bias_lines[h, :n_pairs, :] = bias_pad[head, :n_pairs, :] + upper
        for a in range(n_pairs):
            line = jnp.broadcast_to(bias_lines[h, a : a + 1, :], (GRID_W, pair))
            rolled = pltpu.roll(line, pair - (WIN_COLS - 1), 1, stride=1, stride_axis=0)
            table[a, h * GRID_W : (h + 1) * GRID_W, :] = jnp.where(col_open, rolled, MASKED)

    mod_tp[me_t] = sum_sp(mod_sp, mod_send, mod_recv)
    share_tp(mod_tp, modt_send, modt_recv)
    begin(wo_partner())
    share_sp(gate_sp, gate_send, gate_recv)
    wait_tp(mod_tp, modt_send, modt_recv)
    for c in range(1, n_pieces):
        begin(wo_far(c))

    def vec(r):
        return jnp.concatenate(
            [mod_tp[j, 4 * b + r : 4 * b + r + 1, :] for j in range(n_tp) for b in range(blocks)],
            axis=1,
        )

    def modulate_rows(first, count, shift, scale):
        def body(i, carry):
            at = pl.ds(pl.multiple_of(first + i * step, step), step)
            hid[at, :] = (x_norm[at, :] * scale + shift).astype(BF16)
            return carry

        lax.fori_loop(0, count // step, body, 0)

    modulate_rows(0, c_rows, vec(1), 1.0 + vec(3))
    modulate_rows(c_rows, rows, vec(0), 1.0 + vec(2))

    head_row = lax.broadcasted_iota(jnp.int32, (width, width), 0) // HEAD_DIM
    head_col = lax.broadcasted_iota(jnp.int32, (width, width), 1) // HEAD_DIM
    same_head = (head_row == head_col).astype(BF16)
    copies[12].wait()
    copies[13].wait()

    def head_scale(p, gain):
        squares = p * p
        high = squares.astype(BF16)
        low = (squares - high.astype(F32)).astype(BF16)
        mean = jnp.dot(high, same_head, preferred_element_type=F32)
        mean = mean + jnp.dot(low, same_head, preferred_element_type=F32)
        mean = mean * (1.0 / HEAD_DIM)
        wide_gain = jnp.concatenate([gain[...]] * heads, axis=1)
        return (p * lax.rsqrt(mean + EPS) * wide_gain).astype(BF16)

    own = pl.ds(rows + pl.multiple_of(side * rows, rows), rows)
    other = pl.ds(rows + pl.multiple_of((1 - side) * rows, rows), rows)

    def split(stage, value):
        for h in range(2):
            stage[h] = value[:, h * half : (h + 1) * half]

    def trade(index, stage, block_all, at):
        c = remote(
            stage.at[1 - side], block_all.at[at], pair_send.at[index], pair_recv.at[index],
            mate, me_t,
        )
        c.start()
        sends.append(c)
        return c

    def share_ctx(index, stage, block_ctx):
        block_ctx[me_s] = stage[side]
        for k in range(1, n_sp):
            peer = lax.rem(me_s + k, n_sp)
            c = remote(
                stage.at[lax.rem(peer, 2)], block_ctx.at[me_s],
                ctx_send.at[index, k], ctx_recv.at[index, me_s], peer, me_t,
            )
            c.start()
            sends.append(c)

    def halo_copies(index, block_all):
        down = remote(
            block_all.at[pl.ds(rows, rows)], block_all.at[pl.ds(3 * rows, rows)],
            halo_send.at[index, 0], halo_recv.at[index, 0], me_s - 2, me_t,
        )
        up = remote(
            block_all.at[pl.ds(2 * rows, rows)], block_all.at[pl.ds(0, rows)],
            halo_send.at[index, 1], halo_recv.at[index, 1], me_s + 2, me_t,
        )
        return down, up

    def halo_start(mine, index, block_all):
        down, up = halo_copies(index, block_all)
        is_low = side == 0 if mine else side == 1

        @pl.when(is_low & (slab > 0))
        def _():
            down.start()

        @pl.when(jnp.logical_not(is_low) & (slab < last_slab))
        def _():
            up.start()

    copies[5].wait()
    keys = head_scale(jnp.dot(hid[...], w_qkv[0], preferred_element_type=F32), key_gain_v)
    split(k_stage, keys[c_rows:])
    k_trade = trade(0, k_stage, k_all, own)
    k_all[own, :] = k_stage[side]
    halo_start(True, 0, k_all)
    split(ck_stage, keys[:c_rows])
    share_ctx(0, ck_stage, ctx_k)
    copies[6].wait()
    values = jnp.dot(hid[...], w_qkv[1], preferred_element_type=F32).astype(BF16)
    split(v_stage, values[c_rows:])
    v_trade = trade(1, v_stage, v_all, own)
    v_all[own, :] = v_stage[side]
    halo_start(True, 1, v_all)
    split(cv_stage, values[:c_rows])
    share_ctx(1, cv_stage, ctx_v)
    copies[7].wait()
    queries = head_scale(
        jnp.dot(hid[c_rows:, :], w_qkv[2], preferred_element_type=F32), query_gain_v
    ) * jnp.asarray(HEAD_DIM ** (-0.5), BF16)
    split(q_stage, queries)
    q_own = pl.ds(pl.multiple_of(side * rows, rows), rows)
    q_trade = trade(2, q_stage, q_all, q_own)
    q_all[q_own, :] = q_stage[side]
    gate_tp[me_t] = sum_sp(gate_sp, gate_send, gate_recv)
    share_tp(gate_tp, gatet_send, gatet_recv)
    wo_forward(0)
    k_trade.wait_recv()
    halo_start(False, 0, k_all)
    v_trade.wait_recv()
    halo_start(False, 1, v_all)
    q_trade.wait_recv()

    for index, block_ctx in enumerate((ctx_k, ctx_v)):
        for k in range(1, n_sp):
            peer = lax.rem(me_s + k, n_sp)
            remote(
                block_ctx.at[peer], block_ctx.at[peer],
                ctx_send.at[index, k], ctx_recv.at[index, peer], peer, me_t,
            ).wait_recv()
    for index, block_all in enumerate((k_all, v_all)):
        down, up = halo_copies(index, block_all)

        @pl.when(slab < last_slab)
        def _():
            down.wait_recv()

        @pl.when(slab > 0)
        def _():
            up.wait_recv()

    lane_head = lax.broadcasted_iota(jnp.int32, (GRID_W, half), 1) // HEAD_DIM
    masks = [(lane_head == h).astype(F32) for h in range(half_heads)]
    contract_last = (((1,), (1,)), ((), ()))
    all_ck = ctx_k[...].reshape(n_sp * c_rows, half)
    all_cv = ctx_v[...].reshape(n_sp * c_rows, half)

    def attend(i):
        start = jnp.where(
            slab == 0,
            jnp.maximum(i, halo),
            jnp.where(slab == last_slab, jnp.minimum(i, halo), i),
        )
        if last_slab == 0:
            start = jnp.int32(halo)
        at = pl.ds(pl.multiple_of(start * GRID_W, GRID_W), win)
        row_at = pl.ds(pl.multiple_of(i * GRID_W, GRID_W), GRID_W)
        qi = q_all[row_at, :].astype(F32)
        qs = jnp.concatenate([(qi * m).astype(BF16) for m in masks], axis=0)
        s1 = lax.dot_general(qs, k_all[at, :], contract_last, preferred_element_type=F32)
        first = start - i + WIN_ROWS - 1 - halo
        s1 = s1 + jnp.concatenate([table[first + 2 * m] for m in range(WIN_ROWS // 2)], axis=1)
        s2 = lax.dot_general(qs, all_ck, contract_last, preferred_element_type=F32)
        top = jnp.maximum(
            jnp.max(s1, axis=1, keepdims=True), jnp.max(s2, axis=1, keepdims=True)
        )
        e1 = jnp.exp(s1 - top)
        e2 = jnp.exp(s2 - top)
        inv = 1.0 / (jnp.sum(e1, axis=1, keepdims=True) + jnp.sum(e2, axis=1, keepdims=True))
        o = jnp.dot((e1 * inv).astype(BF16), v_all[at, :], preferred_element_type=F32)
        o = o + jnp.dot((e2 * inv).astype(BF16), all_cv, preferred_element_type=F32)
        picked = o[:GRID_W] * masks[0]
        for h in range(1, half_heads):
            picked = picked + o[h * GRID_W : (h + 1) * GRID_W] * masks[h]
        return picked.astype(BF16)

    for i in range(l_rows):
        att_slab[i * GRID_W : (i + 1) * GRID_W, :] = attend((1 - side) * l_rows + i)
    back = remote(
        att_slab, att.at[me_t, side], pair_send.at[3], pair_recv.at[3], mate, me_t
    )
    back.start()
    sends.append(back)
    wo_forward(1)
    for i in range(l_rows):
        att[me_t, side, i * GRID_W : (i + 1) * GRID_W, :] = attend(side * l_rows + i)

    back_in = remote(
        att_slab, att.at[me_t, 1 - side], pair_send.at[3], pair_recv.at[3], mate, me_t
    )
    first, second = att_view(side), att_view(1 - side)
    gather_start(first, att_sems(0))
    back_in.wait_recv()
    gather_start(second, att_sems(1))
    for c in range(2, n_pieces):
        wo_forward(c)
    for c in range(y_pieces):
        wo_cross(c)
    wait_tp(gate_tp, gatet_send, gatet_recv)
    gate = jnp.concatenate(
        [gate_tp[j, b : b + 1, :] for j in range(n_tp) for b in range(blocks)], axis=1
    )
    copies[8].wait()
    cols = 512

    def project(j, first_group, last_group):
        heads_of = jnp.concatenate([att[j, 0], att[j, 1]], axis=1)
        for n in range(d // cols):
            at = slice(n * cols, (n + 1) * cols)
            term = jnp.dot(heads_of, w_out[j, :, at], preferred_element_type=F32)
            term = term.astype(BF16).astype(F32)
            if not first_group:
                term = acc[:, at] + term
            if last_group:
                base = x_in[c_rows:, at].astype(F32)
                out[:, at] = (base + gate[:, at] * term).astype(BF16)
            else:
                acc[:, at] = term

    project(me_t, True, False)
    gather_forward(first, att_sems(0))
    gather_forward(second, att_sems(1))
    remote(
        w_out.at[partner], w_out.at[partner], wo_send.at[4, 0], wo_recv.at[4, 0], me_s, partner
    ).wait_recv()

    def att_wait(view, sems):
        send, recv = sems
        remote(
            view(partner), view(partner), send(0), recv(partner), me_s, partner
        ).wait_recv()

    def att_wait_far(view, sems):
        send, recv = sems
        remote(
            view(far_partner), view(far_partner), send(n_x + 1), recv(far_partner), me_s, partner
        ).wait_recv()

    att_wait(first, att_sems(0))
    att_wait(second, att_sems(1))
    project(partner, False, False)
    project(far, False, False)
    wo_finish_far()
    att_wait_far(first, att_sems(0))
    att_wait_far(second, att_sems(1))
    project(far_partner, False, True)

    for c in sends:
        c.wait_send()
    for index, block_all in enumerate((k_all, v_all)):
        down, up = halo_copies(index, block_all)

        @pl.when(slab > 0)
        def _():
            down.wait_send()

        @pl.when(slab < last_slab)
        def _():
            up.wait_send()


def per_device(
    latent,
    context,
    condition,
    ctx_condition,
    shift_weight,
    scale_weight,
    gate_weight,
    norm_gain,
    query_weight,
    key_weight,
    value_weight,
    query_gain,
    key_gain,
    offset_bias,
    out_weight,
):
    n_sp, n_tp = lax.axis_size("sp"), lax.axis_size("tp")
    rows, d = latent.shape
    c_rows = context.shape[0]
    width = key_weight.shape[1]
    heads = width // HEAD_DIM
    block = shift_weight.shape[1]
    n_pairs = 2 * WIN_ROWS - 2
    half = width // 2
    half_heads = heads // 2
    blocks = block // 128
    any_spec = pl.BlockSpec(memory_space=pl.ANY)
    vmem_spec = pl.BlockSpec(memory_space=pltpu.VMEM)
    dma = pltpu.SemaphoreType.DMA
    return pl.pallas_call(
        functools.partial(fused_kernel, n_sp, n_tp),
        out_shape=pltpu.VMEM((rows, d), BF16),
        in_specs=[any_spec] * 15,
        out_specs=vmem_spec,
        scratch_shapes=[
            pltpu.VMEM((1, condition.shape[0]), F32),
            pltpu.VMEM((1, condition.shape[0]), F32),
            pltpu.VMEM((1, d), F32),
            pltpu.VMEM((1, HEAD_DIM), F32),
            pltpu.VMEM((1, HEAD_DIM), F32),
            pltpu.VMEM((2 * WIN_ROWS - 1, heads, 2 * WIN_COLS - 1), F32),
            pltpu.VMEM((rows + c_rows, d), BF16),
            pltpu.VMEM((rows + c_rows, d), F32),
            pltpu.VMEM((rows + c_rows, d), BF16),
            pltpu.VMEM((3, shift_weight.shape[0], block), BF16),
            pltpu.VMEM((3, d, width), BF16),
            pltpu.VMEM((n_tp, width, d), BF16),
            pltpu.VMEM((n_sp, 4 * blocks, 128), F32),
            pltpu.VMEM((n_tp, 4 * blocks, 128), F32),
            pltpu.VMEM((n_sp, blocks, 128), F32),
            pltpu.VMEM((n_tp, blocks, 128), F32),
            pltpu.VMEM((rows, d), F32),
            pltpu.VMEM((2, rows, half), BF16),
            pltpu.VMEM((2, rows, half), BF16),
            pltpu.VMEM((2, rows, half), BF16),
            pltpu.VMEM((2, c_rows, half), BF16),
            pltpu.VMEM((2, c_rows, half), BF16),
            pltpu.VMEM((2 * rows, half), BF16),
            pltpu.VMEM((4 * rows, half), BF16),
            pltpu.VMEM((4 * rows, half), BF16),
            pltpu.VMEM((n_sp, c_rows, half), BF16),
            pltpu.VMEM((n_sp, c_rows, half), BF16),
            pltpu.VMEM((heads, 2 * WIN_ROWS, 2 * GRID_W), F32),
            pltpu.VMEM((half_heads, 2 * WIN_ROWS, 2 * GRID_W), F32),
            pltpu.VMEM((n_pairs, half_heads * GRID_W, 2 * GRID_W), F32),
            pltpu.VMEM((rows, half), BF16),
            pltpu.VMEM((n_tp, 2, rows, half), BF16),
            dma((15,)),
            dma((n_sp,)),
            dma((n_sp,)),
            dma((n_tp,)),
            dma((n_tp,)),
            dma((n_sp,)),
            dma((n_sp,)),
            dma((n_tp,)),
            dma((n_tp,)),
            dma((4,)),
            dma((4,)),
            dma((2, 2)),
            dma((2, 2)),
            dma((2, n_sp)),
            dma((2, n_sp)),
            dma((5, 8)),
            dma((5, 8)),
            dma((2, n_tp)),
            dma((2, n_tp)),
        ],
        compiler_params=pltpu.CompilerParams(collective_id=0, has_side_effects=True),
        name="fused_block",
    )(
        latent,
        context,
        shift_weight,
        scale_weight,
        gate_weight,
        query_weight,
        key_weight,
        value_weight,
        out_weight,
        condition.reshape(1, -1),
        ctx_condition.reshape(1, -1),
        norm_gain.reshape(1, -1),
        query_gain.reshape(1, -1),
        key_gain.reshape(1, -1),
        offset_bias.transpose(1, 0, 2),
    )


def fused_fits(latent, context, condition, query_weight, n_sp, n_tp):
    rows, c_rows = latent.shape[0] // n_sp, context.shape[0] // n_sp
    width = query_weight.shape[1] // n_tp
    return (
        rows == WIN_ROWS // 2 * GRID_W
        and c_rows % 32 == 0
        and condition.shape[0] // n_sp % 128 == 0
        and condition.shape[0] // n_tp % 256 == 0
        and condition.shape[0] // n_tp <= 1024
        and width % 256 == 0
        and n_tp == 4
        and n_sp % 2 == 0
    )


def solution(mesh):
    in_specs = (
        P("sp", None),
        P("sp", None),
        P("sp"),
        P("sp"),
        P("sp", "tp"),
        P("sp", "tp"),
        P("sp", "tp"),
        P(),
        P(None, "tp"),
        P(None, "tp"),
        P(None, "tp"),
        P(),
        P(),
        P("tp", None, None),
        P("tp", None),
    )
    out_specs = P("sp", None)

    def step(latent, context, condition, ctx_condition, *rest):
        n_sp, n_tp = mesh.shape["sp"], mesh.shape["tp"]
        fits = fused_fits(latent, context, condition, rest[4], n_sp, n_tp)
        body = per_device if fits else per_device_plain
        return jax.shard_map(
            body, mesh=mesh, in_specs=in_specs, out_specs=out_specs, check_vma=False
        )(latent, context, condition, ctx_condition, *rest)

    return step
```

```python
import functools

import jax
import jax.numpy as jnp
from jax import lax
from jax.experimental import pallas as pl
from jax.experimental.pallas import tpu as pltpu
from jax.sharding import PartitionSpec as P

HEAD_DIM = 64
GRID_W = 64
WIN_ROWS = 8
WIN_COLS = 16


EPS = 1e-06


def extended(x, sides, width):
    for axis, dim in sides:
        count, length = (lax.axis_size(axis), x.shape[dim])
        up = [(i, (i + 1) % count) for i in range(count - 1)]
        down = [(j, i) for i, j in up]
        last = lax.slice_in_dim(x, length - width, length, axis=dim)
        initial = lax.slice_in_dim(x, 0, width, axis=dim)
        before = lax.ppermute(last, axis, up)
        after = lax.ppermute(initial, axis, down)
        x = jnp.concatenate([before, x, after], axis=dim)
    return x


def modulate(rows_in, norm_gain, shift_vec, scale_vec):
    values = rows_in.astype(jnp.float32)
    normed = values * lax.rsqrt(jnp.mean(values * values, axis=-1, keepdims=True) + EPS)
    return (normed * norm_gain * (1.0 + scale_vec) + shift_vec).astype(jnp.bfloat16)


def head_norm(projected, head_gain):
    row_count = projected.shape[0]
    split_heads = projected.reshape(row_count, -1, head_gain.shape[0])
    normed = split_heads * lax.rsqrt(
        jnp.mean(split_heads * split_heads, axis=-1, keepdims=True) + EPS
    )
    return (normed * head_gain).astype(jnp.bfloat16).reshape(row_count, -1)


def per_device_plain(
    latent,
    context,
    condition,
    ctx_condition,
    shift_weight,
    scale_weight,
    gate_weight,
    norm_gain,
    query_weight,
    key_weight,
    value_weight,
    query_gain,
    key_gain,
    offset_bias,
    out_weight,
):
    activations = jax.nn.silu(jnp.stack([condition, ctx_condition])).astype(jnp.bfloat16)
    part_shift = jnp.dot(activations, shift_weight, preferred_element_type=jnp.float32)
    part_scale = jnp.dot(activations, scale_weight, preferred_element_type=jnp.float32)
    part_gate = jnp.dot(activations[:1], gate_weight, preferred_element_type=jnp.float32)
    block_cols = shift_weight.shape[1]
    first_col = lax.axis_index("tp") * block_cols

    def spread(piece_part):
        padded_vec = jnp.zeros((piece_part.shape[0], block_cols * lax.axis_size("tp")), jnp.float32)
        return lax.dynamic_update_slice_in_dim(padded_vec, piece_part, first_col, 1)

    shift_vec, scale_vec, gate_vec = lax.psum(
        (spread(part_shift), spread(part_scale), spread(part_gate)), ("sp", "tp")
    )
    hidden = modulate(latent, norm_gain, shift_vec[0], scale_vec[0])
    queries = head_norm(
        jnp.dot(hidden, query_weight, preferred_element_type=jnp.float32), query_gain
    )
    keys_lat = head_norm(jnp.dot(hidden, key_weight, preferred_element_type=jnp.float32), key_gain)
    values_lat = jnp.dot(hidden, value_weight, preferred_element_type=jnp.float32).astype(
        jnp.bfloat16
    )
    ctx_hidden = modulate(
        lax.all_gather(context, "sp", axis=0, tiled=True), norm_gain, shift_vec[1], scale_vec[1]
    )
    ctx_keys = head_norm(
        jnp.dot(ctx_hidden, key_weight, preferred_element_type=jnp.float32), key_gain
    )
    ctx_values = jnp.dot(ctx_hidden, value_weight, preferred_element_type=jnp.float32).astype(
        jnp.bfloat16
    )
    ctx_pairs = jnp.concatenate([ctx_keys, ctx_values], axis=1)
    col_width = keys_lat.shape[1]
    heads_dev = col_width // HEAD_DIM
    local_rows = keys_lat.shape[0] // GRID_W
    halo_rows = WIN_ROWS // 2
    window_keys = WIN_ROWS * GRID_W
    key_value = jnp.concatenate([keys_lat, values_lat], axis=1).reshape(
        local_rows, GRID_W, 2 * col_width
    )
    padded = extended(key_value, (("sp", 0),), halo_rows)
    first_row = lax.axis_index("sp") * local_rows
    total_rows = local_rows * lax.axis_size("sp")
    global_rows = first_row + jnp.arange(local_rows, dtype=jnp.int32)
    band_start = jnp.clip(global_rows - halo_rows, 0, total_rows - WIN_ROWS)
    band_global = band_start[:, None] + jnp.arange(WIN_ROWS, dtype=jnp.int32)[None, :]
    banded = jnp.take(padded, band_global - first_row + halo_rows, axis=0)
    key_band = banded[..., :col_width].reshape(local_rows, window_keys, heads_dev, HEAD_DIM)
    value_band = banded[..., col_width:].reshape(local_rows, window_keys, heads_dev, HEAD_DIM)
    row_steps = band_global - global_rows[:, None] + WIN_ROWS - 1
    row_hot = (
        row_steps[:, :, None] == jnp.arange(2 * WIN_ROWS - 1, dtype=jnp.int32)[None, None, :]
    ).astype(jnp.float32)
    column_ids = jnp.arange(GRID_W, dtype=jnp.int32)
    col_steps = (
        jnp.clip(column_ids[None, :] - column_ids[:, None], 1 - WIN_COLS, WIN_COLS - 1)
        + WIN_COLS
        - 1
    )
    col_hot = (
        col_steps[:, :, None] == jnp.arange(2 * WIN_COLS - 1, dtype=jnp.int32)[None, None, :]
    ).astype(jnp.float32)
    col_start = jnp.clip(column_ids - WIN_COLS // 2, 0, GRID_W - WIN_COLS)
    col_open = (column_ids[None, :] >= col_start[:, None]) & (
        column_ids[None, :] < col_start[:, None] + WIN_COLS
    )
    col_table = jnp.einsum("hab,qkb->haqk", offset_bias, col_hot, precision=lax.Precision.HIGHEST)
    col_table = jnp.where(col_open[None, None, :, :], col_table, -jnp.inf)
    offset_terms = jnp.einsum(
        "rja,haqk->hrqjk",
        row_hot,
        jnp.where(col_open[None, None], col_table, 0.0),
        precision=lax.Precision.HIGHEST,
    )
    offset_terms = jnp.where(col_open[None, None, :, None, :], offset_terms, -jnp.inf)
    offset_terms = offset_terms.reshape(heads_dev, local_rows, GRID_W, window_keys)
    score_scale = HEAD_DIM ** (-0.5)
    q_grid = queries.reshape(local_rows, GRID_W, heads_dev, HEAD_DIM)
    scores = (
        jnp.einsum("rqhd,rnhd->hrqn", q_grid, key_band, preferred_element_type=jnp.float32)
        * score_scale
        + offset_terms
    )
    ctx_count = ctx_pairs.shape[0]
    ctx_keys_all = ctx_pairs[:, :col_width].reshape(ctx_count, heads_dev, HEAD_DIM)
    ctx_values_all = ctx_pairs[:, col_width:].reshape(ctx_count, heads_dev, HEAD_DIM)
    ctx_scores = (
        jnp.einsum("rqhd,nhd->hrqn", q_grid, ctx_keys_all, preferred_element_type=jnp.float32)
        * score_scale
    )
    row_max = jnp.maximum(jnp.max(scores, axis=3), jnp.max(ctx_scores, axis=3))
    local_exp = jnp.exp(scores - row_max[..., None])
    ctx_exp = jnp.exp(ctx_scores - row_max[..., None])
    denominator = jnp.sum(local_exp, axis=3) + jnp.sum(ctx_exp, axis=3)
    local_weights = (local_exp / denominator[..., None]).astype(jnp.bfloat16)
    ctx_weights = (ctx_exp / denominator[..., None]).astype(jnp.bfloat16)
    combined = jnp.einsum(
        "hrqn,rnhd->rqhd", local_weights, value_band, preferred_element_type=jnp.float32
    ) + jnp.einsum(
        "hrqn,nhd->rqhd", ctx_weights, ctx_values_all, preferred_element_type=jnp.float32
    )
    attended = combined.astype(jnp.bfloat16).reshape(local_rows * GRID_W, col_width)
    partial_value = jnp.dot(attended, out_weight, preferred_element_type=jnp.float32)
    branch = lax.psum(partial_value.astype(jnp.bfloat16), "tp").astype(jnp.float32)
    return (latent.astype(jnp.float32) + gate_vec[0] * branch).astype(jnp.bfloat16)


MESH = pl.DeviceIdType.MESH
MASKED = -1e30
LANES = 128
F32 = jnp.float32
BF16 = jnp.bfloat16


def fused_kernel(
    n_sp,
    n_tp,
    latent,
    context,
    shift_w,
    scale_w,
    gate_w,
    query_w,
    key_w,
    value_w,
    out_w,
    cond,
    ctx_cond,
    norm_gain,
    query_gain,
    key_gain,
    bias_in,
    out,
    cond_v,
    ctx_cond_v,
    norm_gain_v,
    query_gain_v,
    key_gain_v,
    bias_v,
    x_in,
    x_norm,
    hid,
    w_mod,
    w_qkv,
    w_out,
    mod_sp,
    mod_tp,
    part_kv,
    part_q,
    gate_sp,
    gate_tp,
    acc,
    q_stage,
    k_stage,
    v_stage,
    ck_stage,
    cv_stage,
    q_all,
    k_all,
    v_all,
    ctx_k,
    ctx_v,
    bias_pad,
    bias_lines,
    table,
    q_heads,
    scores,
    tops,
    sums,
    scores_ctx,
    weights,
    sums_ctx,
    att_slab,
    att,
    local_sem,
    mod_send,
    mod_recv,
    modt_send,
    modt_recv,
    gate_send,
    gate_recv,
    gatet_send,
    gatet_recv,
    pair_send,
    pair_recv,
    halo_send,
    halo_recv,
    ctx_send,
    ctx_recv,
    wo_send,
    wo_recv,
    att_send,
    att_recv,
):
    me_s, me_t = lax.axis_index("sp"), lax.axis_index("tp")
    rows, d = latent.shape
    c_rows = context.shape[0]
    width = key_w.shape[1]
    heads = width // HEAD_DIM
    block = shift_w.shape[1]
    blocks = block // 128
    l_rows = rows // GRID_W
    halo = WIN_ROWS // 2
    win = WIN_ROWS * GRID_W
    core = lax.rem(me_t, 2)
    chip = lax.div(me_t, 2)
    partner = me_t + 1 - 2 * core
    far = 2 * (1 - chip) + core
    far_partner = 2 * (1 - chip) + 1 - core
    side = lax.rem(me_s, 2)
    slab = lax.div(me_s, 2)
    mate = me_s + 1 - 2 * side
    last_slab = n_sp // 2 - 1
    half = width // 2
    half_heads = heads // 2

    def remote(src, dst, send, recv, s, t):
        return pltpu.make_async_remote_copy(
            src_ref=src, dst_ref=dst, send_sem=send, recv_sem=recv,
            device_id=(s, t), device_id_type=MESH,
        )

    loads = [
        (shift_w, w_mod.at[0]),
        (scale_w, w_mod.at[1]),
        (gate_w, w_mod.at[2]),
        (context, x_in.at[pl.ds(0, c_rows)]),
        (latent, x_in.at[pl.ds(c_rows, rows)]),
        (key_w, w_qkv.at[:, pl.ds(0, width)]),
        (value_w, w_qkv.at[:, pl.ds(width, width)]),
        (query_w, w_qkv.at[:, pl.ds(2 * width, width)]),
        (out_w, w_out.at[me_t]),
        (cond, cond_v),
        (ctx_cond, ctx_cond_v),
        (norm_gain, norm_gain_v),
        (query_gain, query_gain_v),
        (key_gain, key_gain_v),
        (bias_in, bias_v),
    ]
    copies = [pltpu.make_async_copy(a, b, local_sem.at[i]) for i, (a, b) in enumerate(loads)]
    for i in (9, 10, 0, 1, 2, 11, 12, 13, 14, 3, 4):
        copies[i].start()

    barrier = pltpu.get_barrier_semaphore()
    for k in range(1, n_sp):
        pl.semaphore_signal(
            barrier, inc=1, device_id=(lax.rem(me_s + k, n_sp), me_t), device_id_type=MESH
        )
    for k in range(1, n_tp):
        pl.semaphore_signal(
            barrier, inc=1, device_id=(me_s, lax.rem(me_t + k, n_tp)), device_id_type=MESH
        )
    pl.semaphore_signal(barrier, inc=1, device_id=(mate, far), device_id_type=MESH)

    def silu(v):
        return v / (1.0 + jnp.exp(-v))

    two = (16, cond.shape[1])
    row_id = lax.broadcasted_iota(jnp.int32, two, 0)
    copies[9].wait()
    copies[10].wait()
    act0 = jnp.broadcast_to(silu(cond_v[...]), two)
    act1 = jnp.broadcast_to(silu(ctx_cond_v[...]), two)

    def placed(first, second):
        picked = jnp.where(row_id == first, act0, 0.0)
        if second is not None:
            picked = jnp.where(row_id == second, act1, picked)
        return picked.astype(BF16)

    part = jnp.zeros((16, block), F32)
    for i in range(2):
        copies[i].wait()
        part += jnp.dot(placed(2 * i, 2 * i + 1), w_mod[i], preferred_element_type=F32)
    for b in range(blocks):
        mod_sp[me_s, 4 * b : 4 * b + 4, :] = part[:4, b * 128 : (b + 1) * 128]
    pl.semaphore_wait(barrier, n_sp + n_tp - 1)
    sends = []

    def share_sp(buf, send, recv):
        for k in range(1, n_sp):
            peer = lax.rem(me_s + k, n_sp)
            c = remote(buf.at[me_s], buf.at[me_s], send.at[k], recv.at[me_s], peer, me_t)
            c.start()
            sends.append(c)

    def sum_sp(buf, send, recv):
        for k in range(1, n_sp):
            peer = lax.rem(me_s + k, n_sp)
            remote(buf.at[peer], buf.at[peer], send.at[k], recv.at[peer], peer, me_t).wait_recv()
        total = buf[0]
        for k in range(1, n_sp):
            total = total + buf[k]
        return total

    def share_tp(buf, send, recv):
        for k in range(1, n_tp):
            peer = lax.rem(me_t + k, n_tp)
            c = remote(buf.at[me_t], buf.at[me_t], send.at[k], recv.at[me_t], me_s, peer)
            c.start()
            sends.append(c)

    def wait_tp(buf, send, recv):
        for k in range(1, n_tp):
            peer = lax.rem(me_t + k, n_tp)
            remote(buf.at[peer], buf.at[peer], send.at[k], recv.at[peer], me_s, peer).wait_recv()

    share_sp(mod_sp, mod_send, mod_recv)
    for i in (5, 6, 7, 8):
        copies[i].start()
    copies[2].wait()
    gate_part = jnp.dot(placed(0, None), w_mod[2], preferred_element_type=F32)
    for b in range(blocks):
        gate_sp[me_s, b : b + 1, :] = gate_part[:1, b * 128 : (b + 1) * 128]

    piece = width // 8
    y_pieces = 2
    direct = width - 2 * y_pieces * piece

    def wo_rows(c, at_side):
        if c < y_pieces:
            start = direct + at_side * y_pieces * piece + c * piece
        else:
            start = (c - y_pieces) * piece
        return pl.ds(pl.multiple_of(start, piece), piece)

    n_pieces = direct // piece + y_pieces

    def wo_copy(kind, c, source, shard, rows_at, s, t):
        return remote(
            source.at[rows_at], w_out.at[shard, rows_at],
            wo_send.at[kind, c], wo_recv.at[kind, c], s, t,
        )

    def begin(c):
        c.start()
        sends.append(c)

    def wo_far(c):
        return wo_copy(0, c, out_w, me_t, wo_rows(c, side), me_s, far)

    def wo_forward(c):
        at_rows = wo_rows(c, side)
        came = w_out.at[far]
        wo_copy(0, c, came, far, at_rows, me_s, far).wait_recv()
        begin(wo_copy(1, c, came, far, at_rows, me_s, partner))
        if c < y_pieces:
            begin(wo_copy(2, c, came, far, at_rows, mate, me_t))

    def wo_cross(c):
        at_rows = wo_rows(c, 1 - side)
        came = w_out.at[far]
        wo_copy(2, c, came, far, at_rows, mate, me_t).wait_recv()
        begin(wo_copy(3, c, came, far, at_rows, me_s, partner))

    def wo_finish_far():
        for c in range(n_pieces):
            wo_copy(
                1, c, w_out.at[far_partner], far_partner, wo_rows(c, side), me_s, partner
            ).wait_recv()
        for c in range(y_pieces):
            wo_copy(
                3, c, w_out.at[far_partner], far_partner, wo_rows(c, 1 - side), me_s, partner
            ).wait_recv()

    def wo_partner():
        return remote(
            out_w, w_out.at[me_t], wo_send.at[4, 0], wo_recv.at[4, 0], me_s, partner
        )

    begin(wo_far(0))

    copies[3].wait()
    copies[4].wait()
    copies[11].wait()
    step = 32

    def norm_rows(i, carry):
        at = pl.ds(pl.multiple_of(i * step, step), step)
        v = x_in[at, :].astype(F32)
        r = lax.rsqrt(jnp.mean(v * v, axis=-1, keepdims=True) + EPS)
        x_norm[at, :] = v * r * norm_gain_v[...]
        return carry

    lax.fori_loop(0, (rows + c_rows) // step, norm_rows, 0)

    pair = 2 * GRID_W
    q_col = lax.broadcasted_iota(jnp.int32, (GRID_W, pair), 0)
    k_col = lax.broadcasted_iota(jnp.int32, (GRID_W, pair), 1) % GRID_W
    col0 = jnp.clip(q_col - WIN_COLS // 2, 0, GRID_W - WIN_COLS)
    col_open = (k_col >= col0) & (k_col < col0 + WIN_COLS)
    n_pairs = 2 * WIN_ROWS - 2
    copies[14].wait()
    bias_pad[...] = jnp.zeros_like(bias_pad)
    for h in range(heads):
        bias_pad[h, : 2 * WIN_ROWS - 1, : 2 * WIN_COLS - 1] = bias_v[:, h, :]
    for h in range(half_heads):
        head = side * half_heads + h
        upper = pltpu.roll(bias_pad[head, 1 : n_pairs + 1, :], GRID_W, 1)
        bias_lines[h, :n_pairs, :] = bias_pad[head, :n_pairs, :] + upper
        for a in range(n_pairs):
            line = jnp.broadcast_to(bias_lines[h, a : a + 1, :], (GRID_W, pair))
            rolled = pltpu.roll(line, pair - (WIN_COLS - 1), 1, stride=1, stride_axis=0)
            table[a, h * GRID_W : (h + 1) * GRID_W, :] = jnp.where(col_open, rolled, MASKED)

    mod_tp[me_t] = sum_sp(mod_sp, mod_send, mod_recv)
    share_tp(mod_tp, modt_send, modt_recv)
    for c in range(1, n_pieces):
        begin(wo_far(c))
    share_sp(gate_sp, gate_send, gate_recv)

    def wait_mod(peer):
        remote(
            mod_tp.at[peer], mod_tp.at[peer], modt_send.at[1], modt_recv.at[peer], me_s, peer
        ).wait_recv()

    pair_cols = 2 * block

    def vec(which, r):
        return jnp.concatenate(
            [
                mod_tp[2 * which + j, 4 * b + r : 4 * b + r + 1, :]
                for j in range(2)
                for b in range(blocks)
            ],
            axis=1,
        )

    def cols_of(which):
        return pl.ds(pl.multiple_of(which * pair_cols, pair_cols), pair_cols)

    def modulate_rows(which, first, count, shift, scale):
        def body(i, carry):
            at = pl.ds(pl.multiple_of(first + i * step, step), step)
            hid[at, cols_of(which)] = (x_norm[at, cols_of(which)] * scale + shift).astype(BF16)
            return carry

        lax.fori_loop(0, count // step, body, 0)

    def modulate_pair(which):
        modulate_rows(which, 0, c_rows, vec(which, 1), 1.0 + vec(which, 3))
        modulate_rows(which, c_rows, rows, vec(which, 0), 1.0 + vec(which, 2))

    def hidden_dot(which, start_row, start_col, count_col):
        return jnp.dot(
            hid[start_row:, cols_of(which)],
            w_qkv[cols_of(which), start_col : start_col + count_col],
            preferred_element_type=F32,
        )

    wait_mod(partner)
    modulate_pair(chip)
    for i in (5, 6, 7):
        copies[i].wait()
    part_kv[...] = hidden_dot(chip, 0, 0, 2 * width)
    part_q[...] = hidden_dot(chip, c_rows, 2 * width, width)
    wait_mod(far)
    wait_mod(far_partner)
    modulate_pair(1 - chip)

    head_row = lax.broadcasted_iota(jnp.int32, (width, width), 0) // HEAD_DIM
    head_col = lax.broadcasted_iota(jnp.int32, (width, width), 1) // HEAD_DIM
    same_head = (head_row == head_col).astype(BF16)
    copies[12].wait()
    copies[13].wait()

    def head_scale(p, gain):
        squares = p * p
        high = squares.astype(BF16)
        low = (squares - high.astype(F32)).astype(BF16)
        mean = jnp.dot(high, same_head, preferred_element_type=F32)
        mean = mean + jnp.dot(low, same_head, preferred_element_type=F32)
        mean = mean * (1.0 / HEAD_DIM)
        wide_gain = jnp.concatenate([gain[...]] * heads, axis=1)
        return (p * lax.rsqrt(mean + EPS) * wide_gain).astype(BF16)

    own = pl.ds(rows + pl.multiple_of(side * rows, rows), rows)
    other = pl.ds(rows + pl.multiple_of((1 - side) * rows, rows), rows)

    def split(stage, value):
        for h in range(2):
            stage[h] = value[:, h * half : (h + 1) * half]

    def trade(index, stage, block_all, at):
        c = remote(
            stage.at[1 - side], block_all.at[at], pair_send.at[index], pair_recv.at[index],
            mate, me_t,
        )
        c.start()
        sends.append(c)
        return c

    n_z = n_sp // 2
    z_order = tuple(range(2, n_z)) + (1,)

    def ctx_copy(index, slot, source, shard, block_ctx, s):
        return remote(
            source, block_ctx.at[shard], ctx_send.at[index, slot], ctx_recv.at[index, shard],
            s, me_t,
        )

    def along_z(index, slot, source, shard, block_ctx):
        for k in z_order:
            peer = 2 * lax.rem(slab + k, n_z) + side
            begin(ctx_copy(index, slot + k, source, shard, block_ctx, peer))

    def relay_ctx(index, block_ctx):
        ctx_copy(index, 0, block_ctx.at[mate], mate, block_ctx, mate).wait_recv()
        along_z(index, n_z - 1, block_ctx.at[mate], mate, block_ctx)

    lower = rows - GRID_W

    def halo_copies(index, block_all):
        down = remote(
            block_all.at[pl.ds(rows, lower)], block_all.at[pl.ds(3 * rows, lower)],
            halo_send.at[index, 0], halo_recv.at[index, 0], me_s - 2, me_t,
        )
        up = remote(
            block_all.at[pl.ds(2 * rows, rows)], block_all.at[pl.ds(0, rows)],
            halo_send.at[index, 1], halo_recv.at[index, 1], me_s + 2, me_t,
        )
        return down, up

    def halo_start(mine, index, block_all):
        down, up = halo_copies(index, block_all)
        is_low = side == 0 if mine else side == 1

        @pl.when(is_low & (slab > 0))
        def _():
            down.start()

        @pl.when(jnp.logical_not(is_low) & (slab < last_slab))
        def _():
            up.start()

    both = part_kv[...] + hidden_dot(1 - chip, 0, 0, 2 * width)
    keys = head_scale(both[:, :width], key_gain_v)
    split(ck_stage, keys[:c_rows])
    split(k_stage, keys[c_rows:])
    begin(ctx_copy(0, 0, ck_stage.at[1 - side], me_s, ctx_k, mate))
    k_trade = trade(0, k_stage, k_all, own)
    k_all[own, :] = k_stage[side]
    halo_start(True, 0, k_all)
    along_z(0, 0, ck_stage.at[side], me_s, ctx_k)
    ctx_k[me_s] = ck_stage[side]
    values = both[:, width:].astype(BF16)
    split(cv_stage, values[:c_rows])
    split(v_stage, values[c_rows:])
    begin(ctx_copy(1, 0, cv_stage.at[1 - side], me_s, ctx_v, mate))
    v_trade = trade(1, v_stage, v_all, own)
    v_all[own, :] = v_stage[side]
    halo_start(True, 1, v_all)
    along_z(1, 0, cv_stage.at[side], me_s, ctx_v)
    ctx_v[me_s] = cv_stage[side]
    queries = head_scale(
        part_q[...] + hidden_dot(1 - chip, c_rows, 2 * width, width), query_gain_v
    ) * jnp.asarray(HEAD_DIM ** (-0.5), BF16)
    split(q_stage, queries)
    q_own = pl.ds(pl.multiple_of(side * rows, rows), rows)
    q_trade = trade(2, q_stage, q_all, q_own)
    q_all[q_own, :] = q_stage[side]
    begin(wo_partner())
    gate_tp[me_t] = sum_sp(gate_sp, gate_send, gate_recv)
    share_tp(gate_tp, gatet_send, gatet_recv)
    relay_ctx(0, ctx_k)
    relay_ctx(1, ctx_v)
    for c in range(y_pieces):
        wo_forward(c)
    k_trade.wait_recv()
    halo_start(False, 0, k_all)
    v_trade.wait_recv()
    halo_start(False, 1, v_all)
    q_trade.wait_recv()
    for index, block_all in enumerate((k_all, v_all)):
        down, up = halo_copies(index, block_all)

        @pl.when(slab < last_slab)
        def _():
            down.wait_recv()

        @pl.when(slab > 0)
        def _():
            up.wait_recv()

    lane_head = lax.broadcasted_iota(jnp.int32, (GRID_W, half), 1) // HEAD_DIM
    masks = [(lane_head == h).astype(F32) for h in range(half_heads)]
    contract_last = (((1,), (1,)), ((), ()))
    stack = half_heads * GRID_W
    n_local = 2 * l_rows
    ones = jnp.ones((win, 128), BF16)

    def score_local(i):
        start = jnp.where(
            slab == 0,
            jnp.maximum(i, halo),
            jnp.where(slab == last_slab, jnp.minimum(i, halo), i),
        )
        if last_slab == 0:
            start = jnp.int32(halo)
        at = pl.ds(pl.multiple_of(start * GRID_W, GRID_W), win)
        qi = q_all[i * GRID_W : (i + 1) * GRID_W, :].astype(F32)
        qs = jnp.concatenate([(qi * m).astype(BF16) for m in masks], axis=0)
        q_heads[i] = qs
        s = lax.dot_general(qs, k_all[at, :], contract_last, preferred_element_type=F32)
        first = start - i + WIN_ROWS - 1 - halo
        s = s + jnp.concatenate([table[first + 2 * m] for m in range(WIN_ROWS // 2)], axis=1)
        scores[i % 2] = s
        return at, jnp.max(s, axis=1, keepdims=True)

    def weigh_local(i, at, top):
        e = jnp.exp(scores[i % 2] - top)
        tops[i] = jnp.broadcast_to(top, (stack, 128))
        values_at = jnp.concatenate([v_all[at, :], ones], axis=1)
        sums[i] = jnp.dot(e.astype(BF16), values_at, preferred_element_type=F32)

    held = score_local(0)
    for i in range(n_local):
        later = score_local(i + 1) if i + 1 < n_local else None
        weigh_local(i, *held)
        held = later

    for c in range(2, n_pieces - 2):
        wo_forward(c)
    for index, block_ctx in enumerate((ctx_k, ctx_v)):
        for s in range(n_sp):
            @pl.when((s != me_s) & (s != mate))
            def _():
                ctx_copy(index, 0, block_ctx.at[s], s, block_ctx, s).wait_recv()

    all_ck = ctx_k[...].reshape(n_sp * c_rows, half)
    all_cv = ctx_v[...].reshape(n_sp * c_rows, half)
    values_ctx = jnp.concatenate([all_cv, jnp.ones((n_sp * c_rows, 128), BF16)], axis=1)
    top_head = lax.broadcasted_iota(jnp.int32, (GRID_W, half), 1) // HEAD_DIM

    n_ctx = n_sp * c_rows
    half_stack = l_rows * stack

    def attend_half(which, store):
        blocks_of = [which * l_rows + i for i in range(l_rows)]
        qs = q_heads[pl.ds(which * l_rows, l_rows)].reshape(half_stack, half)
        scores_ctx[...] = lax.dot_general(
            qs, all_ck, contract_last, preferred_element_type=F32
        )
        fades = []
        for i in range(l_rows):
            at = slice(i * stack, (i + 1) * stack)
            s = scores_ctx[at, :]
            old = tops[blocks_of[i]]
            top = jnp.maximum(old, jnp.max(s, axis=1, keepdims=True))
            fades.append(jnp.exp(old - top))
            wide_top = jnp.concatenate([top] * (n_ctx // 128), axis=1)
            weights[at, :] = jnp.exp(s - wide_top).astype(BF16)
        sums_ctx[...] = jnp.dot(weights[...], values_ctx, preferred_element_type=F32)
        for i in range(l_rows):
            at = slice(i * stack, (i + 1) * stack)
            fade = jnp.concatenate([fades[i]] * ((half + 128) // 128), axis=1)
            o = sums_ctx[at, :] + sums[blocks_of[i]] * fade
            up, down = o[:, :half], o[:, half:]
            num, den = up[:GRID_W], down[:GRID_W]
            for h in range(1, half_heads):
                part_h = slice(h * GRID_W, (h + 1) * GRID_W)
                num = jnp.where(top_head == h, up[part_h], num)
                den = jnp.where(top_head == h, down[part_h], den)
            store(i, (num / den).astype(BF16))

    def att_copy(index, source, dest, s, t):
        return remote(source, dest, att_send.at[index], att_recv.at[index], s, t)

    def store_theirs(i, value):
        att_slab[i * GRID_W : (i + 1) * GRID_W, :] = value

    def store_mine(i, value):
        att[me_t, side, i * GRID_W : (i + 1) * GRID_W, :] = value

    attend_half(1 - side, store_theirs)
    begin(att_copy(0, att_slab, att.at[me_t, side], mate, far))
    begin(att_copy(1, att_slab, att.at[me_t, side], mate, me_t))
    attend_half(side, store_mine)
    begin(att_copy(2, att.at[me_t, side], att.at[me_t, side], me_s, far))
    begin(att_copy(3, att.at[me_t, side], att.at[me_t, side], me_s, partner))

    def arrived(index, shard, part_of):
        return att_copy(index, att.at[shard, part_of], att.at[shard, part_of], me_s, partner)

    def pass_on(index, onto, shard, part_of):
        arrived(index, shard, part_of).wait_recv()
        begin(arrived(onto, shard, part_of))

    for c in range(n_pieces - 2, n_pieces):
        wo_forward(c)
    for c in range(y_pieces):
        wo_cross(c)
    wait_tp(gate_tp, gatet_send, gatet_recv)
    gate = jnp.concatenate(
        [gate_tp[j, b : b + 1, :] for j in range(n_tp) for b in range(blocks)], axis=1
    )
    copies[8].wait()
    cols = 512

    def project(groups, last_pass):
        heads_of = [jnp.concatenate([att[j, 0], att[j, 1]], axis=1) for j in groups]
        for n in range(d // cols):
            at = slice(n * cols, (n + 1) * cols)
            total = None if not last_pass else acc[:, at]
            for j, lhs in zip(groups, heads_of):
                term = jnp.dot(lhs, w_out[j, :, at], preferred_element_type=F32)
                term = term.astype(BF16).astype(F32)
                total = term if total is None else total + term
            if last_pass:
                base = x_in[c_rows:, at].astype(F32)
                out[:, at] = (base + gate[:, at] * total).astype(BF16)
            else:
                acc[:, at] = total

    pass_on(1, 5, me_t, 1 - side)
    pass_on(0, 4, far, 1 - side)
    pass_on(2, 6, far, side)
    project((me_t, far), False)
    remote(
        w_out.at[partner], w_out.at[partner], wo_send.at[4, 0], wo_recv.at[4, 0], me_s, partner
    ).wait_recv()
    arrived(3, partner, side).wait_recv()
    arrived(5, partner, 1 - side).wait_recv()
    wo_finish_far()
    arrived(4, far_partner, 1 - side).wait_recv()
    arrived(6, far_partner, side).wait_recv()
    project((partner, far_partner), True)

    for c in sends:
        c.wait_send()
    for index, block_all in enumerate((k_all, v_all)):
        down, up = halo_copies(index, block_all)

        @pl.when(slab > 0)
        def _():
            down.wait_send()

        @pl.when(slab < last_slab)
        def _():
            up.wait_send()


def per_device(
    latent,
    context,
    condition,
    ctx_condition,
    shift_weight,
    scale_weight,
    gate_weight,
    norm_gain,
    query_weight,
    key_weight,
    value_weight,
    query_gain,
    key_gain,
    offset_bias,
    out_weight,
):
    n_sp, n_tp = lax.axis_size("sp"), lax.axis_size("tp")
    rows, d = latent.shape
    c_rows = context.shape[0]
    width = key_weight.shape[1]
    heads = width // HEAD_DIM
    block = shift_weight.shape[1]
    n_pairs = 2 * WIN_ROWS - 2
    half = width // 2
    half_heads = heads // 2
    blocks = block // 128
    l_rows = rows // GRID_W
    stack = half_heads * GRID_W
    any_spec = pl.BlockSpec(memory_space=pl.ANY)
    vmem_spec = pl.BlockSpec(memory_space=pltpu.VMEM)
    dma = pltpu.SemaphoreType.DMA
    return pl.pallas_call(
        functools.partial(fused_kernel, n_sp, n_tp),
        out_shape=pltpu.VMEM((rows, d), BF16),
        in_specs=[any_spec] * 15,
        out_specs=vmem_spec,
        scratch_shapes=[
            pltpu.VMEM((1, condition.shape[0]), F32),
            pltpu.VMEM((1, condition.shape[0]), F32),
            pltpu.VMEM((1, d), F32),
            pltpu.VMEM((1, HEAD_DIM), F32),
            pltpu.VMEM((1, HEAD_DIM), F32),
            pltpu.VMEM((2 * WIN_ROWS - 1, heads, 2 * WIN_COLS - 1), F32),
            pltpu.VMEM((rows + c_rows, d), BF16),
            pltpu.VMEM((rows + c_rows, d), F32),
            pltpu.VMEM((rows + c_rows, d), BF16),
            pltpu.VMEM((3, shift_weight.shape[0], block), BF16),
            pltpu.VMEM((d, 3 * width), BF16),
            pltpu.VMEM((n_tp, width, d), BF16),
            pltpu.VMEM((n_sp, 4 * blocks, 128), F32),
            pltpu.VMEM((n_tp, 4 * blocks, 128), F32),
            pltpu.VMEM((rows + c_rows, 2 * width), F32),
            pltpu.VMEM((rows, width), F32),
            pltpu.VMEM((n_sp, blocks, 128), F32),
            pltpu.VMEM((n_tp, blocks, 128), F32),
            pltpu.VMEM((rows, d), F32),
            pltpu.VMEM((2, rows, half), BF16),
            pltpu.VMEM((2, rows, half), BF16),
            pltpu.VMEM((2, rows, half), BF16),
            pltpu.VMEM((2, c_rows, half), BF16),
            pltpu.VMEM((2, c_rows, half), BF16),
            pltpu.VMEM((2 * rows, half), BF16),
            pltpu.VMEM((4 * rows, half), BF16),
            pltpu.VMEM((4 * rows, half), BF16),
            pltpu.VMEM((n_sp, c_rows, half), BF16),
            pltpu.VMEM((n_sp, c_rows, half), BF16),
            pltpu.VMEM((heads, 2 * WIN_ROWS, 2 * GRID_W), F32),
            pltpu.VMEM((half_heads, 2 * WIN_ROWS, 2 * GRID_W), F32),
            pltpu.VMEM((n_pairs, half_heads * GRID_W, 2 * GRID_W), F32),
            pltpu.VMEM((2 * l_rows, stack, half), BF16),
            pltpu.VMEM((2, stack, WIN_ROWS * GRID_W), F32),
            pltpu.VMEM((2 * l_rows, stack, 128), F32),
            pltpu.VMEM((2 * l_rows, stack, half + 128), F32),
            pltpu.VMEM((l_rows * stack, n_sp * c_rows), F32),
            pltpu.VMEM((l_rows * stack, n_sp * c_rows), BF16),
            pltpu.VMEM((l_rows * stack, half + 128), F32),
            pltpu.VMEM((rows, half), BF16),
            pltpu.VMEM((n_tp, 2, rows, half), BF16),
            dma((15,)),
            dma((n_sp,)),
            dma((n_sp,)),
            dma((n_tp,)),
            dma((n_tp,)),
            dma((n_sp,)),
            dma((n_sp,)),
            dma((n_tp,)),
            dma((n_tp,)),
            dma((4,)),
            dma((4,)),
            dma((2, 2)),
            dma((2, 2)),
            dma((2, n_sp)),
            dma((2, n_sp)),
            dma((5, 8)),
            dma((5, 8)),
            dma((7,)),
            dma((7,)),
        ],
        compiler_params=pltpu.CompilerParams(collective_id=0, has_side_effects=True),
        name="fused_block",
    )(
        latent,
        context,
        shift_weight,
        scale_weight,
        gate_weight,
        query_weight,
        key_weight,
        value_weight,
        out_weight,
        condition.reshape(1, -1),
        ctx_condition.reshape(1, -1),
        norm_gain.reshape(1, -1),
        query_gain.reshape(1, -1),
        key_gain.reshape(1, -1),
        offset_bias.transpose(1, 0, 2),
    )


def fused_fits(latent, context, condition, query_weight, n_sp, n_tp):
    rows, c_rows = latent.shape[0] // n_sp, context.shape[0] // n_sp
    width = query_weight.shape[1] // n_tp
    return (
        rows == WIN_ROWS // 2 * GRID_W
        and c_rows % 32 == 0
        and condition.shape[0] // n_sp % 128 == 0
        and condition.shape[0] // n_tp % 256 == 0
        and condition.shape[0] // n_tp <= 1024
        and width == 2 * LANES
        and n_tp == 4
        and n_sp % 2 == 0
    )


def solution(mesh):
    in_specs = (
        P("sp", None),
        P("sp", None),
        P("sp"),
        P("sp"),
        P("sp", "tp"),
        P("sp", "tp"),
        P("sp", "tp"),
        P(),
        P(None, "tp"),
        P(None, "tp"),
        P(None, "tp"),
        P(),
        P(),
        P("tp", None, None),
        P("tp", None),
    )
    out_specs = P("sp", None)

    def step(latent, context, condition, ctx_condition, *rest):
        n_sp, n_tp = mesh.shape["sp"], mesh.shape["tp"]
        fits = fused_fits(latent, context, condition, rest[4], n_sp, n_tp)
        body = per_device if fits else per_device_plain
        return jax.shard_map(
            body, mesh=mesh, in_specs=in_specs, out_specs=out_specs, check_vma=False
        )(latent, context, condition, ctx_condition, *rest)

    return step
```

```python
import functools

import jax
import jax.numpy as jnp
from jax import lax
from jax.experimental import pallas as pl
from jax.experimental.pallas import tpu as pltpu
from jax.sharding import PartitionSpec as P

HEAD_DIM = 64
GRID_W = 64
WIN_ROWS = 8
WIN_COLS = 16


EPS = 1e-06


def extended(x, sides, width):
    for axis, dim in sides:
        count, length = (lax.axis_size(axis), x.shape[dim])
        up = [(i, (i + 1) % count) for i in range(count - 1)]
        down = [(j, i) for i, j in up]
        last = lax.slice_in_dim(x, length - width, length, axis=dim)
        initial = lax.slice_in_dim(x, 0, width, axis=dim)
        before = lax.ppermute(last, axis, up)
        after = lax.ppermute(initial, axis, down)
        x = jnp.concatenate([before, x, after], axis=dim)
    return x


def modulate(rows_in, norm_gain, shift_vec, scale_vec):
    values = rows_in.astype(jnp.float32)
    normed = values * lax.rsqrt(jnp.mean(values * values, axis=-1, keepdims=True) + EPS)
    return (normed * norm_gain * (1.0 + scale_vec) + shift_vec).astype(jnp.bfloat16)


def head_norm(projected, head_gain):
    row_count = projected.shape[0]
    split_heads = projected.reshape(row_count, -1, head_gain.shape[0])
    normed = split_heads * lax.rsqrt(
        jnp.mean(split_heads * split_heads, axis=-1, keepdims=True) + EPS
    )
    return (normed * head_gain).astype(jnp.bfloat16).reshape(row_count, -1)


def per_device_plain(
    latent,
    context,
    condition,
    ctx_condition,
    shift_weight,
    scale_weight,
    gate_weight,
    norm_gain,
    query_weight,
    key_weight,
    value_weight,
    query_gain,
    key_gain,
    offset_bias,
    out_weight,
):
    activations = jax.nn.silu(jnp.stack([condition, ctx_condition])).astype(jnp.bfloat16)
    part_shift = jnp.dot(activations, shift_weight, preferred_element_type=jnp.float32)
    part_scale = jnp.dot(activations, scale_weight, preferred_element_type=jnp.float32)
    part_gate = jnp.dot(activations[:1], gate_weight, preferred_element_type=jnp.float32)
    block_cols = shift_weight.shape[1]
    first_col = lax.axis_index("tp") * block_cols

    def spread(piece_part):
        padded_vec = jnp.zeros((piece_part.shape[0], block_cols * lax.axis_size("tp")), jnp.float32)
        return lax.dynamic_update_slice_in_dim(padded_vec, piece_part, first_col, 1)

    shift_vec, scale_vec, gate_vec = lax.psum(
        (spread(part_shift), spread(part_scale), spread(part_gate)), ("sp", "tp")
    )
    hidden = modulate(latent, norm_gain, shift_vec[0], scale_vec[0])
    queries = head_norm(
        jnp.dot(hidden, query_weight, preferred_element_type=jnp.float32), query_gain
    )
    keys_lat = head_norm(jnp.dot(hidden, key_weight, preferred_element_type=jnp.float32), key_gain)
    values_lat = jnp.dot(hidden, value_weight, preferred_element_type=jnp.float32).astype(
        jnp.bfloat16
    )
    ctx_hidden = modulate(
        lax.all_gather(context, "sp", axis=0, tiled=True), norm_gain, shift_vec[1], scale_vec[1]
    )
    ctx_keys = head_norm(
        jnp.dot(ctx_hidden, key_weight, preferred_element_type=jnp.float32), key_gain
    )
    ctx_values = jnp.dot(ctx_hidden, value_weight, preferred_element_type=jnp.float32).astype(
        jnp.bfloat16
    )
    ctx_pairs = jnp.concatenate([ctx_keys, ctx_values], axis=1)
    col_width = keys_lat.shape[1]
    heads_dev = col_width // HEAD_DIM
    local_rows = keys_lat.shape[0] // GRID_W
    halo_rows = WIN_ROWS // 2
    window_keys = WIN_ROWS * GRID_W
    key_value = jnp.concatenate([keys_lat, values_lat], axis=1).reshape(
        local_rows, GRID_W, 2 * col_width
    )
    padded = extended(key_value, (("sp", 0),), halo_rows)
    first_row = lax.axis_index("sp") * local_rows
    total_rows = local_rows * lax.axis_size("sp")
    global_rows = first_row + jnp.arange(local_rows, dtype=jnp.int32)
    band_start = jnp.clip(global_rows - halo_rows, 0, total_rows - WIN_ROWS)
    band_global = band_start[:, None] + jnp.arange(WIN_ROWS, dtype=jnp.int32)[None, :]
    banded = jnp.take(padded, band_global - first_row + halo_rows, axis=0)
    key_band = banded[..., :col_width].reshape(local_rows, window_keys, heads_dev, HEAD_DIM)
    value_band = banded[..., col_width:].reshape(local_rows, window_keys, heads_dev, HEAD_DIM)
    row_steps = band_global - global_rows[:, None] + WIN_ROWS - 1
    row_hot = (
        row_steps[:, :, None] == jnp.arange(2 * WIN_ROWS - 1, dtype=jnp.int32)[None, None, :]
    ).astype(jnp.float32)
    column_ids = jnp.arange(GRID_W, dtype=jnp.int32)
    col_steps = (
        jnp.clip(column_ids[None, :] - column_ids[:, None], 1 - WIN_COLS, WIN_COLS - 1)
        + WIN_COLS
        - 1
    )
    col_hot = (
        col_steps[:, :, None] == jnp.arange(2 * WIN_COLS - 1, dtype=jnp.int32)[None, None, :]
    ).astype(jnp.float32)
    col_start = jnp.clip(column_ids - WIN_COLS // 2, 0, GRID_W - WIN_COLS)
    col_open = (column_ids[None, :] >= col_start[:, None]) & (
        column_ids[None, :] < col_start[:, None] + WIN_COLS
    )
    col_table = jnp.einsum("hab,qkb->haqk", offset_bias, col_hot, precision=lax.Precision.HIGHEST)
    col_table = jnp.where(col_open[None, None, :, :], col_table, -jnp.inf)
    offset_terms = jnp.einsum(
        "rja,haqk->hrqjk",
        row_hot,
        jnp.where(col_open[None, None], col_table, 0.0),
        precision=lax.Precision.HIGHEST,
    )
    offset_terms = jnp.where(col_open[None, None, :, None, :], offset_terms, -jnp.inf)
    offset_terms = offset_terms.reshape(heads_dev, local_rows, GRID_W, window_keys)
    score_scale = HEAD_DIM ** (-0.5)
    q_grid = queries.reshape(local_rows, GRID_W, heads_dev, HEAD_DIM)
    scores = (
        jnp.einsum("rqhd,rnhd->hrqn", q_grid, key_band, preferred_element_type=jnp.float32)
        * score_scale
        + offset_terms
    )
    ctx_count = ctx_pairs.shape[0]
    ctx_keys_all = ctx_pairs[:, :col_width].reshape(ctx_count, heads_dev, HEAD_DIM)
    ctx_values_all = ctx_pairs[:, col_width:].reshape(ctx_count, heads_dev, HEAD_DIM)
    ctx_scores = (
        jnp.einsum("rqhd,nhd->hrqn", q_grid, ctx_keys_all, preferred_element_type=jnp.float32)
        * score_scale
    )
    row_max = jnp.maximum(jnp.max(scores, axis=3), jnp.max(ctx_scores, axis=3))
    local_exp = jnp.exp(scores - row_max[..., None])
    ctx_exp = jnp.exp(ctx_scores - row_max[..., None])
    denominator = jnp.sum(local_exp, axis=3) + jnp.sum(ctx_exp, axis=3)
    local_weights = (local_exp / denominator[..., None]).astype(jnp.bfloat16)
    ctx_weights = (ctx_exp / denominator[..., None]).astype(jnp.bfloat16)
    combined = jnp.einsum(
        "hrqn,rnhd->rqhd", local_weights, value_band, preferred_element_type=jnp.float32
    ) + jnp.einsum(
        "hrqn,nhd->rqhd", ctx_weights, ctx_values_all, preferred_element_type=jnp.float32
    )
    attended = combined.astype(jnp.bfloat16).reshape(local_rows * GRID_W, col_width)
    partial_value = jnp.dot(attended, out_weight, preferred_element_type=jnp.float32)
    branch = lax.psum(partial_value.astype(jnp.bfloat16), "tp").astype(jnp.float32)
    return (latent.astype(jnp.float32) + gate_vec[0] * branch).astype(jnp.bfloat16)


MESH = pl.DeviceIdType.MESH
MASKED = -1e30
LANES = 128
F32 = jnp.float32
BF16 = jnp.bfloat16


def fused_kernel(
    n_sp,
    n_tp,
    latent,
    context,
    shift_w,
    scale_w,
    gate_w,
    query_w,
    key_w,
    value_w,
    out_w,
    cond,
    ctx_cond,
    norm_gain,
    query_gain,
    key_gain,
    bias_in,
    out,
    cond_v,
    ctx_cond_v,
    norm_gain_v,
    query_gain_v,
    key_gain_v,
    bias_v,
    x_in,
    x_norm,
    hid,
    w_mod,
    w_qkv,
    w_out,
    mod_sp,
    mod_tp,
    part_kv,
    part_q,
    gate_sp,
    gate_tp,
    acc,
    q_stage,
    k_stage,
    v_stage,
    ck_stage,
    cv_stage,
    q_all,
    k_all,
    v_all,
    ctx_k,
    ctx_v,
    bias_pad,
    bias_lines,
    table,
    q_heads,
    scores,
    tops,
    sums,
    scores_ctx,
    weights,
    sums_ctx,
    att_slab,
    att,
    local_sem,
    mod_send,
    mod_recv,
    modt_send,
    modt_recv,
    gate_send,
    gate_recv,
    gatet_send,
    gatet_recv,
    pair_send,
    pair_recv,
    halo_send,
    halo_recv,
    ctx_send,
    ctx_recv,
    end_send,
    wo_send,
    wo_recv,
    att_send,
    att_recv,
):
    me_s, me_t = lax.axis_index("sp"), lax.axis_index("tp")
    rows, d = latent.shape
    c_rows = context.shape[0]
    width = key_w.shape[1]
    heads = width // HEAD_DIM
    block = shift_w.shape[1]
    blocks = block // 128
    l_rows = rows // GRID_W
    halo = WIN_ROWS // 2
    win = WIN_ROWS * GRID_W
    core = lax.rem(me_t, 2)
    chip = lax.div(me_t, 2)
    partner = me_t + 1 - 2 * core
    far = 2 * (1 - chip) + core
    far_partner = 2 * (1 - chip) + 1 - core
    side = lax.rem(me_s, 2)
    slab = lax.div(me_s, 2)
    mate = me_s + 1 - 2 * side
    last_slab = n_sp // 2 - 1
    half = width // 2
    half_heads = heads // 2

    def remote(src, dst, send, recv, s, t):
        return pltpu.make_async_remote_copy(
            src_ref=src, dst_ref=dst, send_sem=send, recv_sem=recv,
            device_id=(s, t), device_id_type=MESH,
        )

    barrier = pltpu.get_barrier_semaphore()
    for k in range(1, n_sp):
        pl.semaphore_signal(
            barrier, inc=1, device_id=(lax.rem(me_s + k, n_sp), me_t), device_id_type=MESH
        )
    for k in range(1, n_tp):
        pl.semaphore_signal(
            barrier, inc=1, device_id=(me_s, lax.rem(me_t + k, n_tp)), device_id_type=MESH
        )
    pl.semaphore_signal(barrier, inc=1, device_id=(mate, far), device_id_type=MESH)

    loads = [
        (shift_w, w_mod.at[0]),
        (scale_w, w_mod.at[1]),
        (gate_w, w_mod.at[2]),
        (context, x_in.at[pl.ds(0, c_rows)]),
        (latent, x_in.at[pl.ds(c_rows, rows)]),
        (key_w, w_qkv.at[:, pl.ds(0, width)]),
        (value_w, w_qkv.at[:, pl.ds(width, width)]),
        (query_w, w_qkv.at[:, pl.ds(2 * width, width)]),
        (out_w, w_out.at[me_t]),
        (cond, cond_v),
        (ctx_cond, ctx_cond_v),
        (norm_gain, norm_gain_v),
        (query_gain, query_gain_v),
        (key_gain, key_gain_v),
        (bias_in, bias_v),
    ]
    copies = [pltpu.make_async_copy(a, b, local_sem.at[i]) for i, (a, b) in enumerate(loads)]
    for i in (9, 10, 0, 1, 2, 11, 12, 13, 14, 3, 4):
        copies[i].start()

    def silu(v):
        return v / (1.0 + jnp.exp(-v))

    two = (16, cond.shape[1])
    row_id = lax.broadcasted_iota(jnp.int32, two, 0)
    copies[9].wait()
    copies[10].wait()
    act0 = jnp.broadcast_to(silu(cond_v[...]), two)
    act1 = jnp.broadcast_to(silu(ctx_cond_v[...]), two)

    def placed(first, second):
        picked = jnp.where(row_id == first, act0, 0.0)
        if second is not None:
            picked = jnp.where(row_id == second, act1, picked)
        return picked.astype(BF16)

    part = jnp.zeros((16, block), F32)
    for i in range(2):
        copies[i].wait()
        part += jnp.dot(placed(2 * i, 2 * i + 1), w_mod[i], preferred_element_type=F32)
    for b in range(blocks):
        mod_sp[me_s, 4 * b : 4 * b + 4, :] = part[:4, b * 128 : (b + 1) * 128]
    pl.semaphore_wait(barrier, n_sp + n_tp - 1)
    sends = []

    def share_sp(buf, send, recv):
        for k in range(1, n_sp):
            peer = lax.rem(me_s + k, n_sp)
            c = remote(buf.at[me_s], buf.at[me_s], send.at[k], recv.at[me_s], peer, me_t)
            c.start()
            sends.append(c)

    def sum_sp(buf, send, recv):
        for k in range(1, n_sp):
            peer = lax.rem(me_s + k, n_sp)
            remote(buf.at[peer], buf.at[peer], send.at[k], recv.at[peer], peer, me_t).wait_recv()
        total = buf[0]
        for k in range(1, n_sp):
            total = total + buf[k]
        return total

    def share_tp(buf, send, recv):
        for k in range(1, n_tp):
            peer = lax.rem(me_t + k, n_tp)
            c = remote(buf.at[me_t], buf.at[me_t], send.at[k], recv.at[me_t], me_s, peer)
            c.start()
            sends.append(c)

    def wait_tp(buf, send, recv):
        for k in range(1, n_tp):
            peer = lax.rem(me_t + k, n_tp)
            remote(buf.at[peer], buf.at[peer], send.at[k], recv.at[peer], me_s, peer).wait_recv()

    share_sp(mod_sp, mod_send, mod_recv)
    for i in (5, 6, 7, 8):
        copies[i].start()
    copies[2].wait()
    gate_part = jnp.dot(placed(0, None), w_mod[2], preferred_element_type=F32)
    for b in range(blocks):
        gate_sp[me_s, b : b + 1, :] = gate_part[:1, b * 128 : (b + 1) * 128]

    piece = width // 16
    n_cross, n_direct = 3, 4
    n_pieces = 2 * n_cross + n_direct
    early = (0, n_cross)
    later = [c + o for c in range(1, n_cross) for o in (0, n_cross)]
    later = later + list(range(2 * n_cross, n_pieces))
    z_side = lax.rem(slab, 2)
    z_mate = me_s + 2 - 4 * z_side

    def wo_rows(c, away_from):
        if c < n_cross:
            start = (side + away_from - 2 * side * away_from) * n_cross * piece + c * piece
        elif c < 2 * n_cross:
            start = (
                2 * n_cross * piece
                + (z_side + away_from - 2 * z_side * away_from) * n_cross * piece
                + (c - n_cross) * piece
            )
        else:
            start = (2 * n_cross + c) * piece
        return pl.ds(pl.multiple_of(start, piece), piece)

    def wo_copy(kind, c, source, shard, rows_at, s, t):
        return remote(
            source.at[rows_at], w_out.at[shard, rows_at],
            wo_send.at[kind, c], wo_recv.at[kind, c], s, t,
        )

    def begin(c):
        c.start()
        sends.append(c)

    def wo_far(c):
        return wo_copy(0, c, out_w, me_t, wo_rows(c, 0), me_s, far)

    def wo_forward(c):
        at_rows = wo_rows(c, 0)
        came = w_out.at[far]
        wo_copy(0, c, came, far, at_rows, me_s, far).wait_recv()
        begin(wo_copy(1, c, came, far, at_rows, me_s, partner))
        if c < 2 * n_cross:
            begin(wo_copy(2, c, came, far, at_rows, mate if c < n_cross else z_mate, me_t))

    def wo_cross(c):
        at_rows = wo_rows(c, 1)
        came = w_out.at[far]
        wo_copy(2, c, came, far, at_rows, mate, me_t).wait_recv()
        begin(wo_copy(3, c, came, far, at_rows, me_s, partner))

    def wo_finish_far():
        for c in range(n_pieces):
            wo_copy(
                1, c, w_out.at[far_partner], far_partner, wo_rows(c, 0), me_s, partner
            ).wait_recv()
        for c in range(2 * n_cross):
            wo_copy(
                3, c, w_out.at[far_partner], far_partner, wo_rows(c, 1), me_s, partner
            ).wait_recv()

    def wo_partner():
        return remote(
            out_w, w_out.at[me_t], wo_send.at[4, 0], wo_recv.at[4, 0], me_s, partner
        )

    for c in early:
        begin(wo_far(c))

    copies[3].wait()
    copies[4].wait()
    copies[11].wait()
    step = 32

    def norm_rows(i, carry):
        at = pl.ds(pl.multiple_of(i * step, step), step)
        v = x_in[at, :].astype(F32)
        r = lax.rsqrt(jnp.mean(v * v, axis=-1, keepdims=True) + EPS)
        x_norm[at, :] = v * r * norm_gain_v[...]
        return carry

    lax.fori_loop(0, (rows + c_rows) // step, norm_rows, 0)

    pair = 2 * GRID_W
    q_col = lax.broadcasted_iota(jnp.int32, (GRID_W, pair), 0)
    k_col = lax.broadcasted_iota(jnp.int32, (GRID_W, pair), 1) % GRID_W
    col0 = jnp.clip(q_col - WIN_COLS // 2, 0, GRID_W - WIN_COLS)
    col_open = (k_col >= col0) & (k_col < col0 + WIN_COLS)
    n_pairs = 2 * WIN_ROWS - 2
    copies[14].wait()
    bias_pad[...] = jnp.zeros_like(bias_pad)
    for h in range(heads):
        bias_pad[h, : 2 * WIN_ROWS - 1, : 2 * WIN_COLS - 1] = bias_v[:, h, :]
    for h in range(half_heads):
        head = side * half_heads + h
        upper = pltpu.roll(bias_pad[head, 1 : n_pairs + 1, :], GRID_W, 1)
        bias_lines[h, :n_pairs, :] = bias_pad[head, :n_pairs, :] + upper
        for a in range(n_pairs):
            line = jnp.broadcast_to(bias_lines[h, a : a + 1, :], (GRID_W, pair))
            rolled = pltpu.roll(line, pair - (WIN_COLS - 1), 1, stride=1, stride_axis=0)
            table[a, h * GRID_W : (h + 1) * GRID_W, :] = jnp.where(col_open, rolled, MASKED)

    mod_tp[me_t] = sum_sp(mod_sp, mod_send, mod_recv)
    share_tp(mod_tp, modt_send, modt_recv)
    for c in later:
        begin(wo_far(c))
    share_sp(gate_sp, gate_send, gate_recv)

    def wait_mod(peer):
        remote(
            mod_tp.at[peer], mod_tp.at[peer], modt_send.at[1], modt_recv.at[peer], me_s, peer
        ).wait_recv()

    pair_cols = 2 * block

    def vec(which, r):
        return jnp.concatenate(
            [
                mod_tp[2 * which + j, 4 * b + r : 4 * b + r + 1, :]
                for j in range(2)
                for b in range(blocks)
            ],
            axis=1,
        )

    def cols_of(which):
        return pl.ds(pl.multiple_of(which * pair_cols, pair_cols), pair_cols)

    def modulate_rows(which, first, count, shift, scale):
        def body(i, carry):
            at = pl.ds(pl.multiple_of(first + i * step, step), step)
            hid[at, cols_of(which)] = (x_norm[at, cols_of(which)] * scale + shift).astype(BF16)
            return carry

        lax.fori_loop(0, count // step, body, 0)

    def modulate_pair(which):
        modulate_rows(which, 0, c_rows, vec(which, 1), 1.0 + vec(which, 3))
        modulate_rows(which, c_rows, rows, vec(which, 0), 1.0 + vec(which, 2))

    def hidden_dot(which, start_row, start_col, count_col):
        return jnp.dot(
            hid[start_row:, cols_of(which)],
            w_qkv[cols_of(which), start_col : start_col + count_col],
            preferred_element_type=F32,
        )

    wait_mod(partner)
    modulate_pair(chip)
    for i in (5, 6, 7):
        copies[i].wait()
    part_kv[...] = hidden_dot(chip, 0, 0, 2 * width)
    part_q[...] = hidden_dot(chip, c_rows, 2 * width, width)
    for c in early:
        wo_forward(c)
    wait_mod(far)
    wait_mod(far_partner)
    head_row = lax.broadcasted_iota(jnp.int32, (width, width), 0) // HEAD_DIM
    head_col = lax.broadcasted_iota(jnp.int32, (width, width), 1) // HEAD_DIM
    same_head = (head_row == head_col).astype(BF16)
    copies[12].wait()
    copies[13].wait()

    def head_scale(p, gain):
        squares = p * p
        high = squares.astype(BF16)
        low = (squares - high.astype(F32)).astype(BF16)
        mean = jnp.dot(high, same_head, preferred_element_type=F32)
        mean = mean + jnp.dot(low, same_head, preferred_element_type=F32)
        mean = mean * (1.0 / HEAD_DIM)
        wide_gain = jnp.concatenate([gain[...]] * heads, axis=1)
        return (p * lax.rsqrt(mean + EPS) * wide_gain).astype(BF16)

    own = pl.ds(rows + pl.multiple_of(side * rows, rows), rows)
    other = pl.ds(rows + pl.multiple_of((1 - side) * rows, rows), rows)

    def split(stage, value):
        for h in range(2):
            stage[h] = value[:, h * half : (h + 1) * half]

    def trade(index, stage, block_all, at):
        c = remote(
            stage.at[1 - side], block_all.at[at], pair_send.at[index], pair_recv.at[index],
            mate, me_t,
        )
        c.start()
        sends.append(c)
        return c

    n_z = n_sp // 2
    z_order = tuple(range(2, n_z)) + (1,)

    def ctx_copy(index, slot, source, shard, block_ctx, s):
        return remote(
            source, block_ctx.at[shard], ctx_send.at[index, slot], ctx_recv.at[index, shard],
            s, me_t,
        )

    at_end = (slab == 0) | (slab == last_slab)
    sends_when = []

    def along_z(index, slot, source, shard, block_ctx, all_direct=False):
        for k in z_order:
            peer = lax.rem(slab + k, n_z)
            c = ctx_copy(index, slot + k, source, shard, block_ctx, 2 * peer + side)
            low = (peer == 0) & (slab >= 2)
            high = (peer == last_slab) & (slab <= last_slab - 2)
            if all_direct:
                begin(c)
                continue
            direct = jnp.logical_not(low | high)
            pl.when(direct)(c.start)
            sends_when.append((direct, c))

    z_pair = lax.div(slab, 2)

    def relay_end(of_side):
        def body():
            for j in range(2):
                shard = 2 * (2 * (1 - z_pair) + j) + of_side
                for index, block_ctx in enumerate((ctx_k, ctx_v)):
                    ctx_copy(index, 0, block_ctx.at[shard], shard, block_ctx, shard).wait_recv()
                    end_copy(index, shard, block_ctx).start()

        pl.when(jnp.logical_not(at_end))(body)
        for j in range(2):
            shard = 2 * (2 * (1 - z_pair) + j) + of_side
            for index, block_ctx in enumerate((ctx_k, ctx_v)):
                sends_when.append((jnp.logical_not(at_end), end_copy(index, shard, block_ctx)))

    def end_copy(index, shard, block_ctx):
        return remote(
            block_ctx.at[shard], block_ctx.at[shard],
            end_send.at[index, shard], ctx_recv.at[index, shard],
            2 * z_pair * last_slab + side, me_t,
        )


    def relay_ctx(index, block_ctx):
        ctx_copy(index, 0, block_ctx.at[mate], mate, block_ctx, mate).wait_recv()
        along_z(index, n_z - 1, block_ctx.at[mate], mate, block_ctx, True)

    lower = rows - GRID_W

    def halo_copies(index, block_all):
        down = remote(
            block_all.at[pl.ds(rows, lower)], block_all.at[pl.ds(3 * rows, lower)],
            halo_send.at[index, 0], halo_recv.at[index, 0], me_s - 2, me_t,
        )
        up = remote(
            block_all.at[pl.ds(2 * rows, rows)], block_all.at[pl.ds(0, rows)],
            halo_send.at[index, 1], halo_recv.at[index, 1], me_s + 2, me_t,
        )
        return down, up

    def halo_start(mine, index, block_all):
        down, up = halo_copies(index, block_all)
        is_low = side == 0 if mine else side == 1

        @pl.when(is_low & (slab > 0))
        def _():
            down.start()

        @pl.when(jnp.logical_not(is_low) & (slab < last_slab))
        def _():
            up.start()

    away = 1 - chip
    modulate_rows(away, 0, c_rows, vec(away, 1), 1.0 + vec(away, 3))
    ctx_both = part_kv[:c_rows, :] + jnp.dot(
        hid[:c_rows, cols_of(away)], w_qkv[cols_of(away), : 2 * width], preferred_element_type=F32
    )
    ctx_keys = head_scale(ctx_both[:, :width], key_gain_v)
    ctx_values = ctx_both[:, width:].astype(BF16)
    split(ck_stage, ctx_keys)
    split(cv_stage, ctx_values)
    for index, (stage, block_ctx) in enumerate(((ck_stage, ctx_k), (cv_stage, ctx_v))):
        begin(ctx_copy(index, 0, stage.at[1 - side], me_s, block_ctx, mate))
        along_z(index, 0, stage.at[side], me_s, block_ctx)
        block_ctx[me_s] = stage[side]
    modulate_rows(away, c_rows, rows, vec(away, 0), 1.0 + vec(away, 2))
    both = part_kv[c_rows:, :] + hidden_dot(away, c_rows, 0, 2 * width)
    keys = head_scale(both[:, :width], key_gain_v)
    split(k_stage, keys)
    k_trade = trade(0, k_stage, k_all, own)
    k_all[own, :] = k_stage[side]
    halo_start(True, 0, k_all)
    split(v_stage, both[:, width:].astype(BF16))
    v_trade = trade(1, v_stage, v_all, own)
    v_all[own, :] = v_stage[side]
    halo_start(True, 1, v_all)
    queries = head_scale(
        part_q[...] + hidden_dot(away, c_rows, 2 * width, width), query_gain_v
    ) * jnp.asarray(HEAD_DIM ** (-0.5), BF16)
    split(q_stage, queries)
    q_own = pl.ds(pl.multiple_of(side * rows, rows), rows)
    q_trade = trade(2, q_stage, q_all, q_own)
    q_all[q_own, :] = q_stage[side]
    begin(wo_partner())
    gate_tp[me_t] = sum_sp(gate_sp, gate_send, gate_recv)
    share_tp(gate_tp, gatet_send, gatet_recv)
    relay_ctx(0, ctx_k)
    relay_ctx(1, ctx_v)
    relay_end(side)
    k_trade.wait_recv()
    halo_start(False, 0, k_all)
    for c in range(1, n_cross):
        wo_forward(c)
    v_trade.wait_recv()
    halo_start(False, 1, v_all)
    q_trade.wait_recv()
    def halo_wait(theirs_need):
        below = side == 0 if theirs_need else side == 1
        for index, block_all in enumerate((k_all, v_all)):
            down, up = halo_copies(index, block_all)

            @pl.when(below & (slab < last_slab))
            def _():
                down.wait_recv()

            @pl.when(jnp.logical_not(below) & (slab > 0))
            def _():
                up.wait_recv()

    lane_head = lax.broadcasted_iota(jnp.int32, (GRID_W, half), 1) // HEAD_DIM
    masks = [(lane_head == h).astype(F32) for h in range(half_heads)]
    contract_last = (((1,), (1,)), ((), ()))
    stack = half_heads * GRID_W
    ones = jnp.ones((win, 128), BF16)

    def score_local(i, held_at, slot):
        start = jnp.where(
            slab == 0,
            jnp.maximum(i, halo),
            jnp.where(slab == last_slab, jnp.minimum(i, halo), i),
        )
        if last_slab == 0:
            start = jnp.int32(halo)
        at = pl.ds(pl.multiple_of(start * GRID_W, GRID_W), win)
        qi = q_all[pl.ds(pl.multiple_of(i * GRID_W, GRID_W), GRID_W), :].astype(F32)
        qs = jnp.concatenate([(qi * m).astype(BF16) for m in masks], axis=0)
        q_heads[held_at] = qs
        s = lax.dot_general(qs, k_all[at, :], contract_last, preferred_element_type=F32)
        first = start - i + WIN_ROWS - 1 - halo
        s = s + jnp.concatenate([table[first + 2 * m] for m in range(WIN_ROWS // 2)], axis=1)
        scores[slot] = s
        return at, jnp.max(s, axis=1, keepdims=True)

    def weigh_local(held_at, slot, at, top):
        e = jnp.exp(scores[slot] - top)
        tops[held_at] = jnp.broadcast_to(top, (stack, 128))
        values_at = jnp.concatenate([v_all[at, :], ones], axis=1)
        sums[held_at] = jnp.dot(e.astype(BF16), values_at, preferred_element_type=F32)

    def local_half(which, base):
        first = which * l_rows
        held = score_local(first, base, 0)
        for i in range(l_rows):
            later = None
            if i + 1 < l_rows:
                later = score_local(first + i + 1, base + i + 1, (i + 1) % 2)
            weigh_local(base + i, i % 2, *held)
            held = later

    def ctx_wait():
        for index, block_ctx in enumerate((ctx_k, ctx_v)):
            for s in range(n_sp):

                relayed = jnp.logical_not(at_end) & (z_pair != s // 4) & (side == s % 2)

                @pl.when((s != me_s) & (s != mate) & jnp.logical_not(relayed))
                def _():
                    ctx_copy(index, 0, block_ctx.at[s], s, block_ctx, s).wait_recv()

    top_head = lax.broadcasted_iota(jnp.int32, (GRID_W, half), 1) // HEAD_DIM
    half_stack = l_rows * stack
    n_ctx = n_sp * c_rows
    ctx_ones = jnp.ones((n_ctx, 128), BF16)

    def ctx_half(base, store):
        qs = q_heads[base : base + l_rows].reshape(half_stack, half)
        scores_ctx[...] = lax.dot_general(
            qs, ctx_k[...].reshape(n_ctx, half), contract_last, preferred_element_type=F32
        )
        fades = []
        for i in range(l_rows):
            at_rows = slice(i * stack, (i + 1) * stack)
            s = scores_ctx[at_rows, :]
            old = tops[base + i]
            top = jnp.maximum(old, jnp.max(s, axis=1, keepdims=True))
            fade = jnp.exp(old - top)
            fades.append(jnp.concatenate([fade] * ((half + 128) // 128), axis=1))
            wide_top = jnp.concatenate([top] * (n_ctx // 128), axis=1)
            weights[at_rows, :] = jnp.exp(s - wide_top).astype(BF16)
        values_ctx = jnp.concatenate([ctx_v[...].reshape(n_ctx, half), ctx_ones], axis=1)
        sums_ctx[...] = jnp.dot(weights[...], values_ctx, preferred_element_type=F32)
        for i in range(l_rows):
            at_rows = slice(i * stack, (i + 1) * stack)
            o = sums_ctx[at_rows, :] + sums[base + i] * fades[i]
            up, down = o[:, :half], o[:, half:]
            num, den = up[:GRID_W], down[:GRID_W]
            for h in range(1, half_heads):
                part_h = slice(h * GRID_W, (h + 1) * GRID_W)
                num = jnp.where(top_head == h, up[part_h], num)
                den = jnp.where(top_head == h, down[part_h], den)
            store(i, (num / den).astype(BF16))

    def att_copy(index, source, dest, s, t):
        return remote(source, dest, att_send.at[index], att_recv.at[index], s, t)

    def store_theirs(i, value):
        att_slab[i * GRID_W : (i + 1) * GRID_W, :] = value

    def store_mine(i, value):
        att[me_t, side, i * GRID_W : (i + 1) * GRID_W, :] = value

    def local_mine():
        halo_wait(False)
        local_half(side, l_rows)

    for c in range(n_cross + 1, 2 * n_cross):
        wo_forward(c)
    halo_wait(True)
    local_half(1 - side, 0)
    no_halo = ((slab == 0) & (side == 0)) | ((slab == last_slab) & (side == 1))
    pl.when(no_halo)(local_mine)
    ctx_wait()
    ctx_half(0, store_theirs)
    begin(att_copy(0, att_slab, att.at[me_t, side], mate, far))
    begin(att_copy(1, att_slab, att.at[me_t, side], mate, me_t))
    pl.when(jnp.logical_not(no_halo))(local_mine)
    ctx_half(l_rows, store_mine)
    begin(att_copy(2, att.at[me_t, side], att.at[me_t, side], me_s, far))
    begin(att_copy(3, att.at[me_t, side], att.at[me_t, side], me_s, partner))

    def arrived(index, shard, part_of):
        return att_copy(index, att.at[shard, part_of], att.at[shard, part_of], me_s, partner)

    def pass_on(index, onto, shard, part_of):
        arrived(index, shard, part_of).wait_recv()
        begin(arrived(onto, shard, part_of))

    for c in range(2 * n_cross, n_pieces):
        wo_forward(c)
    for c in range(2 * n_cross):
        wo_cross(c)
    wait_tp(gate_tp, gatet_send, gatet_recv)
    gate = jnp.concatenate(
        [gate_tp[j, b : b + 1, :] for j in range(n_tp) for b in range(blocks)], axis=1
    )
    copies[8].wait()
    cols = 512

    def project(groups, last_pass):
        heads_of = [jnp.concatenate([att[j, 0], att[j, 1]], axis=1) for j in groups]
        for n in range(d // cols):
            at = slice(n * cols, (n + 1) * cols)
            total = None if not last_pass else acc[:, at]
            for j, lhs in zip(groups, heads_of):
                term = jnp.dot(lhs, w_out[j, :, at], preferred_element_type=F32)
                term = term.astype(BF16).astype(F32)
                total = term if total is None else total + term
            if last_pass:
                base = x_in[c_rows:, at].astype(F32)
                out[:, at] = (base + gate[:, at] * total).astype(BF16)
            else:
                acc[:, at] = total

    pass_on(1, 5, me_t, 1 - side)
    pass_on(0, 4, far, 1 - side)
    pass_on(2, 6, far, side)
    project((me_t, far), False)
    remote(
        w_out.at[partner], w_out.at[partner], wo_send.at[4, 0], wo_recv.at[4, 0], me_s, partner
    ).wait_recv()
    arrived(3, partner, side).wait_recv()
    arrived(5, partner, 1 - side).wait_recv()
    wo_finish_far()
    arrived(4, far_partner, 1 - side).wait_recv()
    arrived(6, far_partner, side).wait_recv()
    project((partner, far_partner), True)

    for c in sends:
        c.wait_send()
    for condition, c in sends_when:
        pl.when(condition)(c.wait_send)
    for index, block_all in enumerate((k_all, v_all)):
        down, up = halo_copies(index, block_all)

        @pl.when(slab > 0)
        def _():
            down.wait_send()

        @pl.when(slab < last_slab)
        def _():
            up.wait_send()


def per_device(
    latent,
    context,
    condition,
    ctx_condition,
    shift_weight,
    scale_weight,
    gate_weight,
    norm_gain,
    query_weight,
    key_weight,
    value_weight,
    query_gain,
    key_gain,
    offset_bias,
    out_weight,
):
    n_sp, n_tp = lax.axis_size("sp"), lax.axis_size("tp")
    rows, d = latent.shape
    c_rows = context.shape[0]
    width = key_weight.shape[1]
    heads = width // HEAD_DIM
    block = shift_weight.shape[1]
    n_pairs = 2 * WIN_ROWS - 2
    half = width // 2
    half_heads = heads // 2
    blocks = block // 128
    l_rows = rows // GRID_W
    stack = half_heads * GRID_W
    any_spec = pl.BlockSpec(memory_space=pl.ANY)
    vmem_spec = pl.BlockSpec(memory_space=pltpu.VMEM)
    dma = pltpu.SemaphoreType.DMA
    return pl.pallas_call(
        functools.partial(fused_kernel, n_sp, n_tp),
        out_shape=pltpu.VMEM((rows, d), BF16),
        in_specs=[any_spec] * 15,
        out_specs=vmem_spec,
        scratch_shapes=[
            pltpu.VMEM((1, condition.shape[0]), F32),
            pltpu.VMEM((1, condition.shape[0]), F32),
            pltpu.VMEM((1, d), F32),
            pltpu.VMEM((1, HEAD_DIM), F32),
            pltpu.VMEM((1, HEAD_DIM), F32),
            pltpu.VMEM((2 * WIN_ROWS - 1, heads, 2 * WIN_COLS - 1), F32),
            pltpu.VMEM((rows + c_rows, d), BF16),
            pltpu.VMEM((rows + c_rows, d), F32),
            pltpu.VMEM((rows + c_rows, d), BF16),
            pltpu.VMEM((3, shift_weight.shape[0], block), BF16),
            pltpu.VMEM((d, 3 * width), BF16),
            pltpu.VMEM((n_tp, width, d), BF16),
            pltpu.VMEM((n_sp, 4 * blocks, 128), F32),
            pltpu.VMEM((n_tp, 4 * blocks, 128), F32),
            pltpu.VMEM((rows + c_rows, 2 * width), F32),
            pltpu.VMEM((rows, width), F32),
            pltpu.VMEM((n_sp, blocks, 128), F32),
            pltpu.VMEM((n_tp, blocks, 128), F32),
            pltpu.VMEM((rows, d), F32),
            pltpu.VMEM((2, rows, half), BF16),
            pltpu.VMEM((2, rows, half), BF16),
            pltpu.VMEM((2, rows, half), BF16),
            pltpu.VMEM((2, c_rows, half), BF16),
            pltpu.VMEM((2, c_rows, half), BF16),
            pltpu.VMEM((2 * rows, half), BF16),
            pltpu.VMEM((4 * rows, half), BF16),
            pltpu.VMEM((4 * rows, half), BF16),
            pltpu.VMEM((n_sp, c_rows, half), BF16),
            pltpu.VMEM((n_sp, c_rows, half), BF16),
            pltpu.VMEM((heads, 2 * WIN_ROWS, 2 * GRID_W), F32),
            pltpu.VMEM((half_heads, 2 * WIN_ROWS, 2 * GRID_W), F32),
            pltpu.VMEM((n_pairs, half_heads * GRID_W, 2 * GRID_W), F32),
            pltpu.VMEM((2 * l_rows, stack, half), BF16),
            pltpu.VMEM((2, stack, WIN_ROWS * GRID_W), F32),
            pltpu.VMEM((2 * l_rows, stack, 128), F32),
            pltpu.VMEM((2 * l_rows, stack, half + 128), F32),
            pltpu.VMEM((l_rows * stack, n_sp * c_rows), F32),
            pltpu.VMEM((l_rows * stack, n_sp * c_rows), BF16),
            pltpu.VMEM((l_rows * stack, half + 128), F32),
            pltpu.VMEM((rows, half), BF16),
            pltpu.VMEM((n_tp, 2, rows, half), BF16),
            dma((15,)),
            dma((n_sp,)),
            dma((n_sp,)),
            dma((n_tp,)),
            dma((n_tp,)),
            dma((n_sp,)),
            dma((n_sp,)),
            dma((n_tp,)),
            dma((n_tp,)),
            dma((4,)),
            dma((4,)),
            dma((2, 2)),
            dma((2, 2)),
            dma((2, n_sp)),
            dma((2, n_sp)),
            dma((2, n_sp)),
            dma((5, 16)),
            dma((5, 16)),
            dma((7,)),
            dma((7,)),
        ],
        compiler_params=pltpu.CompilerParams(collective_id=0, has_side_effects=True),
        name="fused_block",
    )(
        latent,
        context,
        shift_weight,
        scale_weight,
        gate_weight,
        query_weight,
        key_weight,
        value_weight,
        out_weight,
        condition.reshape(1, -1),
        ctx_condition.reshape(1, -1),
        norm_gain.reshape(1, -1),
        query_gain.reshape(1, -1),
        key_gain.reshape(1, -1),
        offset_bias.transpose(1, 0, 2),
    )


def fused_fits(latent, context, condition, query_weight, n_sp, n_tp):
    rows, c_rows = latent.shape[0] // n_sp, context.shape[0] // n_sp
    width = query_weight.shape[1] // n_tp
    return (
        rows == WIN_ROWS // 2 * GRID_W
        and c_rows % 32 == 0
        and condition.shape[0] // n_sp % 128 == 0
        and condition.shape[0] // n_tp % 256 == 0
        and condition.shape[0] // n_tp <= 1024
        and width == 2 * LANES
        and n_tp == 4
        and n_sp == 8
    )


def solution(mesh):
    in_specs = (
        P("sp", None),
        P("sp", None),
        P("sp"),
        P("sp"),
        P("sp", "tp"),
        P("sp", "tp"),
        P("sp", "tp"),
        P(),
        P(None, "tp"),
        P(None, "tp"),
        P(None, "tp"),
        P(),
        P(),
        P("tp", None, None),
        P("tp", None),
    )
    out_specs = P("sp", None)

    def step(latent, context, condition, ctx_condition, *rest):
        n_sp, n_tp = mesh.shape["sp"], mesh.shape["tp"]
        fits = fused_fits(latent, context, condition, rest[4], n_sp, n_tp)
        body = per_device if fits else per_device_plain
        return jax.shard_map(
            body, mesh=mesh, in_specs=in_specs, out_specs=out_specs, check_vma=False
        )(latent, context, condition, ctx_condition, *rest)

    return step
```

```python
import functools

import jax
import jax.numpy as jnp
from jax import lax
from jax.experimental import pallas as pl
from jax.experimental.pallas import tpu as pltpu
from jax.sharding import PartitionSpec as P

HEAD_DIM = 64
GRID_W = 64
WIN_ROWS = 8
WIN_COLS = 16


EPS = 1e-06


def extended(x, sides, width):
    for axis, dim in sides:
        count, length = (lax.axis_size(axis), x.shape[dim])
        up = [(i, (i + 1) % count) for i in range(count - 1)]
        down = [(j, i) for i, j in up]
        last = lax.slice_in_dim(x, length - width, length, axis=dim)
        initial = lax.slice_in_dim(x, 0, width, axis=dim)
        before = lax.ppermute(last, axis, up)
        after = lax.ppermute(initial, axis, down)
        x = jnp.concatenate([before, x, after], axis=dim)
    return x


def modulate(rows_in, norm_gain, shift_vec, scale_vec):
    values = rows_in.astype(jnp.float32)
    normed = values * lax.rsqrt(jnp.mean(values * values, axis=-1, keepdims=True) + EPS)
    return (normed * norm_gain * (1.0 + scale_vec) + shift_vec).astype(jnp.bfloat16)


def head_norm(projected, head_gain):
    row_count = projected.shape[0]
    split_heads = projected.reshape(row_count, -1, head_gain.shape[0])
    normed = split_heads * lax.rsqrt(
        jnp.mean(split_heads * split_heads, axis=-1, keepdims=True) + EPS
    )
    return (normed * head_gain).astype(jnp.bfloat16).reshape(row_count, -1)


def per_device_plain(
    latent,
    context,
    condition,
    ctx_condition,
    shift_weight,
    scale_weight,
    gate_weight,
    norm_gain,
    query_weight,
    key_weight,
    value_weight,
    query_gain,
    key_gain,
    offset_bias,
    out_weight,
):
    activations = jax.nn.silu(jnp.stack([condition, ctx_condition])).astype(jnp.bfloat16)
    part_shift = jnp.dot(activations, shift_weight, preferred_element_type=jnp.float32)
    part_scale = jnp.dot(activations, scale_weight, preferred_element_type=jnp.float32)
    part_gate = jnp.dot(activations[:1], gate_weight, preferred_element_type=jnp.float32)
    block_cols = shift_weight.shape[1]
    first_col = lax.axis_index("tp") * block_cols

    def spread(piece_part):
        padded_vec = jnp.zeros((piece_part.shape[0], block_cols * lax.axis_size("tp")), jnp.float32)
        return lax.dynamic_update_slice_in_dim(padded_vec, piece_part, first_col, 1)

    shift_vec, scale_vec, gate_vec = lax.psum(
        (spread(part_shift), spread(part_scale), spread(part_gate)), ("sp", "tp")
    )
    hidden = modulate(latent, norm_gain, shift_vec[0], scale_vec[0])
    queries = head_norm(
        jnp.dot(hidden, query_weight, preferred_element_type=jnp.float32), query_gain
    )
    keys_lat = head_norm(jnp.dot(hidden, key_weight, preferred_element_type=jnp.float32), key_gain)
    values_lat = jnp.dot(hidden, value_weight, preferred_element_type=jnp.float32).astype(
        jnp.bfloat16
    )
    ctx_hidden = modulate(
        lax.all_gather(context, "sp", axis=0, tiled=True), norm_gain, shift_vec[1], scale_vec[1]
    )
    ctx_keys = head_norm(
        jnp.dot(ctx_hidden, key_weight, preferred_element_type=jnp.float32), key_gain
    )
    ctx_values = jnp.dot(ctx_hidden, value_weight, preferred_element_type=jnp.float32).astype(
        jnp.bfloat16
    )
    ctx_pairs = jnp.concatenate([ctx_keys, ctx_values], axis=1)
    col_width = keys_lat.shape[1]
    heads_dev = col_width // HEAD_DIM
    local_rows = keys_lat.shape[0] // GRID_W
    halo_rows = WIN_ROWS // 2
    window_keys = WIN_ROWS * GRID_W
    key_value = jnp.concatenate([keys_lat, values_lat], axis=1).reshape(
        local_rows, GRID_W, 2 * col_width
    )
    padded = extended(key_value, (("sp", 0),), halo_rows)
    first_row = lax.axis_index("sp") * local_rows
    total_rows = local_rows * lax.axis_size("sp")
    global_rows = first_row + jnp.arange(local_rows, dtype=jnp.int32)
    band_start = jnp.clip(global_rows - halo_rows, 0, total_rows - WIN_ROWS)
    band_global = band_start[:, None] + jnp.arange(WIN_ROWS, dtype=jnp.int32)[None, :]
    banded = jnp.take(padded, band_global - first_row + halo_rows, axis=0)
    key_band = banded[..., :col_width].reshape(local_rows, window_keys, heads_dev, HEAD_DIM)
    value_band = banded[..., col_width:].reshape(local_rows, window_keys, heads_dev, HEAD_DIM)
    row_steps = band_global - global_rows[:, None] + WIN_ROWS - 1
    row_hot = (
        row_steps[:, :, None] == jnp.arange(2 * WIN_ROWS - 1, dtype=jnp.int32)[None, None, :]
    ).astype(jnp.float32)
    column_ids = jnp.arange(GRID_W, dtype=jnp.int32)
    col_steps = (
        jnp.clip(column_ids[None, :] - column_ids[:, None], 1 - WIN_COLS, WIN_COLS - 1)
        + WIN_COLS
        - 1
    )
    col_hot = (
        col_steps[:, :, None] == jnp.arange(2 * WIN_COLS - 1, dtype=jnp.int32)[None, None, :]
    ).astype(jnp.float32)
    col_start = jnp.clip(column_ids - WIN_COLS // 2, 0, GRID_W - WIN_COLS)
    col_open = (column_ids[None, :] >= col_start[:, None]) & (
        column_ids[None, :] < col_start[:, None] + WIN_COLS
    )
    col_table = jnp.einsum("hab,qkb->haqk", offset_bias, col_hot, precision=lax.Precision.HIGHEST)
    col_table = jnp.where(col_open[None, None, :, :], col_table, -jnp.inf)
    offset_terms = jnp.einsum(
        "rja,haqk->hrqjk",
        row_hot,
        jnp.where(col_open[None, None], col_table, 0.0),
        precision=lax.Precision.HIGHEST,
    )
    offset_terms = jnp.where(col_open[None, None, :, None, :], offset_terms, -jnp.inf)
    offset_terms = offset_terms.reshape(heads_dev, local_rows, GRID_W, window_keys)
    score_scale = HEAD_DIM ** (-0.5)
    q_grid = queries.reshape(local_rows, GRID_W, heads_dev, HEAD_DIM)
    scores = (
        jnp.einsum("rqhd,rnhd->hrqn", q_grid, key_band, preferred_element_type=jnp.float32)
        * score_scale
        + offset_terms
    )
    ctx_count = ctx_pairs.shape[0]
    ctx_keys_all = ctx_pairs[:, :col_width].reshape(ctx_count, heads_dev, HEAD_DIM)
    ctx_values_all = ctx_pairs[:, col_width:].reshape(ctx_count, heads_dev, HEAD_DIM)
    ctx_scores = (
        jnp.einsum("rqhd,nhd->hrqn", q_grid, ctx_keys_all, preferred_element_type=jnp.float32)
        * score_scale
    )
    row_max = jnp.maximum(jnp.max(scores, axis=3), jnp.max(ctx_scores, axis=3))
    local_exp = jnp.exp(scores - row_max[..., None])
    ctx_exp = jnp.exp(ctx_scores - row_max[..., None])
    denominator = jnp.sum(local_exp, axis=3) + jnp.sum(ctx_exp, axis=3)
    local_weights = (local_exp / denominator[..., None]).astype(jnp.bfloat16)
    ctx_weights = (ctx_exp / denominator[..., None]).astype(jnp.bfloat16)
    combined = jnp.einsum(
        "hrqn,rnhd->rqhd", local_weights, value_band, preferred_element_type=jnp.float32
    ) + jnp.einsum(
        "hrqn,nhd->rqhd", ctx_weights, ctx_values_all, preferred_element_type=jnp.float32
    )
    attended = combined.astype(jnp.bfloat16).reshape(local_rows * GRID_W, col_width)
    partial_value = jnp.dot(attended, out_weight, preferred_element_type=jnp.float32)
    branch = lax.psum(partial_value.astype(jnp.bfloat16), "tp").astype(jnp.float32)
    return (latent.astype(jnp.float32) + gate_vec[0] * branch).astype(jnp.bfloat16)


MESH = pl.DeviceIdType.MESH
MASKED = -1e30
LANES = 128
F32 = jnp.float32
BF16 = jnp.bfloat16


def fused_kernel(
    n_sp,
    n_tp,
    latent,
    context,
    shift_w,
    scale_w,
    gate_w,
    query_w,
    key_w,
    value_w,
    out_w,
    cond,
    ctx_cond,
    norm_gain,
    query_gain,
    key_gain,
    bias_in,
    out,
    cond_v,
    ctx_cond_v,
    norm_gain_v,
    query_gain_v,
    key_gain_v,
    bias_v,
    x_in,
    x_norm,
    hid,
    w_mod,
    w_qkv,
    w_out,
    mod_sp,
    mod_tp,
    part_kv,
    part_q,
    gate_sp,
    gate_tp,
    acc,
    q_stage,
    k_stage,
    v_stage,
    ck_stage,
    cv_stage,
    q_all,
    k_all,
    v_all,
    ctx_k,
    ctx_v,
    bias_pad,
    bias_lines,
    table,
    q_heads,
    scores,
    tops,
    sums,
    scores_ctx,
    weights,
    sums_ctx,
    att_slab,
    att,
    local_sem,
    mod_send,
    mod_recv,
    modt_send,
    modt_recv,
    gate_send,
    gate_recv,
    gatet_send,
    gatet_recv,
    pair_send,
    pair_recv,
    halo_send,
    halo_recv,
    ctx_send,
    ctx_recv,
    end_send,
    wo_send,
    wo_recv,
    att_send,
    att_recv,
):
    me_s, me_t = lax.axis_index("sp"), lax.axis_index("tp")
    rows, d = latent.shape
    c_rows = context.shape[0]
    width = key_w.shape[1]
    heads = width // HEAD_DIM
    block = shift_w.shape[1]
    blocks = block // 128
    l_rows = rows // GRID_W
    halo = WIN_ROWS // 2
    win = WIN_ROWS * GRID_W
    core = lax.rem(me_t, 2)
    chip = lax.div(me_t, 2)
    partner = me_t + 1 - 2 * core
    far = 2 * (1 - chip) + core
    far_partner = 2 * (1 - chip) + 1 - core
    side = lax.rem(me_s, 2)
    slab = lax.div(me_s, 2)
    mate = me_s + 1 - 2 * side
    last_slab = n_sp // 2 - 1
    half = width // 2
    half_heads = heads // 2

    def remote(src, dst, send, recv, s, t):
        return pltpu.make_async_remote_copy(
            src_ref=src, dst_ref=dst, send_sem=send, recv_sem=recv,
            device_id=(s, t), device_id_type=MESH,
        )

    barrier = pltpu.get_barrier_semaphore()
    for k in range(1, n_sp):
        pl.semaphore_signal(
            barrier, inc=1, device_id=(lax.rem(me_s + k, n_sp), me_t), device_id_type=MESH
        )
    for k in range(1, n_tp):
        pl.semaphore_signal(
            barrier, inc=1, device_id=(me_s, lax.rem(me_t + k, n_tp)), device_id_type=MESH
        )
    pl.semaphore_signal(barrier, inc=1, device_id=(mate, far), device_id_type=MESH)

    loads = [
        (shift_w, w_mod.at[0]),
        (scale_w, w_mod.at[1]),
        (gate_w, w_mod.at[2]),
        (context, x_in.at[pl.ds(0, c_rows)]),
        (latent, x_in.at[pl.ds(c_rows, rows)]),
        (key_w, w_qkv.at[:, pl.ds(0, width)]),
        (value_w, w_qkv.at[:, pl.ds(width, width)]),
        (query_w, w_qkv.at[:, pl.ds(2 * width, width)]),
        (out_w, w_out.at[me_t]),
        (cond, cond_v),
        (ctx_cond, ctx_cond_v),
        (norm_gain, norm_gain_v),
        (query_gain, query_gain_v),
        (key_gain, key_gain_v),
        (bias_in, bias_v),
    ]
    copies = [pltpu.make_async_copy(a, b, local_sem.at[i]) for i, (a, b) in enumerate(loads)]
    for i in (9, 10, 0, 1, 2, 11, 12, 13, 14, 3, 4):
        copies[i].start()

    def silu(v):
        return v / (1.0 + jnp.exp(-v))

    two = (16, cond.shape[1])
    row_id = lax.broadcasted_iota(jnp.int32, two, 0)
    copies[9].wait()
    copies[10].wait()
    act0 = jnp.broadcast_to(silu(cond_v[...]), two)
    act1 = jnp.broadcast_to(silu(ctx_cond_v[...]), two)

    def placed(first, second):
        picked = jnp.where(row_id == first, act0, 0.0)
        if second is not None:
            picked = jnp.where(row_id == second, act1, picked)
        return picked.astype(BF16)

    part = jnp.zeros((16, block), F32)
    for i in range(2):
        copies[i].wait()
        part += jnp.dot(placed(2 * i, 2 * i + 1), w_mod[i], preferred_element_type=F32)
    for b in range(blocks):
        mod_sp[me_s, 4 * b : 4 * b + 4, :] = part[:4, b * 128 : (b + 1) * 128]
    pl.semaphore_wait(barrier, n_sp + n_tp - 1)
    sends = []

    def share_sp(buf, send, recv):
        for k in range(1, n_sp):
            peer = lax.rem(me_s + k, n_sp)
            c = remote(buf.at[me_s], buf.at[me_s], send.at[k], recv.at[me_s], peer, me_t)
            c.start()
            sends.append(c)

    def sum_sp(buf, send, recv):
        for k in range(1, n_sp):
            peer = lax.rem(me_s + k, n_sp)
            remote(buf.at[peer], buf.at[peer], send.at[k], recv.at[peer], peer, me_t).wait_recv()
        total = buf[0]
        for k in range(1, n_sp):
            total = total + buf[k]
        return total

    def share_tp(buf, send, recv):
        for k in range(1, n_tp):
            peer = lax.rem(me_t + k, n_tp)
            c = remote(buf.at[me_t], buf.at[me_t], send.at[k], recv.at[me_t], me_s, peer)
            c.start()
            sends.append(c)

    def wait_tp(buf, send, recv):
        for k in range(1, n_tp):
            peer = lax.rem(me_t + k, n_tp)
            remote(buf.at[peer], buf.at[peer], send.at[k], recv.at[peer], me_s, peer).wait_recv()

    share_sp(mod_sp, mod_send, mod_recv)
    for i in (5, 6, 7, 8):
        copies[i].start()
    copies[2].wait()
    gate_part = jnp.dot(placed(0, None), w_mod[2], preferred_element_type=F32)
    for b in range(blocks):
        gate_sp[me_s, b : b + 1, :] = gate_part[:1, b * 128 : (b + 1) * 128]

    piece = width // 16
    n_cross, n_direct = 3, 4
    n_pieces = 2 * n_cross + n_direct
    early = (0, n_cross)
    later = [c + o for c in range(1, n_cross) for o in (0, n_cross)]
    later = later + list(range(2 * n_cross, n_pieces))
    z_side = lax.rem(slab, 2)
    z_mate = me_s + 2 - 4 * z_side

    def wo_rows(c, away_from):
        if c < n_cross:
            start = (side + away_from - 2 * side * away_from) * n_cross * piece + c * piece
        elif c < 2 * n_cross:
            start = (
                2 * n_cross * piece
                + (z_side + away_from - 2 * z_side * away_from) * n_cross * piece
                + (c - n_cross) * piece
            )
        else:
            start = (2 * n_cross + c) * piece
        return pl.ds(pl.multiple_of(start, piece), piece)

    def wo_copy(kind, c, source, shard, rows_at, s, t):
        return remote(
            source.at[rows_at], w_out.at[shard, rows_at],
            wo_send.at[kind, c], wo_recv.at[kind, c], s, t,
        )

    def begin(c):
        c.start()
        sends.append(c)

    def wo_far(c):
        return wo_copy(0, c, out_w, me_t, wo_rows(c, 0), me_s, far)

    def wo_forward(c):
        at_rows = wo_rows(c, 0)
        came = w_out.at[far]
        wo_copy(0, c, came, far, at_rows, me_s, far).wait_recv()
        begin(wo_copy(1, c, came, far, at_rows, me_s, partner))
        if c < 2 * n_cross:
            begin(wo_copy(2, c, came, far, at_rows, mate if c < n_cross else z_mate, me_t))

    def wo_cross(c):
        at_rows = wo_rows(c, 1)
        came = w_out.at[far]
        wo_copy(2, c, came, far, at_rows, mate, me_t).wait_recv()
        begin(wo_copy(3, c, came, far, at_rows, me_s, partner))

    def wo_finish_far():
        for c in range(n_pieces):
            wo_copy(
                1, c, w_out.at[far_partner], far_partner, wo_rows(c, 0), me_s, partner
            ).wait_recv()
        for c in range(2 * n_cross):
            wo_copy(
                3, c, w_out.at[far_partner], far_partner, wo_rows(c, 1), me_s, partner
            ).wait_recv()

    def wo_partner():
        return remote(
            out_w, w_out.at[me_t], wo_send.at[4, 0], wo_recv.at[4, 0], me_s, partner
        )

    for c in early:
        begin(wo_far(c))

    copies[3].wait()
    copies[4].wait()
    copies[11].wait()
    step = 32

    def norm_rows(i, carry):
        at = pl.ds(pl.multiple_of(i * step, step), step)
        v = x_in[at, :].astype(F32)
        r = lax.rsqrt(jnp.mean(v * v, axis=-1, keepdims=True) + EPS)
        x_norm[at, :] = v * r * norm_gain_v[...]
        return carry

    lax.fori_loop(0, (rows + c_rows) // step, norm_rows, 0)

    pair = 2 * GRID_W
    q_col = lax.broadcasted_iota(jnp.int32, (GRID_W, pair), 0)
    k_col = lax.broadcasted_iota(jnp.int32, (GRID_W, pair), 1) % GRID_W
    col0 = jnp.clip(q_col - WIN_COLS // 2, 0, GRID_W - WIN_COLS)
    col_open = (k_col >= col0) & (k_col < col0 + WIN_COLS)
    n_pairs = 2 * WIN_ROWS - 2
    copies[14].wait()
    bias_pad[...] = jnp.zeros_like(bias_pad)
    for h in range(heads):
        bias_pad[h, : 2 * WIN_ROWS - 1, : 2 * WIN_COLS - 1] = bias_v[:, h, :]
    for h in range(half_heads):
        head = side * half_heads + h
        upper = pltpu.roll(bias_pad[head, 1 : n_pairs + 1, :], GRID_W, 1)
        bias_lines[h, :n_pairs, :] = bias_pad[head, :n_pairs, :] + upper
        for a in range(n_pairs):
            line = jnp.broadcast_to(bias_lines[h, a : a + 1, :], (GRID_W, pair))
            rolled = pltpu.roll(line, pair - (WIN_COLS - 1), 1, stride=1, stride_axis=0)
            table[a, h * GRID_W : (h + 1) * GRID_W, :] = jnp.where(col_open, rolled, MASKED)

    mod_tp[me_t] = sum_sp(mod_sp, mod_send, mod_recv)
    share_tp(mod_tp, modt_send, modt_recv)
    for c in later:
        begin(wo_far(c))
    share_sp(gate_sp, gate_send, gate_recv)

    def wait_mod(peer):
        remote(
            mod_tp.at[peer], mod_tp.at[peer], modt_send.at[1], modt_recv.at[peer], me_s, peer
        ).wait_recv()

    pair_cols = 2 * block

    def vec(which, r):
        return jnp.concatenate(
            [
                mod_tp[2 * which + j, 4 * b + r : 4 * b + r + 1, :]
                for j in range(2)
                for b in range(blocks)
            ],
            axis=1,
        )

    def cols_of(which):
        return pl.ds(pl.multiple_of(which * pair_cols, pair_cols), pair_cols)

    def modulate_rows(which, first, count, shift, scale):
        def body(i, carry):
            at = pl.ds(pl.multiple_of(first + i * step, step), step)
            hid[at, cols_of(which)] = (x_norm[at, cols_of(which)] * scale + shift).astype(BF16)
            return carry

        lax.fori_loop(0, count // step, body, 0)

    def modulate_pair(which):
        modulate_rows(which, 0, c_rows, vec(which, 1), 1.0 + vec(which, 3))
        modulate_rows(which, c_rows, rows, vec(which, 0), 1.0 + vec(which, 2))

    def hidden_dot(which, start_row, start_col, count_col):
        return jnp.dot(
            hid[start_row:, cols_of(which)],
            w_qkv[cols_of(which), start_col : start_col + count_col],
            preferred_element_type=F32,
        )

    wait_mod(partner)
    modulate_pair(chip)
    for i in (5, 6, 7):
        copies[i].wait()
    part_kv[...] = hidden_dot(chip, 0, 0, 2 * width)
    part_q[...] = hidden_dot(chip, c_rows, 2 * width, width)
    for c in early:
        wo_forward(c)
    wait_mod(far)
    wait_mod(far_partner)
    head_row = lax.broadcasted_iota(jnp.int32, (width, width), 0) // HEAD_DIM
    head_col = lax.broadcasted_iota(jnp.int32, (width, width), 1) // HEAD_DIM
    same_head = (head_row == head_col).astype(BF16)
    copies[12].wait()
    copies[13].wait()

    def head_scale(p, gain):
        squares = p * p
        high = squares.astype(BF16)
        low = (squares - high.astype(F32)).astype(BF16)
        mean = jnp.dot(high, same_head, preferred_element_type=F32)
        mean = mean + jnp.dot(low, same_head, preferred_element_type=F32)
        mean = mean * (1.0 / HEAD_DIM)
        wide_gain = jnp.concatenate([gain[...]] * heads, axis=1)
        return (p * lax.rsqrt(mean + EPS) * wide_gain).astype(BF16)

    own = pl.ds(rows + pl.multiple_of(side * rows, rows), rows)
    other = pl.ds(rows + pl.multiple_of((1 - side) * rows, rows), rows)

    def split(stage, value):
        for h in range(2):
            stage[h] = value[:, h * half : (h + 1) * half]

    def trade(index, stage, block_all, at):
        c = remote(
            stage.at[1 - side], block_all.at[at], pair_send.at[index], pair_recv.at[index],
            mate, me_t,
        )
        c.start()
        sends.append(c)
        return c

    n_z = n_sp // 2
    z_order = tuple(range(2, n_z)) + (1,)

    def ctx_copy(index, slot, source, shard, block_ctx, s):
        return remote(
            source, block_ctx.at[shard], ctx_send.at[index, slot], ctx_recv.at[index, shard],
            s, me_t,
        )

    at_end = (slab == 0) | (slab == last_slab)
    sends_when = []

    def along_z(index, slot, source, shard, block_ctx, all_direct=False):
        for k in z_order:
            peer = lax.rem(slab + k, n_z)
            c = ctx_copy(index, slot + k, source, shard, block_ctx, 2 * peer + side)
            low = (peer == 0) & (slab >= 2)
            high = (peer == last_slab) & (slab <= last_slab - 2)
            if all_direct:
                begin(c)
                continue
            direct = jnp.logical_not(low | high)
            pl.when(direct)(c.start)
            sends_when.append((direct, c))

    z_pair = lax.div(slab, 2)

    def relay_end(of_side):
        def body():
            for j in range(2):
                shard = 2 * (2 * (1 - z_pair) + j) + of_side
                for index, block_ctx in enumerate((ctx_k, ctx_v)):
                    ctx_copy(index, 0, block_ctx.at[shard], shard, block_ctx, shard).wait_recv()
                    end_copy(index, shard, block_ctx).start()

        pl.when(jnp.logical_not(at_end))(body)
        for j in range(2):
            shard = 2 * (2 * (1 - z_pair) + j) + of_side
            for index, block_ctx in enumerate((ctx_k, ctx_v)):
                sends_when.append((jnp.logical_not(at_end), end_copy(index, shard, block_ctx)))

    def end_copy(index, shard, block_ctx):
        return remote(
            block_ctx.at[shard], block_ctx.at[shard],
            end_send.at[index, shard], ctx_recv.at[index, shard],
            2 * z_pair * last_slab + side, me_t,
        )


    def relay_ctx(index, block_ctx):
        ctx_copy(index, 0, block_ctx.at[mate], mate, block_ctx, mate).wait_recv()
        along_z(index, n_z - 1, block_ctx.at[mate], mate, block_ctx, True)

    lower = rows - GRID_W

    def halo_copies(index, block_all):
        down = remote(
            block_all.at[pl.ds(rows, lower)], block_all.at[pl.ds(3 * rows, lower)],
            halo_send.at[index, 0], halo_recv.at[index, 0], me_s - 2, me_t,
        )
        up = remote(
            block_all.at[pl.ds(2 * rows, rows)], block_all.at[pl.ds(0, rows)],
            halo_send.at[index, 1], halo_recv.at[index, 1], me_s + 2, me_t,
        )
        return down, up

    def halo_start(mine, index, block_all):
        down, up = halo_copies(index, block_all)
        is_low = side == 0 if mine else side == 1

        @pl.when(is_low & (slab > 0))
        def _():
            down.start()

        @pl.when(jnp.logical_not(is_low) & (slab < last_slab))
        def _():
            up.start()

    away = 1 - chip
    modulate_rows(away, 0, c_rows, vec(away, 1), 1.0 + vec(away, 3))
    ctx_both = part_kv[:c_rows, :] + jnp.dot(
        hid[:c_rows, cols_of(away)], w_qkv[cols_of(away), : 2 * width], preferred_element_type=F32
    )
    ctx_keys = head_scale(ctx_both[:, :width], key_gain_v)
    ctx_values = ctx_both[:, width:].astype(BF16)
    split(ck_stage, ctx_keys)
    split(cv_stage, ctx_values)
    for index, (stage, block_ctx) in enumerate(((ck_stage, ctx_k), (cv_stage, ctx_v))):
        begin(ctx_copy(index, 0, stage.at[1 - side], me_s, block_ctx, mate))
        along_z(index, 0, stage.at[side], me_s, block_ctx)
        block_ctx[me_s] = stage[side]
    modulate_rows(away, c_rows, rows, vec(away, 0), 1.0 + vec(away, 2))
    both = part_kv[c_rows:, :] + hidden_dot(away, c_rows, 0, 2 * width)
    keys = head_scale(both[:, :width], key_gain_v)
    split(k_stage, keys)
    k_trade = trade(0, k_stage, k_all, own)
    k_all[own, :] = k_stage[side]
    halo_start(True, 0, k_all)
    split(v_stage, both[:, width:].astype(BF16))
    v_trade = trade(1, v_stage, v_all, own)
    v_all[own, :] = v_stage[side]
    halo_start(True, 1, v_all)
    queries = head_scale(
        part_q[...] + hidden_dot(away, c_rows, 2 * width, width), query_gain_v
    ) * jnp.asarray(HEAD_DIM ** (-0.5), BF16)
    split(q_stage, queries)
    q_own = pl.ds(pl.multiple_of(side * rows, rows), rows)
    q_trade = trade(2, q_stage, q_all, q_own)
    q_all[q_own, :] = q_stage[side]
    begin(wo_partner())
    gate_tp[me_t] = sum_sp(gate_sp, gate_send, gate_recv)
    share_tp(gate_tp, gatet_send, gatet_recv)
    relay_ctx(0, ctx_k)
    relay_ctx(1, ctx_v)
    relay_end(side)
    k_trade.wait_recv()
    halo_start(False, 0, k_all)
    for c in range(1, n_cross):
        wo_forward(c)
    v_trade.wait_recv()
    halo_start(False, 1, v_all)
    def halo_wait(theirs_need):
        below = side == 0 if theirs_need else side == 1
        for index, block_all in enumerate((k_all, v_all)):
            down, up = halo_copies(index, block_all)

            @pl.when(below & (slab < last_slab))
            def _():
                down.wait_recv()

            @pl.when(jnp.logical_not(below) & (slab > 0))
            def _():
                up.wait_recv()

    lane_head = lax.broadcasted_iota(jnp.int32, (GRID_W, half), 1) // HEAD_DIM
    masks = [(lane_head == h).astype(F32) for h in range(half_heads)]
    contract_last = (((1,), (1,)), ((), ()))
    stack = half_heads * GRID_W
    ones = jnp.ones((win, 128), BF16)

    def score_local(i, held_at, slot):
        start = jnp.where(
            slab == 0,
            jnp.maximum(i, halo),
            jnp.where(slab == last_slab, jnp.minimum(i, halo), i),
        )
        if last_slab == 0:
            start = jnp.int32(halo)
        at = pl.ds(pl.multiple_of(start * GRID_W, GRID_W), win)
        qi = q_all[pl.ds(pl.multiple_of(i * GRID_W, GRID_W), GRID_W), :].astype(F32)
        qs = jnp.concatenate([(qi * m).astype(BF16) for m in masks], axis=0)
        q_heads[held_at] = qs
        s = lax.dot_general(qs, k_all[at, :], contract_last, preferred_element_type=F32)
        first = start - i + WIN_ROWS - 1 - halo
        s = s + jnp.concatenate([table[first + 2 * m] for m in range(WIN_ROWS // 2)], axis=1)
        scores[slot] = s
        return at, jnp.max(s, axis=1, keepdims=True)

    def weigh_local(held_at, slot, at, top):
        e = jnp.exp(scores[slot] - top)
        tops[held_at] = jnp.broadcast_to(top, (stack, 128))
        values_at = jnp.concatenate([v_all[at, :], ones], axis=1)
        sums[held_at] = jnp.dot(e.astype(BF16), values_at, preferred_element_type=F32)

    def local_half(which, base):
        first = which * l_rows
        held = score_local(first, base, 0)
        for i in range(l_rows):
            later = None
            if i + 1 < l_rows:
                later = score_local(first + i + 1, base + i + 1, (i + 1) % 2)
            weigh_local(base + i, i % 2, *held)
            held = later

    def ctx_wait(wait_near):
        for index, block_ctx in enumerate((ctx_k, ctx_v)):
            for s in range(n_sp):

                relayed = jnp.logical_not(at_end) & (z_pair != s // 4) & (side == s % 2)

                wanted = (z_pair == s // 4) if wait_near else (z_pair != s // 4)

                @pl.when((s != me_s) & (s != mate) & jnp.logical_not(relayed) & wanted)
                def _():
                    ctx_copy(index, 0, block_ctx.at[s], s, block_ctx, s).wait_recv()

    top_head = lax.broadcasted_iota(jnp.int32, (GRID_W, half), 1) // HEAD_DIM
    half_stack = l_rows * stack
    n_ctx = n_sp * c_rows
    ctx_ones = jnp.ones((n_ctx, 128), BF16)

    n_part = n_ctx // 2
    shards_part = n_sp // 2

    def ctx_scores(base, first_shard, n_keys, exp_all):
        shards = pl.ds(first_shard, n_keys // c_rows)
        qs = q_heads[base : base + l_rows].reshape(half_stack, half)
        scores_ctx[:, :n_keys] = lax.dot_general(
            qs, ctx_k[shards].reshape(n_keys, half), contract_last, preferred_element_type=F32
        )
        fades = []
        for i in range(l_rows):
            at_rows = slice(i * stack, (i + 1) * stack)
            s = scores_ctx[at_rows, :n_keys]
            old = tops[base + i]
            top = jnp.maximum(old, jnp.max(s, axis=1, keepdims=True))
            fade = jnp.exp(old - top)
            fades.append(jnp.concatenate([fade] * ((half + 128) // 128), axis=1))
            if exp_all:
                tops[base + i] = top
            wide_top = jnp.concatenate([top] * (n_keys // 128), axis=1)
            weights[at_rows, :n_keys] = jnp.exp(s - wide_top).astype(BF16)
        values_ctx = jnp.concatenate(
            [ctx_v[shards].reshape(n_keys, half), ctx_ones[:n_keys]], axis=1
        )
        sums_ctx[...] = jnp.dot(
            weights[:, :n_keys], values_ctx, preferred_element_type=F32
        )
        return fades

    def ctx_near(base):
        fades = ctx_scores(base, shards_part * z_pair, n_part, True)
        for i in range(l_rows):
            at_rows = slice(i * stack, (i + 1) * stack)
            sums[base + i] = sums_ctx[at_rows, :] + sums[base + i] * fades[i]

    def ctx_last(base, store, everything):
        if everything:
            fades = ctx_scores(base, 0, n_ctx, False)
        else:
            fades = ctx_scores(base, shards_part * (1 - z_pair), n_part, False)
        for i in range(l_rows):
            at_rows = slice(i * stack, (i + 1) * stack)
            o = sums_ctx[at_rows, :] + sums[base + i] * fades[i]
            up, down = o[:, :half], o[:, half:]
            num, den = up[:GRID_W], down[:GRID_W]
            for h in range(1, half_heads):
                part_h = slice(h * GRID_W, (h + 1) * GRID_W)
                num = jnp.where(top_head == h, up[part_h], num)
                den = jnp.where(top_head == h, down[part_h], den)
            store(i, (num / den).astype(BF16))

    def att_copy(index, source, dest, s, t):
        return remote(source, dest, att_send.at[index], att_recv.at[index], s, t)

    def store_theirs(i, value):
        att_slab[i * GRID_W : (i + 1) * GRID_W, :] = value

    def store_mine(i, value):
        att[me_t, side, i * GRID_W : (i + 1) * GRID_W, :] = value

    def local_mine():
        halo_wait(False)
        local_half(side, l_rows)

    n_early = len(sends)
    for c in range(n_cross + 1, 2 * n_cross):
        wo_forward(c)
    no_halo = ((slab == 0) & (side == 0)) | ((slab == last_slab) & (side == 1))
    pl.when(no_halo)(local_mine)
    q_trade.wait_recv()
    halo_wait(True)
    local_half(1 - side, 0)
    ctx_wait(True)
    ctx_near(0)
    @pl.when(no_halo)
    def _():
        ctx_near(l_rows)

    ctx_wait(False)
    ctx_last(0, store_theirs, False)
    begin(att_copy(0, att_slab, att.at[me_t, side], mate, far))
    begin(att_copy(1, att_slab, att.at[me_t, side], mate, me_t))
    @pl.when(no_halo)
    def _():
        ctx_last(l_rows, store_mine, False)

    @pl.when(jnp.logical_not(no_halo))
    def _():
        local_mine()
        ctx_last(l_rows, store_mine, True)

    begin(att_copy(2, att.at[me_t, side], att.at[me_t, side], me_s, far))
    begin(att_copy(3, att.at[me_t, side], att.at[me_t, side], me_s, partner))

    def arrived(index, shard, part_of):
        return att_copy(index, att.at[shard, part_of], att.at[shard, part_of], me_s, partner)

    def pass_on(index, onto, shard, part_of):
        arrived(index, shard, part_of).wait_recv()
        begin(arrived(onto, shard, part_of))

    for c in range(2 * n_cross, n_pieces):
        wo_forward(c)
    for c in range(2 * n_cross):
        wo_cross(c)
    wait_tp(gate_tp, gatet_send, gatet_recv)
    gate = jnp.concatenate(
        [gate_tp[j, b : b + 1, :] for j in range(n_tp) for b in range(blocks)], axis=1
    )
    copies[8].wait()
    cols = 512

    def project(groups, first_pass, last_pass):
        heads_of = [jnp.concatenate([att[j, 0], att[j, 1]], axis=1) for j in groups]
        for n in range(d // cols):
            at = slice(n * cols, (n + 1) * cols)
            total = None if first_pass else acc[:, at]
            for j, lhs in zip(groups, heads_of):
                term = jnp.dot(lhs, w_out[j, :, at], preferred_element_type=F32)
                term = term.astype(BF16).astype(F32)
                total = term if total is None else total + term
            if last_pass:
                base = x_in[c_rows:, at].astype(F32)
                out[:, at] = (base + gate[:, at] * total).astype(BF16)
            else:
                acc[:, at] = total

    for c in sends[:n_early]:
        c.wait_send()
    for condition, c in sends_when:
        pl.when(condition)(c.wait_send)
    for index, block_all in enumerate((k_all, v_all)):
        down, up = halo_copies(index, block_all)

        @pl.when(slab > 0)
        def _():
            down.wait_send()

        @pl.when(slab < last_slab)
        def _():
            up.wait_send()
    pass_on(1, 5, me_t, 1 - side)
    project((me_t,), True, False)
    pass_on(0, 4, far, 1 - side)
    pass_on(2, 6, far, side)
    project((far,), False, False)
    remote(
        w_out.at[partner], w_out.at[partner], wo_send.at[4, 0], wo_recv.at[4, 0], me_s, partner
    ).wait_recv()
    arrived(3, partner, side).wait_recv()
    arrived(5, partner, 1 - side).wait_recv()
    project((partner,), False, False)
    wo_finish_far()
    arrived(4, far_partner, 1 - side).wait_recv()
    arrived(6, far_partner, side).wait_recv()
    project((far_partner,), False, True)

    for c in sends[n_early:]:
        c.wait_send()


def per_device(
    latent,
    context,
    condition,
    ctx_condition,
    shift_weight,
    scale_weight,
    gate_weight,
    norm_gain,
    query_weight,
    key_weight,
    value_weight,
    query_gain,
    key_gain,
    offset_bias,
    out_weight,
):
    n_sp, n_tp = lax.axis_size("sp"), lax.axis_size("tp")
    rows, d = latent.shape
    c_rows = context.shape[0]
    width = key_weight.shape[1]
    heads = width // HEAD_DIM
    block = shift_weight.shape[1]
    n_pairs = 2 * WIN_ROWS - 2
    half = width // 2
    half_heads = heads // 2
    blocks = block // 128
    l_rows = rows // GRID_W
    stack = half_heads * GRID_W
    any_spec = pl.BlockSpec(memory_space=pl.ANY)
    vmem_spec = pl.BlockSpec(memory_space=pltpu.VMEM)
    dma = pltpu.SemaphoreType.DMA
    return pl.pallas_call(
        functools.partial(fused_kernel, n_sp, n_tp),
        out_shape=pltpu.VMEM((rows, d), BF16),
        in_specs=[any_spec] * 15,
        out_specs=vmem_spec,
        scratch_shapes=[
            pltpu.VMEM((1, condition.shape[0]), F32),
            pltpu.VMEM((1, condition.shape[0]), F32),
            pltpu.VMEM((1, d), F32),
            pltpu.VMEM((1, HEAD_DIM), F32),
            pltpu.VMEM((1, HEAD_DIM), F32),
            pltpu.VMEM((2 * WIN_ROWS - 1, heads, 2 * WIN_COLS - 1), F32),
            pltpu.VMEM((rows + c_rows, d), BF16),
            pltpu.VMEM((rows + c_rows, d), F32),
            pltpu.VMEM((rows + c_rows, d), BF16),
            pltpu.VMEM((3, shift_weight.shape[0], block), BF16),
            pltpu.VMEM((d, 3 * width), BF16),
            pltpu.VMEM((n_tp, width, d), BF16),
            pltpu.VMEM((n_sp, 4 * blocks, 128), F32),
            pltpu.VMEM((n_tp, 4 * blocks, 128), F32),
            pltpu.VMEM((rows + c_rows, 2 * width), F32),
            pltpu.VMEM((rows, width), F32),
            pltpu.VMEM((n_sp, blocks, 128), F32),
            pltpu.VMEM((n_tp, blocks, 128), F32),
            pltpu.VMEM((rows, d), F32),
            pltpu.VMEM((2, rows, half), BF16),
            pltpu.VMEM((2, rows, half), BF16),
            pltpu.VMEM((2, rows, half), BF16),
            pltpu.VMEM((2, c_rows, half), BF16),
            pltpu.VMEM((2, c_rows, half), BF16),
            pltpu.VMEM((2 * rows, half), BF16),
            pltpu.VMEM((4 * rows, half), BF16),
            pltpu.VMEM((4 * rows, half), BF16),
            pltpu.VMEM((n_sp, c_rows, half), BF16),
            pltpu.VMEM((n_sp, c_rows, half), BF16),
            pltpu.VMEM((heads, 2 * WIN_ROWS, 2 * GRID_W), F32),
            pltpu.VMEM((half_heads, 2 * WIN_ROWS, 2 * GRID_W), F32),
            pltpu.VMEM((n_pairs, half_heads * GRID_W, 2 * GRID_W), F32),
            pltpu.VMEM((2 * l_rows, stack, half), BF16),
            pltpu.VMEM((2, stack, WIN_ROWS * GRID_W), F32),
            pltpu.VMEM((2 * l_rows, stack, 128), F32),
            pltpu.VMEM((2 * l_rows, stack, half + 128), F32),
            pltpu.VMEM((l_rows * stack, n_sp * c_rows), F32),
            pltpu.VMEM((l_rows * stack, n_sp * c_rows), BF16),
            pltpu.VMEM((l_rows * stack, half + 128), F32),
            pltpu.VMEM((rows, half), BF16),
            pltpu.VMEM((n_tp, 2, rows, half), BF16),
            dma((15,)),
            dma((n_sp,)),
            dma((n_sp,)),
            dma((n_tp,)),
            dma((n_tp,)),
            dma((n_sp,)),
            dma((n_sp,)),
            dma((n_tp,)),
            dma((n_tp,)),
            dma((4,)),
            dma((4,)),
            dma((2, 2)),
            dma((2, 2)),
            dma((2, n_sp)),
            dma((2, n_sp)),
            dma((2, n_sp)),
            dma((5, 16)),
            dma((5, 16)),
            dma((7,)),
            dma((7,)),
        ],
        compiler_params=pltpu.CompilerParams(collective_id=0, has_side_effects=True),
        name="fused_block",
    )(
        latent,
        context,
        shift_weight,
        scale_weight,
        gate_weight,
        query_weight,
        key_weight,
        value_weight,
        out_weight,
        condition.reshape(1, -1),
        ctx_condition.reshape(1, -1),
        norm_gain.reshape(1, -1),
        query_gain.reshape(1, -1),
        key_gain.reshape(1, -1),
        offset_bias.transpose(1, 0, 2),
    )


def fused_fits(latent, context, condition, query_weight, n_sp, n_tp):
    rows, c_rows = latent.shape[0] // n_sp, context.shape[0] // n_sp
    width = query_weight.shape[1] // n_tp
    return (
        rows == WIN_ROWS // 2 * GRID_W
        and c_rows % 32 == 0
        and condition.shape[0] // n_sp % 128 == 0
        and condition.shape[0] // n_tp % 256 == 0
        and condition.shape[0] // n_tp <= 1024
        and width == 2 * LANES
        and n_tp == 4
        and n_sp == 8
    )


def solution(mesh):
    in_specs = (
        P("sp", None),
        P("sp", None),
        P("sp"),
        P("sp"),
        P("sp", "tp"),
        P("sp", "tp"),
        P("sp", "tp"),
        P(),
        P(None, "tp"),
        P(None, "tp"),
        P(None, "tp"),
        P(),
        P(),
        P("tp", None, None),
        P("tp", None),
    )
    out_specs = P("sp", None)

    def step(latent, context, condition, ctx_condition, *rest):
        n_sp, n_tp = mesh.shape["sp"], mesh.shape["tp"]
        fits = fused_fits(latent, context, condition, rest[4], n_sp, n_tp)
        body = per_device if fits else per_device_plain
        return jax.shard_map(
            body, mesh=mesh, in_specs=in_specs, out_specs=out_specs, check_vma=False
        )(latent, context, condition, ctx_condition, *rest)

    return step
```

```python
import functools

import jax
import jax.numpy as jnp
from jax import lax
from jax.experimental import pallas as pl
from jax.experimental.pallas import tpu as pltpu
from jax.sharding import PartitionSpec as P

HEAD_DIM = 64
GRID_W = 64
WIN_ROWS = 8
WIN_COLS = 16


EPS = 1e-06


def extended(x, sides, width):
    for axis, dim in sides:
        count, length = (lax.axis_size(axis), x.shape[dim])
        up = [(i, (i + 1) % count) for i in range(count - 1)]
        down = [(j, i) for i, j in up]
        last = lax.slice_in_dim(x, length - width, length, axis=dim)
        initial = lax.slice_in_dim(x, 0, width, axis=dim)
        before = lax.ppermute(last, axis, up)
        after = lax.ppermute(initial, axis, down)
        x = jnp.concatenate([before, x, after], axis=dim)
    return x


def modulate(rows_in, norm_gain, shift_vec, scale_vec):
    values = rows_in.astype(jnp.float32)
    normed = values * lax.rsqrt(jnp.mean(values * values, axis=-1, keepdims=True) + EPS)
    return (normed * norm_gain * (1.0 + scale_vec) + shift_vec).astype(jnp.bfloat16)


def head_norm(projected, head_gain):
    row_count = projected.shape[0]
    split_heads = projected.reshape(row_count, -1, head_gain.shape[0])
    normed = split_heads * lax.rsqrt(
        jnp.mean(split_heads * split_heads, axis=-1, keepdims=True) + EPS
    )
    return (normed * head_gain).astype(jnp.bfloat16).reshape(row_count, -1)


def per_device_plain(
    latent,
    context,
    condition,
    ctx_condition,
    shift_weight,
    scale_weight,
    gate_weight,
    norm_gain,
    query_weight,
    key_weight,
    value_weight,
    query_gain,
    key_gain,
    offset_bias,
    out_weight,
):
    activations = jax.nn.silu(jnp.stack([condition, ctx_condition])).astype(jnp.bfloat16)
    part_shift = jnp.dot(activations, shift_weight, preferred_element_type=jnp.float32)
    part_scale = jnp.dot(activations, scale_weight, preferred_element_type=jnp.float32)
    part_gate = jnp.dot(activations[:1], gate_weight, preferred_element_type=jnp.float32)
    block_cols = shift_weight.shape[1]
    first_col = lax.axis_index("tp") * block_cols

    def spread(piece_part):
        padded_vec = jnp.zeros((piece_part.shape[0], block_cols * lax.axis_size("tp")), jnp.float32)
        return lax.dynamic_update_slice_in_dim(padded_vec, piece_part, first_col, 1)

    shift_vec, scale_vec, gate_vec = lax.psum(
        (spread(part_shift), spread(part_scale), spread(part_gate)), ("sp", "tp")
    )
    hidden = modulate(latent, norm_gain, shift_vec[0], scale_vec[0])
    queries = head_norm(
        jnp.dot(hidden, query_weight, preferred_element_type=jnp.float32), query_gain
    )
    keys_lat = head_norm(jnp.dot(hidden, key_weight, preferred_element_type=jnp.float32), key_gain)
    values_lat = jnp.dot(hidden, value_weight, preferred_element_type=jnp.float32).astype(
        jnp.bfloat16
    )
    ctx_hidden = modulate(
        lax.all_gather(context, "sp", axis=0, tiled=True), norm_gain, shift_vec[1], scale_vec[1]
    )
    ctx_keys = head_norm(
        jnp.dot(ctx_hidden, key_weight, preferred_element_type=jnp.float32), key_gain
    )
    ctx_values = jnp.dot(ctx_hidden, value_weight, preferred_element_type=jnp.float32).astype(
        jnp.bfloat16
    )
    ctx_pairs = jnp.concatenate([ctx_keys, ctx_values], axis=1)
    col_width = keys_lat.shape[1]
    heads_dev = col_width // HEAD_DIM
    local_rows = keys_lat.shape[0] // GRID_W
    halo_rows = WIN_ROWS // 2
    window_keys = WIN_ROWS * GRID_W
    key_value = jnp.concatenate([keys_lat, values_lat], axis=1).reshape(
        local_rows, GRID_W, 2 * col_width
    )
    padded = extended(key_value, (("sp", 0),), halo_rows)
    first_row = lax.axis_index("sp") * local_rows
    total_rows = local_rows * lax.axis_size("sp")
    global_rows = first_row + jnp.arange(local_rows, dtype=jnp.int32)
    band_start = jnp.clip(global_rows - halo_rows, 0, total_rows - WIN_ROWS)
    band_global = band_start[:, None] + jnp.arange(WIN_ROWS, dtype=jnp.int32)[None, :]
    banded = jnp.take(padded, band_global - first_row + halo_rows, axis=0)
    key_band = banded[..., :col_width].reshape(local_rows, window_keys, heads_dev, HEAD_DIM)
    value_band = banded[..., col_width:].reshape(local_rows, window_keys, heads_dev, HEAD_DIM)
    row_steps = band_global - global_rows[:, None] + WIN_ROWS - 1
    row_hot = (
        row_steps[:, :, None] == jnp.arange(2 * WIN_ROWS - 1, dtype=jnp.int32)[None, None, :]
    ).astype(jnp.float32)
    column_ids = jnp.arange(GRID_W, dtype=jnp.int32)
    col_steps = (
        jnp.clip(column_ids[None, :] - column_ids[:, None], 1 - WIN_COLS, WIN_COLS - 1)
        + WIN_COLS
        - 1
    )
    col_hot = (
        col_steps[:, :, None] == jnp.arange(2 * WIN_COLS - 1, dtype=jnp.int32)[None, None, :]
    ).astype(jnp.float32)
    col_start = jnp.clip(column_ids - WIN_COLS // 2, 0, GRID_W - WIN_COLS)
    col_open = (column_ids[None, :] >= col_start[:, None]) & (
        column_ids[None, :] < col_start[:, None] + WIN_COLS
    )
    col_table = jnp.einsum("hab,qkb->haqk", offset_bias, col_hot, precision=lax.Precision.HIGHEST)
    col_table = jnp.where(col_open[None, None, :, :], col_table, -jnp.inf)
    offset_terms = jnp.einsum(
        "rja,haqk->hrqjk",
        row_hot,
        jnp.where(col_open[None, None], col_table, 0.0),
        precision=lax.Precision.HIGHEST,
    )
    offset_terms = jnp.where(col_open[None, None, :, None, :], offset_terms, -jnp.inf)
    offset_terms = offset_terms.reshape(heads_dev, local_rows, GRID_W, window_keys)
    score_scale = HEAD_DIM ** (-0.5)
    q_grid = queries.reshape(local_rows, GRID_W, heads_dev, HEAD_DIM)
    scores = (
        jnp.einsum("rqhd,rnhd->hrqn", q_grid, key_band, preferred_element_type=jnp.float32)
        * score_scale
        + offset_terms
    )
    ctx_count = ctx_pairs.shape[0]
    ctx_keys_all = ctx_pairs[:, :col_width].reshape(ctx_count, heads_dev, HEAD_DIM)
    ctx_values_all = ctx_pairs[:, col_width:].reshape(ctx_count, heads_dev, HEAD_DIM)
    ctx_scores = (
        jnp.einsum("rqhd,nhd->hrqn", q_grid, ctx_keys_all, preferred_element_type=jnp.float32)
        * score_scale
    )
    row_max = jnp.maximum(jnp.max(scores, axis=3), jnp.max(ctx_scores, axis=3))
    local_exp = jnp.exp(scores - row_max[..., None])
    ctx_exp = jnp.exp(ctx_scores - row_max[..., None])
    denominator = jnp.sum(local_exp, axis=3) + jnp.sum(ctx_exp, axis=3)
    local_weights = (local_exp / denominator[..., None]).astype(jnp.bfloat16)
    ctx_weights = (ctx_exp / denominator[..., None]).astype(jnp.bfloat16)
    combined = jnp.einsum(
        "hrqn,rnhd->rqhd", local_weights, value_band, preferred_element_type=jnp.float32
    ) + jnp.einsum(
        "hrqn,nhd->rqhd", ctx_weights, ctx_values_all, preferred_element_type=jnp.float32
    )
    attended = combined.astype(jnp.bfloat16).reshape(local_rows * GRID_W, col_width)
    partial_value = jnp.dot(attended, out_weight, preferred_element_type=jnp.float32)
    branch = lax.psum(partial_value.astype(jnp.bfloat16), "tp").astype(jnp.float32)
    return (latent.astype(jnp.float32) + gate_vec[0] * branch).astype(jnp.bfloat16)


MESH = pl.DeviceIdType.MESH
MASKED = -1e30
LANES = 128
F32 = jnp.float32
BF16 = jnp.bfloat16


def fused_kernel(
    n_sp,
    n_tp,
    latent,
    context,
    shift_w,
    scale_w,
    gate_w,
    query_w,
    key_w,
    value_w,
    out_w,
    cond,
    ctx_cond,
    norm_gain,
    query_gain,
    key_gain,
    bias_in,
    out,
    cond_v,
    ctx_cond_v,
    norm_gain_v,
    query_gain_v,
    key_gain_v,
    bias_v,
    x_in,
    x_norm,
    hid,
    w_mod,
    w_qkv,
    w_out,
    mod_sp,
    mod_tp,
    part_kv,
    part_q,
    gate_sp,
    gate_tp,
    acc,
    q_stage,
    k_stage,
    v_stage,
    ck_stage,
    cv_stage,
    q_all,
    k_all,
    v_all,
    ctx_k,
    ctx_v,
    bias_pad,
    bias_lines,
    table,
    q_heads,
    scores,
    tops,
    sums,
    scores_ctx,
    weights,
    sums_ctx,
    att_slab,
    att,
    local_sem,
    mod_send,
    mod_recv,
    modt_send,
    modt_recv,
    gate_send,
    gate_recv,
    gatet_send,
    gatet_recv,
    pair_send,
    pair_recv,
    halo_send,
    halo_recv,
    ctx_send,
    ctx_recv,
    end_send,
    wo_send,
    wo_recv,
    att_send,
    att_recv,
):
    me_s, me_t = lax.axis_index("sp"), lax.axis_index("tp")
    rows, d = latent.shape
    c_rows = context.shape[0]
    width = key_w.shape[1]
    heads = width // HEAD_DIM
    block = shift_w.shape[1]
    blocks = block // 128
    l_rows = rows // GRID_W
    halo = WIN_ROWS // 2
    win = WIN_ROWS * GRID_W
    core = lax.rem(me_t, 2)
    chip = lax.div(me_t, 2)
    partner = me_t + 1 - 2 * core
    far = 2 * (1 - chip) + core
    far_partner = 2 * (1 - chip) + 1 - core
    side = lax.rem(me_s, 2)
    slab = lax.div(me_s, 2)
    mate = me_s + 1 - 2 * side
    last_slab = n_sp // 2 - 1
    half = width // 2
    half_heads = heads // 2

    def remote(src, dst, send, recv, s, t):
        return pltpu.make_async_remote_copy(
            src_ref=src, dst_ref=dst, send_sem=send, recv_sem=recv,
            device_id=(s, t), device_id_type=MESH,
        )

    barrier = pltpu.get_barrier_semaphore()
    for k in range(1, n_sp):
        pl.semaphore_signal(
            barrier, inc=1, device_id=(lax.rem(me_s + k, n_sp), me_t), device_id_type=MESH
        )
    for k in range(1, n_tp):
        pl.semaphore_signal(
            barrier, inc=1, device_id=(me_s, lax.rem(me_t + k, n_tp)), device_id_type=MESH
        )
    pl.semaphore_signal(barrier, inc=1, device_id=(mate, far), device_id_type=MESH)

    loads = [
        (shift_w, w_mod.at[0]),
        (scale_w, w_mod.at[1]),
        (gate_w, w_mod.at[2]),
        (context, x_in.at[pl.ds(0, c_rows)]),
        (latent, x_in.at[pl.ds(c_rows, rows)]),
        (key_w, w_qkv.at[:, pl.ds(0, width)]),
        (value_w, w_qkv.at[:, pl.ds(width, width)]),
        (query_w, w_qkv.at[:, pl.ds(2 * width, width)]),
        (out_w, w_out.at[me_t]),
        (cond, cond_v),
        (ctx_cond, ctx_cond_v),
        (norm_gain, norm_gain_v),
        (query_gain, query_gain_v),
        (key_gain, key_gain_v),
        (bias_in, bias_v),
    ]
    copies = [pltpu.make_async_copy(a, b, local_sem.at[i]) for i, (a, b) in enumerate(loads)]
    for i in (9, 10, 0, 1, 2, 11, 12, 13, 14, 3, 4):
        copies[i].start()

    def silu(v):
        return v / (1.0 + jnp.exp(-v))

    two = (16, cond.shape[1])
    row_id = lax.broadcasted_iota(jnp.int32, two, 0)
    copies[9].wait()
    copies[10].wait()
    act0 = jnp.broadcast_to(silu(cond_v[...]), two)
    act1 = jnp.broadcast_to(silu(ctx_cond_v[...]), two)

    def placed(first, second):
        picked = jnp.where(row_id == first, act0, 0.0)
        if second is not None:
            picked = jnp.where(row_id == second, act1, picked)
        return picked.astype(BF16)

    part = jnp.zeros((16, block), F32)
    for i in range(2):
        copies[i].wait()
        part += jnp.dot(placed(2 * i, 2 * i + 1), w_mod[i], preferred_element_type=F32)
    for b in range(blocks):
        mod_sp[me_s, 4 * b : 4 * b + 4, :] = part[:4, b * 128 : (b + 1) * 128]
    pl.semaphore_wait(barrier, n_sp + n_tp - 1)
    sends = []

    def share_sp(buf, send, recv):
        for k in range(1, n_sp):
            peer = lax.rem(me_s + k, n_sp)
            c = remote(buf.at[me_s], buf.at[me_s], send.at[k], recv.at[me_s], peer, me_t)
            c.start()
            sends.append(c)

    def sum_sp(buf, send, recv):
        for k in range(1, n_sp):
            peer = lax.rem(me_s + k, n_sp)
            remote(buf.at[peer], buf.at[peer], send.at[k], recv.at[peer], peer, me_t).wait_recv()
        total = buf[0]
        for k in range(1, n_sp):
            total = total + buf[k]
        return total

    def share_tp(buf, send, recv):
        for k in range(1, n_tp):
            peer = lax.rem(me_t + k, n_tp)
            c = remote(buf.at[me_t], buf.at[me_t], send.at[k], recv.at[me_t], me_s, peer)
            c.start()
            sends.append(c)

    def wait_tp(buf, send, recv):
        for k in range(1, n_tp):
            peer = lax.rem(me_t + k, n_tp)
            remote(buf.at[peer], buf.at[peer], send.at[k], recv.at[peer], me_s, peer).wait_recv()

    share_sp(mod_sp, mod_send, mod_recv)
    for i in (5, 6, 7, 8):
        copies[i].start()
    copies[2].wait()
    gate_part = jnp.dot(placed(0, None), w_mod[2], preferred_element_type=F32)
    for b in range(blocks):
        gate_sp[me_s, b : b + 1, :] = gate_part[:1, b * 128 : (b + 1) * 128]

    piece = width // 16
    n_cross, n_direct = 3, 4
    n_pieces = 2 * n_cross + n_direct
    early = (0, n_cross)
    later = [c + o for c in range(1, n_cross) for o in (0, n_cross)]
    later = later + list(range(2 * n_cross, n_pieces))
    z_side = lax.rem(slab, 2)
    z_mate = me_s + 2 - 4 * z_side

    def wo_rows(c, away_from):
        if c < n_cross:
            start = (side + away_from - 2 * side * away_from) * n_cross * piece + c * piece
        elif c < 2 * n_cross:
            start = (
                2 * n_cross * piece
                + (z_side + away_from - 2 * z_side * away_from) * n_cross * piece
                + (c - n_cross) * piece
            )
        else:
            start = (2 * n_cross + c) * piece
        return pl.ds(pl.multiple_of(start, piece), piece)

    def wo_copy(kind, c, source, shard, rows_at, s, t):
        return remote(
            source.at[rows_at], w_out.at[shard, rows_at],
            wo_send.at[kind, c], wo_recv.at[kind, c], s, t,
        )

    def begin(c):
        c.start()
        sends.append(c)

    def wo_far(c):
        return wo_copy(0, c, out_w, me_t, wo_rows(c, 0), me_s, far)

    def wo_forward(c):
        at_rows = wo_rows(c, 0)
        came = w_out.at[far]
        wo_copy(0, c, came, far, at_rows, me_s, far).wait_recv()
        begin(wo_copy(1, c, came, far, at_rows, me_s, partner))
        if c < 2 * n_cross:
            begin(wo_copy(2, c, came, far, at_rows, mate if c < n_cross else z_mate, me_t))

    def wo_cross(c):
        at_rows = wo_rows(c, 1)
        came = w_out.at[far]
        wo_copy(2, c, came, far, at_rows, mate, me_t).wait_recv()
        begin(wo_copy(3, c, came, far, at_rows, me_s, partner))

    def wo_finish_far():
        for c in range(n_pieces):
            wo_copy(
                1, c, w_out.at[far_partner], far_partner, wo_rows(c, 0), me_s, partner
            ).wait_recv()
        for c in range(2 * n_cross):
            wo_copy(
                3, c, w_out.at[far_partner], far_partner, wo_rows(c, 1), me_s, partner
            ).wait_recv()

    def wo_partner():
        return remote(
            out_w, w_out.at[me_t], wo_send.at[4, 0], wo_recv.at[4, 0], me_s, partner
        )

    for c in early:
        begin(wo_far(c))

    copies[3].wait()
    copies[4].wait()
    copies[11].wait()
    step = 32

    def norm_rows(i, carry):
        at = pl.ds(pl.multiple_of(i * step, step), step)
        v = x_in[at, :].astype(F32)
        r = lax.rsqrt(jnp.mean(v * v, axis=-1, keepdims=True) + EPS)
        x_norm[at, :] = v * r * norm_gain_v[...]
        return carry

    lax.fori_loop(0, (rows + c_rows) // step, norm_rows, 0)

    pair = 2 * GRID_W
    q_col = lax.broadcasted_iota(jnp.int32, (GRID_W, pair), 0)
    k_col = lax.broadcasted_iota(jnp.int32, (GRID_W, pair), 1) % GRID_W
    col0 = jnp.clip(q_col - WIN_COLS // 2, 0, GRID_W - WIN_COLS)
    col_open = (k_col >= col0) & (k_col < col0 + WIN_COLS)
    n_pairs = 2 * WIN_ROWS - 2
    copies[14].wait()
    bias_pad[...] = jnp.zeros_like(bias_pad)
    for h in range(heads):
        bias_pad[h, : 2 * WIN_ROWS - 1, : 2 * WIN_COLS - 1] = bias_v[:, h, :]
    for h in range(half_heads):
        head = side * half_heads + h
        upper = pltpu.roll(bias_pad[head, 1 : n_pairs + 1, :], GRID_W, 1)
        bias_lines[h, :n_pairs, :] = bias_pad[head, :n_pairs, :] + upper
        for a in range(n_pairs):
            line = jnp.broadcast_to(bias_lines[h, a : a + 1, :], (GRID_W, pair))
            rolled = pltpu.roll(line, pair - (WIN_COLS - 1), 1, stride=1, stride_axis=0)
            table[a, h * GRID_W : (h + 1) * GRID_W, :] = jnp.where(col_open, rolled, MASKED)

    mod_tp[me_t] = sum_sp(mod_sp, mod_send, mod_recv)
    share_tp(mod_tp, modt_send, modt_recv)
    for c in later:
        begin(wo_far(c))
    share_sp(gate_sp, gate_send, gate_recv)

    def wait_mod(peer):
        remote(
            mod_tp.at[peer], mod_tp.at[peer], modt_send.at[1], modt_recv.at[peer], me_s, peer
        ).wait_recv()

    pair_cols = 2 * block

    def vec(which, r):
        return jnp.concatenate(
            [
                mod_tp[2 * which + j, 4 * b + r : 4 * b + r + 1, :]
                for j in range(2)
                for b in range(blocks)
            ],
            axis=1,
        )

    def cols_of(which):
        return pl.ds(pl.multiple_of(which * pair_cols, pair_cols), pair_cols)

    def modulate_rows(which, first, count, shift, scale):
        def body(i, carry):
            at = pl.ds(pl.multiple_of(first + i * step, step), step)
            hid[at, cols_of(which)] = (x_norm[at, cols_of(which)] * scale + shift).astype(BF16)
            return carry

        lax.fori_loop(0, count // step, body, 0)

    def modulate_pair(which):
        modulate_rows(which, 0, c_rows, vec(which, 1), 1.0 + vec(which, 3))
        modulate_rows(which, c_rows, rows, vec(which, 0), 1.0 + vec(which, 2))

    def hidden_dot(which, start_row, start_col, count_col):
        return jnp.dot(
            hid[start_row:, cols_of(which)],
            w_qkv[cols_of(which), start_col : start_col + count_col],
            preferred_element_type=F32,
        )

    wait_mod(partner)
    modulate_pair(chip)
    for i in (5, 6, 7):
        copies[i].wait()
    part_kv[...] = hidden_dot(chip, 0, 0, 2 * width)
    part_q[...] = hidden_dot(chip, c_rows, 2 * width, width)
    for c in early:
        wo_forward(c)
    wait_mod(far)
    wait_mod(far_partner)
    head_row = lax.broadcasted_iota(jnp.int32, (width, width), 0) // HEAD_DIM
    head_col = lax.broadcasted_iota(jnp.int32, (width, width), 1) // HEAD_DIM
    same_head = (head_row == head_col).astype(BF16)
    copies[12].wait()
    copies[13].wait()

    def head_scale(p, gain):
        squares = p * p
        high = squares.astype(BF16)
        low = (squares - high.astype(F32)).astype(BF16)
        mean = jnp.dot(high, same_head, preferred_element_type=F32)
        mean = mean + jnp.dot(low, same_head, preferred_element_type=F32)
        mean = mean * (1.0 / HEAD_DIM)
        wide_gain = jnp.concatenate([gain[...]] * heads, axis=1)
        return (p * lax.rsqrt(mean + EPS) * wide_gain).astype(BF16)

    own = pl.ds(rows + pl.multiple_of(side * rows, rows), rows)
    other = pl.ds(rows + pl.multiple_of((1 - side) * rows, rows), rows)

    def split(stage, value):
        for h in range(2):
            stage[h] = value[:, h * half : (h + 1) * half]

    def trade(index, stage, block_all, at):
        c = remote(
            stage.at[1 - side], block_all.at[at], pair_send.at[index], pair_recv.at[index],
            mate, me_t,
        )
        c.start()
        sends.append(c)
        return c

    n_z = n_sp // 2
    z_order = tuple(range(2, n_z)) + (1,)

    def ctx_copy(index, slot, source, shard, block_ctx, s):
        return remote(
            source, block_ctx.at[shard], ctx_send.at[index, slot], ctx_recv.at[index, shard],
            s, me_t,
        )

    at_end = (slab == 0) | (slab == last_slab)
    sends_when = []

    def along_z(index, slot, source, shard, block_ctx, all_direct=False):
        for k in z_order:
            peer = lax.rem(slab + k, n_z)
            c = ctx_copy(index, slot + k, source, shard, block_ctx, 2 * peer + side)
            low = (peer == 0) & (slab >= 2)
            high = (peer == last_slab) & (slab <= last_slab - 2)
            if all_direct:
                begin(c)
                continue
            direct = jnp.logical_not(low | high)
            pl.when(direct)(c.start)
            sends_when.append((direct, c))

    z_pair = lax.div(slab, 2)

    def relay_end(of_side):
        def body():
            for j in range(2):
                shard = 2 * (2 * (1 - z_pair) + j) + of_side
                for index, block_ctx in enumerate((ctx_k, ctx_v)):
                    ctx_copy(index, 0, block_ctx.at[shard], shard, block_ctx, shard).wait_recv()
                    end_copy(index, shard, block_ctx).start()

        pl.when(jnp.logical_not(at_end))(body)
        for j in range(2):
            shard = 2 * (2 * (1 - z_pair) + j) + of_side
            for index, block_ctx in enumerate((ctx_k, ctx_v)):
                sends_when.append((jnp.logical_not(at_end), end_copy(index, shard, block_ctx)))

    def end_copy(index, shard, block_ctx):
        return remote(
            block_ctx.at[shard], block_ctx.at[shard],
            end_send.at[index, shard], ctx_recv.at[index, shard],
            2 * z_pair * last_slab + side, me_t,
        )


    def relay_ctx(index, block_ctx):
        ctx_copy(index, 0, block_ctx.at[mate], mate, block_ctx, mate).wait_recv()
        along_z(index, n_z - 1, block_ctx.at[mate], mate, block_ctx, True)

    lower = rows - GRID_W

    def halo_copies(index, block_all):
        down = remote(
            block_all.at[pl.ds(rows, lower)], block_all.at[pl.ds(3 * rows, lower)],
            halo_send.at[index, 0], halo_recv.at[index, 0], me_s - 2, me_t,
        )
        up = remote(
            block_all.at[pl.ds(2 * rows, rows)], block_all.at[pl.ds(0, rows)],
            halo_send.at[index, 1], halo_recv.at[index, 1], me_s + 2, me_t,
        )
        return down, up

    def halo_start(mine, index, block_all):
        down, up = halo_copies(index, block_all)
        is_low = side == 0 if mine else side == 1

        @pl.when(is_low & (slab > 0))
        def _():
            down.start()

        @pl.when(jnp.logical_not(is_low) & (slab < last_slab))
        def _():
            up.start()

    away = 1 - chip
    modulate_rows(away, 0, c_rows, vec(away, 1), 1.0 + vec(away, 3))
    ctx_both = part_kv[:c_rows, :] + jnp.dot(
        hid[:c_rows, cols_of(away)], w_qkv[cols_of(away), : 2 * width], preferred_element_type=F32
    )
    ctx_keys = head_scale(ctx_both[:, :width], key_gain_v)
    ctx_values = ctx_both[:, width:].astype(BF16)
    split(ck_stage, ctx_keys)
    split(cv_stage, ctx_values)
    for index, (stage, block_ctx) in enumerate(((ck_stage, ctx_k), (cv_stage, ctx_v))):
        begin(ctx_copy(index, 0, stage.at[1 - side], me_s, block_ctx, mate))
        along_z(index, 0, stage.at[side], me_s, block_ctx)
        block_ctx[me_s] = stage[side]
    modulate_rows(away, c_rows, rows, vec(away, 0), 1.0 + vec(away, 2))
    both = part_kv[c_rows:, :] + hidden_dot(away, c_rows, 0, 2 * width)
    keys = head_scale(both[:, :width], key_gain_v)
    split(k_stage, keys)
    k_trade = trade(0, k_stage, k_all, own)
    k_all[own, :] = k_stage[side]
    halo_start(True, 0, k_all)
    split(v_stage, both[:, width:].astype(BF16))
    v_trade = trade(1, v_stage, v_all, own)
    v_all[own, :] = v_stage[side]
    halo_start(True, 1, v_all)
    queries = head_scale(
        part_q[...] + hidden_dot(away, c_rows, 2 * width, width), query_gain_v
    ) * jnp.asarray(HEAD_DIM ** (-0.5), BF16)
    split(q_stage, queries)
    q_own = pl.ds(pl.multiple_of(side * rows, rows), rows)
    q_trade = trade(2, q_stage, q_all, q_own)
    q_all[q_own, :] = q_stage[side]
    begin(wo_partner())
    gate_tp[me_t] = sum_sp(gate_sp, gate_send, gate_recv)
    share_tp(gate_tp, gatet_send, gatet_recv)
    relay_ctx(0, ctx_k)
    relay_ctx(1, ctx_v)
    relay_end(side)
    k_trade.wait_recv()
    halo_start(False, 0, k_all)
    for c in range(1, n_cross):
        wo_forward(c)
    v_trade.wait_recv()
    halo_start(False, 1, v_all)
    def halo_wait(theirs_need):
        below = side == 0 if theirs_need else side == 1
        for index, block_all in enumerate((k_all, v_all)):
            down, up = halo_copies(index, block_all)

            @pl.when(below & (slab < last_slab))
            def _():
                down.wait_recv()

            @pl.when(jnp.logical_not(below) & (slab > 0))
            def _():
                up.wait_recv()

    lane_head = lax.broadcasted_iota(jnp.int32, (GRID_W, half), 1) // HEAD_DIM
    masks = [(lane_head == h).astype(F32) for h in range(half_heads)]
    contract_last = (((1,), (1,)), ((), ()))
    stack = half_heads * GRID_W
    ones = jnp.ones((win, 128), BF16)

    def stacked(i):
        qi = q_all[pl.ds(pl.multiple_of(i * GRID_W, GRID_W), GRID_W), :].astype(F32)
        return jnp.concatenate([(qi * m).astype(BF16) for m in masks], axis=0)

    def score_local(i, held_at, slot):
        start = jnp.where(
            slab == 0,
            jnp.maximum(i, halo),
            jnp.where(slab == last_slab, jnp.minimum(i, halo), i),
        )
        if last_slab == 0:
            start = jnp.int32(halo)
        at = pl.ds(pl.multiple_of(start * GRID_W, GRID_W), win)
        qs = stacked(i)
        q_heads[held_at] = qs
        s = lax.dot_general(qs, k_all[at, :], contract_last, preferred_element_type=F32)
        first = start - i + WIN_ROWS - 1 - halo
        s = s + jnp.concatenate([table[first + 2 * m] for m in range(WIN_ROWS // 2)], axis=1)
        scores[slot] = s
        return at, jnp.max(s, axis=1, keepdims=True)

    def weigh_local(held_at, slot, at, top):
        e = jnp.exp(scores[slot] - top)
        tops[held_at] = jnp.broadcast_to(top, (stack, 128))
        values_at = jnp.concatenate([v_all[at, :], ones], axis=1)
        sums[held_at] = jnp.dot(e.astype(BF16), values_at, preferred_element_type=F32)

    def local_half(which, base):
        first = which * l_rows
        held = score_local(first, base, 0)
        for i in range(l_rows):
            later = None
            if i + 1 < l_rows:
                later = score_local(first + i + 1, base + i + 1, (i + 1) % 2)
            weigh_local(base + i, i % 2, *held)
            held = later

    def ctx_wait(wait_near):
        for index, block_ctx in enumerate((ctx_k, ctx_v)):
            for s in range(n_sp):

                relayed = jnp.logical_not(at_end) & (z_pair != s // 4) & (side == s % 2)

                wanted = (z_pair == s // 4) if wait_near else (z_pair != s // 4)

                @pl.when((s != me_s) & (s != mate) & jnp.logical_not(relayed) & wanted)
                def _():
                    ctx_copy(index, 0, block_ctx.at[s], s, block_ctx, s).wait_recv()

    top_head = lax.broadcasted_iota(jnp.int32, (GRID_W, half), 1) // HEAD_DIM
    half_stack = l_rows * stack
    n_ctx = n_sp * c_rows
    ctx_ones = jnp.ones((n_ctx, 128), BF16)

    n_part = n_ctx // 2
    shards_part = n_sp // 2

    def ctx_scores(base, first_shard, n_keys, exp_all):
        shards = pl.ds(first_shard, n_keys // c_rows)
        qs = q_heads[base : base + l_rows].reshape(half_stack, half)
        scores_ctx[:, :n_keys] = lax.dot_general(
            qs, ctx_k[shards].reshape(n_keys, half), contract_last, preferred_element_type=F32
        )
        fades = []
        for i in range(l_rows):
            at_rows = slice(i * stack, (i + 1) * stack)
            s = scores_ctx[at_rows, :n_keys]
            old = tops[base + i]
            top = jnp.maximum(old, jnp.max(s, axis=1, keepdims=True))
            fade = jnp.exp(old - top)
            fades.append(jnp.concatenate([fade] * ((half + 128) // 128), axis=1))
            if exp_all:
                tops[base + i] = top
            wide_top = jnp.concatenate([top] * (n_keys // 128), axis=1)
            weights[at_rows, :n_keys] = jnp.exp(s - wide_top).astype(BF16)
        values_ctx = jnp.concatenate(
            [ctx_v[shards].reshape(n_keys, half), ctx_ones[:n_keys]], axis=1
        )
        sums_ctx[...] = jnp.dot(
            weights[:, :n_keys], values_ctx, preferred_element_type=F32
        )
        return fades

    def ctx_near(base):
        fades = ctx_scores(base, shards_part * z_pair, n_part, True)
        for i in range(l_rows):
            at_rows = slice(i * stack, (i + 1) * stack)
            sums[base + i] = sums_ctx[at_rows, :] + sums[base + i] * fades[i]

    def finished(o):
        up, down = o[:, :half], o[:, half:]
        num, den = up[:GRID_W], down[:GRID_W]
        for h in range(1, half_heads):
            part_h = slice(h * GRID_W, (h + 1) * GRID_W)
            num = jnp.where(top_head == h, up[part_h], num)
            den = jnp.where(top_head == h, down[part_h], den)
        return (num / den).astype(BF16)

    def ctx_last(base, store):
        fades = ctx_scores(base, shards_part * (1 - z_pair), n_part, False)
        for i in range(l_rows):
            at_rows = slice(i * stack, (i + 1) * stack)
            o = sums_ctx[at_rows, :] + sums[base + i] * fades[i]
            store(i, finished(o))

    def att_copy(index, source, dest, s, t):
        return remote(source, dest, att_send.at[index], att_recv.at[index], s, t)

    def store_theirs(i, value):
        att_slab[i * GRID_W : (i + 1) * GRID_W, :] = value

    def store_mine(i, value):
        att[me_t, side, i * GRID_W : (i + 1) * GRID_W, :] = value

    def ctx_start():
        for i in range(l_rows):
            q_heads[l_rows + i] = stacked(side * l_rows + i)
        qs = q_heads[l_rows : 2 * l_rows].reshape(half_stack, half)
        scores_ctx[...] = lax.dot_general(
            qs, ctx_k[...].reshape(n_ctx, half), contract_last, preferred_element_type=F32
        )
        for i in range(l_rows):
            at_rows = slice(i * stack, (i + 1) * stack)
            s = scores_ctx[at_rows, :]
            top = jnp.broadcast_to(jnp.max(s, axis=1, keepdims=True), (stack, 128))
            tops[l_rows + i] = top
            wide_top = jnp.concatenate([top] * (n_ctx // 128), axis=1)
            weights[at_rows, :] = jnp.exp(s - wide_top).astype(BF16)
        values_ctx = jnp.concatenate([ctx_v[...].reshape(n_ctx, half), ctx_ones], axis=1)
        sums_ctx[...] = jnp.dot(weights[...], values_ctx, preferred_element_type=F32)

    def local_last():
        first = side * l_rows
        held = score_local(first, l_rows, 0)
        for i in range(l_rows):
            later = None
            if i + 1 < l_rows:
                later = score_local(first + i + 1, l_rows + i + 1, (i + 1) % 2)
            at, top = held
            at_rows = slice(i * stack, (i + 1) * stack)
            old = tops[l_rows + i]
            top = jnp.maximum(old, top)
            wide_top = jnp.concatenate([top] * (win // 128), axis=1)
            e = jnp.exp(scores[i % 2] - wide_top)
            values_at = jnp.concatenate([v_all[at, :], ones], axis=1)
            o = jnp.dot(e.astype(BF16), values_at, preferred_element_type=F32)
            fade = jnp.exp(old - top)
            o = o + sums_ctx[at_rows, :] * jnp.concatenate([fade] * ((half + 128) // 128), axis=1)
            store_mine(i, finished(o))
            held = later

    def local_mine():
        halo_wait(False)
        local_half(side, l_rows)

    n_early = len(sends)
    for c in range(n_cross + 1, 2 * n_cross):
        wo_forward(c)
    no_halo = ((slab == 0) & (side == 0)) | ((slab == last_slab) & (side == 1))
    @pl.when(no_halo)
    def _():
        local_mine()
        ctx_wait(True)
        ctx_near(l_rows)

    q_trade.wait_recv()
    halo_wait(True)
    local_half(1 - side, 0)
    @pl.when(jnp.logical_not(no_halo))
    def _():
        ctx_wait(True)

    ctx_near(0)
    ctx_wait(False)
    ctx_last(0, store_theirs)
    begin(att_copy(0, att_slab, att.at[me_t, side], mate, far))
    begin(att_copy(1, att_slab, att.at[me_t, side], mate, me_t))
    @pl.when(no_halo)
    def _():
        ctx_last(l_rows, store_mine)

    @pl.when(jnp.logical_not(no_halo))
    def _():
        ctx_start()
        halo_wait(False)
        local_last()

    begin(att_copy(2, att.at[me_t, side], att.at[me_t, side], me_s, far))
    begin(att_copy(3, att.at[me_t, side], att.at[me_t, side], me_s, partner))

    def arrived(index, shard, part_of):
        return att_copy(index, att.at[shard, part_of], att.at[shard, part_of], me_s, partner)

    def pass_on(index, onto, shard, part_of):
        arrived(index, shard, part_of).wait_recv()
        begin(arrived(onto, shard, part_of))

    for c in range(2 * n_cross, n_pieces):
        wo_forward(c)
    for c in range(2 * n_cross):
        wo_cross(c)
    wait_tp(gate_tp, gatet_send, gatet_recv)
    gate = jnp.concatenate(
        [gate_tp[j, b : b + 1, :] for j in range(n_tp) for b in range(blocks)], axis=1
    )
    copies[8].wait()
    cols = 512

    def project(groups, first_pass, last_pass):
        heads_of = [jnp.concatenate([att[j, 0], att[j, 1]], axis=1) for j in groups]
        for n in range(d // cols):
            at = slice(n * cols, (n + 1) * cols)
            total = None if first_pass else acc[:, at]
            for j, lhs in zip(groups, heads_of):
                term = jnp.dot(lhs, w_out[j, :, at], preferred_element_type=F32)
                term = term.astype(BF16).astype(F32)
                total = term if total is None else total + term
            if last_pass:
                base = x_in[c_rows:, at].astype(F32)
                out[:, at] = (base + gate[:, at] * total).astype(BF16)
            else:
                acc[:, at] = total

    for c in sends[:n_early]:
        c.wait_send()
    for condition, c in sends_when:
        pl.when(condition)(c.wait_send)
    for index, block_all in enumerate((k_all, v_all)):
        down, up = halo_copies(index, block_all)

        @pl.when(slab > 0)
        def _():
            down.wait_send()

        @pl.when(slab < last_slab)
        def _():
            up.wait_send()
    pass_on(1, 5, me_t, 1 - side)
    pass_on(0, 4, far, 1 - side)
    project((me_t,), True, False)
    pass_on(2, 6, far, side)
    odd = core == 1
    @pl.when(odd)
    def _():
        project((far,), False, False)

    remote(
        w_out.at[partner], w_out.at[partner], wo_send.at[4, 0], wo_recv.at[4, 0], me_s, partner
    ).wait_recv()
    arrived(3, partner, side).wait_recv()
    arrived(5, partner, 1 - side).wait_recv()
    @pl.when(odd)
    def _():
        project((partner,), False, False)

    wo_finish_far()
    arrived(4, far_partner, 1 - side).wait_recv()
    arrived(6, far_partner, side).wait_recv()
    @pl.when(odd)
    def _():
        project((far_partner,), False, True)

    @pl.when(jnp.logical_not(odd))
    def _():
        project((far, partner, far_partner), False, True)

    for c in sends[n_early:]:
        c.wait_send()


def per_device(
    latent,
    context,
    condition,
    ctx_condition,
    shift_weight,
    scale_weight,
    gate_weight,
    norm_gain,
    query_weight,
    key_weight,
    value_weight,
    query_gain,
    key_gain,
    offset_bias,
    out_weight,
):
    n_sp, n_tp = lax.axis_size("sp"), lax.axis_size("tp")
    rows, d = latent.shape
    c_rows = context.shape[0]
    width = key_weight.shape[1]
    heads = width // HEAD_DIM
    block = shift_weight.shape[1]
    n_pairs = 2 * WIN_ROWS - 2
    half = width // 2
    half_heads = heads // 2
    blocks = block // 128
    l_rows = rows // GRID_W
    stack = half_heads * GRID_W
    any_spec = pl.BlockSpec(memory_space=pl.ANY)
    vmem_spec = pl.BlockSpec(memory_space=pltpu.VMEM)
    dma = pltpu.SemaphoreType.DMA
    return pl.pallas_call(
        functools.partial(fused_kernel, n_sp, n_tp),
        out_shape=pltpu.VMEM((rows, d), BF16),
        in_specs=[any_spec] * 15,
        out_specs=vmem_spec,
        scratch_shapes=[
            pltpu.VMEM((1, condition.shape[0]), F32),
            pltpu.VMEM((1, condition.shape[0]), F32),
            pltpu.VMEM((1, d), F32),
            pltpu.VMEM((1, HEAD_DIM), F32),
            pltpu.VMEM((1, HEAD_DIM), F32),
            pltpu.VMEM((2 * WIN_ROWS - 1, heads, 2 * WIN_COLS - 1), F32),
            pltpu.VMEM((rows + c_rows, d), BF16),
            pltpu.VMEM((rows + c_rows, d), F32),
            pltpu.VMEM((rows + c_rows, d), BF16),
            pltpu.VMEM((3, shift_weight.shape[0], block), BF16),
            pltpu.VMEM((d, 3 * width), BF16),
            pltpu.VMEM((n_tp, width, d), BF16),
            pltpu.VMEM((n_sp, 4 * blocks, 128), F32),
            pltpu.VMEM((n_tp, 4 * blocks, 128), F32),
            pltpu.VMEM((rows + c_rows, 2 * width), F32),
            pltpu.VMEM((rows, width), F32),
            pltpu.VMEM((n_sp, blocks, 128), F32),
            pltpu.VMEM((n_tp, blocks, 128), F32),
            pltpu.VMEM((rows, d), F32),
            pltpu.VMEM((2, rows, half), BF16),
            pltpu.VMEM((2, rows, half), BF16),
            pltpu.VMEM((2, rows, half), BF16),
            pltpu.VMEM((2, c_rows, half), BF16),
            pltpu.VMEM((2, c_rows, half), BF16),
            pltpu.VMEM((2 * rows, half), BF16),
            pltpu.VMEM((4 * rows, half), BF16),
            pltpu.VMEM((4 * rows, half), BF16),
            pltpu.VMEM((n_sp, c_rows, half), BF16),
            pltpu.VMEM((n_sp, c_rows, half), BF16),
            pltpu.VMEM((heads, 2 * WIN_ROWS, 2 * GRID_W), F32),
            pltpu.VMEM((half_heads, 2 * WIN_ROWS, 2 * GRID_W), F32),
            pltpu.VMEM((n_pairs, half_heads * GRID_W, 2 * GRID_W), F32),
            pltpu.VMEM((2 * l_rows, stack, half), BF16),
            pltpu.VMEM((2, stack, WIN_ROWS * GRID_W), F32),
            pltpu.VMEM((2 * l_rows, stack, 128), F32),
            pltpu.VMEM((2 * l_rows, stack, half + 128), F32),
            pltpu.VMEM((l_rows * stack, n_sp * c_rows), F32),
            pltpu.VMEM((l_rows * stack, n_sp * c_rows), BF16),
            pltpu.VMEM((l_rows * stack, half + 128), F32),
            pltpu.VMEM((rows, half), BF16),
            pltpu.VMEM((n_tp, 2, rows, half), BF16),
            dma((15,)),
            dma((n_sp,)),
            dma((n_sp,)),
            dma((n_tp,)),
            dma((n_tp,)),
            dma((n_sp,)),
            dma((n_sp,)),
            dma((n_tp,)),
            dma((n_tp,)),
            dma((4,)),
            dma((4,)),
            dma((2, 2)),
            dma((2, 2)),
            dma((2, n_sp)),
            dma((2, n_sp)),
            dma((2, n_sp)),
            dma((5, 16)),
            dma((5, 16)),
            dma((7,)),
            dma((7,)),
        ],
        compiler_params=pltpu.CompilerParams(collective_id=0, has_side_effects=True),
        name="fused_block",
    )(
        latent,
        context,
        shift_weight,
        scale_weight,
        gate_weight,
        query_weight,
        key_weight,
        value_weight,
        out_weight,
        condition.reshape(1, -1),
        ctx_condition.reshape(1, -1),
        norm_gain.reshape(1, -1),
        query_gain.reshape(1, -1),
        key_gain.reshape(1, -1),
        offset_bias.transpose(1, 0, 2),
    )


def fused_fits(latent, context, condition, query_weight, n_sp, n_tp):
    rows, c_rows = latent.shape[0] // n_sp, context.shape[0] // n_sp
    width = query_weight.shape[1] // n_tp
    return (
        rows == WIN_ROWS // 2 * GRID_W
        and c_rows % 32 == 0
        and condition.shape[0] // n_sp % 128 == 0
        and condition.shape[0] // n_tp % 256 == 0
        and condition.shape[0] // n_tp <= 1024
        and width == 2 * LANES
        and n_tp == 4
        and n_sp == 8
    )


def solution(mesh):
    in_specs = (
        P("sp", None),
        P("sp", None),
        P("sp"),
        P("sp"),
        P("sp", "tp"),
        P("sp", "tp"),
        P("sp", "tp"),
        P(),
        P(None, "tp"),
        P(None, "tp"),
        P(None, "tp"),
        P(),
        P(),
        P("tp", None, None),
        P("tp", None),
    )
    out_specs = P("sp", None)

    def step(latent, context, condition, ctx_condition, *rest):
        n_sp, n_tp = mesh.shape["sp"], mesh.shape["tp"]
        fits = fused_fits(latent, context, condition, rest[4], n_sp, n_tp)
        body = per_device if fits else per_device_plain
        return jax.shard_map(
            body, mesh=mesh, in_specs=in_specs, out_specs=out_specs, check_vma=False
        )(latent, context, condition, ctx_condition, *rest)

    return step
```

```python
import functools

import jax
import jax.numpy as jnp
from jax import lax
from jax.experimental import pallas as pl
from jax.experimental.pallas import tpu as pltpu
from jax.sharding import PartitionSpec as P

HEAD_DIM = 64
GRID_W = 64
WIN_ROWS = 8
WIN_COLS = 16


EPS = 1e-06


def extended(x, sides, width):
    for axis, dim in sides:
        count, length = (lax.axis_size(axis), x.shape[dim])
        up = [(i, (i + 1) % count) for i in range(count - 1)]
        down = [(j, i) for i, j in up]
        last = lax.slice_in_dim(x, length - width, length, axis=dim)
        initial = lax.slice_in_dim(x, 0, width, axis=dim)
        before = lax.ppermute(last, axis, up)
        after = lax.ppermute(initial, axis, down)
        x = jnp.concatenate([before, x, after], axis=dim)
    return x


def modulate(rows_in, norm_gain, shift_vec, scale_vec):
    values = rows_in.astype(jnp.float32)
    normed = values * lax.rsqrt(jnp.mean(values * values, axis=-1, keepdims=True) + EPS)
    return (normed * norm_gain * (1.0 + scale_vec) + shift_vec).astype(jnp.bfloat16)


def head_norm(projected, head_gain):
    row_count = projected.shape[0]
    split_heads = projected.reshape(row_count, -1, head_gain.shape[0])
    normed = split_heads * lax.rsqrt(
        jnp.mean(split_heads * split_heads, axis=-1, keepdims=True) + EPS
    )
    return (normed * head_gain).astype(jnp.bfloat16).reshape(row_count, -1)


def per_device_plain(
    latent,
    context,
    condition,
    ctx_condition,
    shift_weight,
    scale_weight,
    gate_weight,
    norm_gain,
    query_weight,
    key_weight,
    value_weight,
    query_gain,
    key_gain,
    offset_bias,
    out_weight,
):
    activations = jax.nn.silu(jnp.stack([condition, ctx_condition])).astype(jnp.bfloat16)
    part_shift = jnp.dot(activations, shift_weight, preferred_element_type=jnp.float32)
    part_scale = jnp.dot(activations, scale_weight, preferred_element_type=jnp.float32)
    part_gate = jnp.dot(activations[:1], gate_weight, preferred_element_type=jnp.float32)
    block_cols = shift_weight.shape[1]
    first_col = lax.axis_index("tp") * block_cols

    def spread(piece_part):
        padded_vec = jnp.zeros((piece_part.shape[0], block_cols * lax.axis_size("tp")), jnp.float32)
        return lax.dynamic_update_slice_in_dim(padded_vec, piece_part, first_col, 1)

    shift_vec, scale_vec, gate_vec = lax.psum(
        (spread(part_shift), spread(part_scale), spread(part_gate)), ("sp", "tp")
    )
    hidden = modulate(latent, norm_gain, shift_vec[0], scale_vec[0])
    queries = head_norm(
        jnp.dot(hidden, query_weight, preferred_element_type=jnp.float32), query_gain
    )
    keys_lat = head_norm(jnp.dot(hidden, key_weight, preferred_element_type=jnp.float32), key_gain)
    values_lat = jnp.dot(hidden, value_weight, preferred_element_type=jnp.float32).astype(
        jnp.bfloat16
    )
    ctx_hidden = modulate(
        lax.all_gather(context, "sp", axis=0, tiled=True), norm_gain, shift_vec[1], scale_vec[1]
    )
    ctx_keys = head_norm(
        jnp.dot(ctx_hidden, key_weight, preferred_element_type=jnp.float32), key_gain
    )
    ctx_values = jnp.dot(ctx_hidden, value_weight, preferred_element_type=jnp.float32).astype(
        jnp.bfloat16
    )
    ctx_pairs = jnp.concatenate([ctx_keys, ctx_values], axis=1)
    col_width = keys_lat.shape[1]
    heads_dev = col_width // HEAD_DIM
    local_rows = keys_lat.shape[0] // GRID_W
    halo_rows = WIN_ROWS // 2
    window_keys = WIN_ROWS * GRID_W
    key_value = jnp.concatenate([keys_lat, values_lat], axis=1).reshape(
        local_rows, GRID_W, 2 * col_width
    )
    padded = extended(key_value, (("sp", 0),), halo_rows)
    first_row = lax.axis_index("sp") * local_rows
    total_rows = local_rows * lax.axis_size("sp")
    global_rows = first_row + jnp.arange(local_rows, dtype=jnp.int32)
    band_start = jnp.clip(global_rows - halo_rows, 0, total_rows - WIN_ROWS)
    band_global = band_start[:, None] + jnp.arange(WIN_ROWS, dtype=jnp.int32)[None, :]
    banded = jnp.take(padded, band_global - first_row + halo_rows, axis=0)
    key_band = banded[..., :col_width].reshape(local_rows, window_keys, heads_dev, HEAD_DIM)
    value_band = banded[..., col_width:].reshape(local_rows, window_keys, heads_dev, HEAD_DIM)
    row_steps = band_global - global_rows[:, None] + WIN_ROWS - 1
    row_hot = (
        row_steps[:, :, None] == jnp.arange(2 * WIN_ROWS - 1, dtype=jnp.int32)[None, None, :]
    ).astype(jnp.float32)
    column_ids = jnp.arange(GRID_W, dtype=jnp.int32)
    col_steps = (
        jnp.clip(column_ids[None, :] - column_ids[:, None], 1 - WIN_COLS, WIN_COLS - 1)
        + WIN_COLS
        - 1
    )
    col_hot = (
        col_steps[:, :, None] == jnp.arange(2 * WIN_COLS - 1, dtype=jnp.int32)[None, None, :]
    ).astype(jnp.float32)
    col_start = jnp.clip(column_ids - WIN_COLS // 2, 0, GRID_W - WIN_COLS)
    col_open = (column_ids[None, :] >= col_start[:, None]) & (
        column_ids[None, :] < col_start[:, None] + WIN_COLS
    )
    col_table = jnp.einsum("hab,qkb->haqk", offset_bias, col_hot, precision=lax.Precision.HIGHEST)
    col_table = jnp.where(col_open[None, None, :, :], col_table, -jnp.inf)
    offset_terms = jnp.einsum(
        "rja,haqk->hrqjk",
        row_hot,
        jnp.where(col_open[None, None], col_table, 0.0),
        precision=lax.Precision.HIGHEST,
    )
    offset_terms = jnp.where(col_open[None, None, :, None, :], offset_terms, -jnp.inf)
    offset_terms = offset_terms.reshape(heads_dev, local_rows, GRID_W, window_keys)
    score_scale = HEAD_DIM ** (-0.5)
    q_grid = queries.reshape(local_rows, GRID_W, heads_dev, HEAD_DIM)
    scores = (
        jnp.einsum("rqhd,rnhd->hrqn", q_grid, key_band, preferred_element_type=jnp.float32)
        * score_scale
        + offset_terms
    )
    ctx_count = ctx_pairs.shape[0]
    ctx_keys_all = ctx_pairs[:, :col_width].reshape(ctx_count, heads_dev, HEAD_DIM)
    ctx_values_all = ctx_pairs[:, col_width:].reshape(ctx_count, heads_dev, HEAD_DIM)
    ctx_scores = (
        jnp.einsum("rqhd,nhd->hrqn", q_grid, ctx_keys_all, preferred_element_type=jnp.float32)
        * score_scale
    )
    row_max = jnp.maximum(jnp.max(scores, axis=3), jnp.max(ctx_scores, axis=3))
    local_exp = jnp.exp(scores - row_max[..., None])
    ctx_exp = jnp.exp(ctx_scores - row_max[..., None])
    denominator = jnp.sum(local_exp, axis=3) + jnp.sum(ctx_exp, axis=3)
    local_weights = (local_exp / denominator[..., None]).astype(jnp.bfloat16)
    ctx_weights = (ctx_exp / denominator[..., None]).astype(jnp.bfloat16)
    combined = jnp.einsum(
        "hrqn,rnhd->rqhd", local_weights, value_band, preferred_element_type=jnp.float32
    ) + jnp.einsum(
        "hrqn,nhd->rqhd", ctx_weights, ctx_values_all, preferred_element_type=jnp.float32
    )
    attended = combined.astype(jnp.bfloat16).reshape(local_rows * GRID_W, col_width)
    partial_value = jnp.dot(attended, out_weight, preferred_element_type=jnp.float32)
    branch = lax.psum(partial_value.astype(jnp.bfloat16), "tp").astype(jnp.float32)
    return (latent.astype(jnp.float32) + gate_vec[0] * branch).astype(jnp.bfloat16)


MESH = pl.DeviceIdType.MESH
MASKED = -1e30
LANES = 128
F32 = jnp.float32
BF16 = jnp.bfloat16


def fused_kernel(
    n_sp,
    n_tp,
    latent,
    context,
    shift_w,
    scale_w,
    gate_w,
    query_w,
    key_w,
    value_w,
    out_w,
    cond,
    ctx_cond,
    norm_gain,
    query_gain,
    key_gain,
    bias_in,
    out,
    cond_v,
    ctx_cond_v,
    norm_gain_v,
    query_gain_v,
    key_gain_v,
    bias_v,
    x_in,
    x_norm,
    hid,
    w_mod,
    w_qkv,
    w_out,
    mod_sp,
    mod_tp,
    part_kv,
    part_q,
    gate_sp,
    gate_tp,
    acc,
    q_stage,
    k_stage,
    v_stage,
    ck_stage,
    cv_stage,
    q_all,
    k_all,
    v_all,
    ctx_k,
    ctx_v,
    bias_pad,
    bias_lines,
    table,
    q_heads,
    scores,
    tops,
    sums,
    scores_ctx,
    weights,
    sums_ctx,
    att_slab,
    att,
    local_sem,
    mod_send,
    mod_recv,
    modt_send,
    modt_recv,
    gate_send,
    gate_recv,
    gatet_send,
    gatet_recv,
    pair_send,
    pair_recv,
    halo_send,
    halo_recv,
    ctx_send,
    ctx_recv,
    end_send,
    wo_send,
    wo_recv,
    att_send,
    att_recv,
):
    me_s, me_t = lax.axis_index("sp"), lax.axis_index("tp")
    rows, d = latent.shape
    c_rows = context.shape[0]
    width = key_w.shape[1]
    heads = width // HEAD_DIM
    block = shift_w.shape[1]
    blocks = block // 128
    l_rows = rows // GRID_W
    halo = WIN_ROWS // 2
    win = WIN_ROWS * GRID_W
    core = lax.rem(me_t, 2)
    chip = lax.div(me_t, 2)
    partner = me_t + 1 - 2 * core
    far = 2 * (1 - chip) + core
    far_partner = 2 * (1 - chip) + 1 - core
    side = lax.rem(me_s, 2)
    slab = lax.div(me_s, 2)
    mate = me_s + 1 - 2 * side
    last_slab = n_sp // 2 - 1
    half = width // 2
    half_heads = heads // 2

    def remote(src, dst, send, recv, s, t):
        return pltpu.make_async_remote_copy(
            src_ref=src, dst_ref=dst, send_sem=send, recv_sem=recv,
            device_id=(s, t), device_id_type=MESH,
        )

    barrier = pltpu.get_barrier_semaphore()
    for k in range(1, n_sp):
        pl.semaphore_signal(
            barrier, inc=1, device_id=(lax.rem(me_s + k, n_sp), me_t), device_id_type=MESH
        )
    for k in range(1, n_tp):
        pl.semaphore_signal(
            barrier, inc=1, device_id=(me_s, lax.rem(me_t + k, n_tp)), device_id_type=MESH
        )
    pl.semaphore_signal(barrier, inc=1, device_id=(mate, far), device_id_type=MESH)

    loads = [
        (shift_w, w_mod.at[0]),
        (scale_w, w_mod.at[1]),
        (gate_w, w_mod.at[2]),
        (context, x_in.at[pl.ds(0, c_rows)]),
        (latent, x_in.at[pl.ds(c_rows, rows)]),
        (key_w, w_qkv.at[:, pl.ds(0, width)]),
        (value_w, w_qkv.at[:, pl.ds(width, width)]),
        (query_w, w_qkv.at[:, pl.ds(2 * width, width)]),
        (out_w, w_out.at[me_t]),
        (cond, cond_v),
        (ctx_cond, ctx_cond_v),
        (norm_gain, norm_gain_v),
        (query_gain, query_gain_v),
        (key_gain, key_gain_v),
        (bias_in, bias_v),
    ]
    copies = [pltpu.make_async_copy(a, b, local_sem.at[i]) for i, (a, b) in enumerate(loads)]
    for i in (9, 10, 0, 1, 2, 11, 12, 13, 14, 3, 4):
        copies[i].start()

    def silu(v):
        return v / (1.0 + jnp.exp(-v))

    two = (16, cond.shape[1])
    row_id = lax.broadcasted_iota(jnp.int32, two, 0)
    copies[9].wait()
    copies[10].wait()
    act0 = jnp.broadcast_to(silu(cond_v[...]), two)
    act1 = jnp.broadcast_to(silu(ctx_cond_v[...]), two)

    def placed(first, second):
        picked = jnp.where(row_id == first, act0, 0.0)
        if second is not None:
            picked = jnp.where(row_id == second, act1, picked)
        return picked.astype(BF16)

    part = jnp.zeros((16, block), F32)
    for i in range(2):
        copies[i].wait()
        part += jnp.dot(placed(2 * i, 2 * i + 1), w_mod[i], preferred_element_type=F32)
    for b in range(blocks):
        mod_sp[me_s, 4 * b : 4 * b + 4, :] = part[:4, b * 128 : (b + 1) * 128]
    pl.semaphore_wait(barrier, n_sp + n_tp - 1)
    sends = []

    def share_sp(buf, send, recv):
        for k in range(1, n_sp):
            away_first = jnp.where(slab <= last_slab // 2, n_sp - k, k)
            peer = lax.rem(me_s + away_first, n_sp)
            c = remote(buf.at[me_s], buf.at[me_s], send.at[k], recv.at[me_s], peer, me_t)
            c.start()
            sends.append(c)

    def sum_sp(buf, send, recv):
        for k in range(1, n_sp):
            peer = lax.rem(me_s + k, n_sp)
            remote(buf.at[peer], buf.at[peer], send.at[k], recv.at[peer], peer, me_t).wait_recv()
        total = buf[0]
        for k in range(1, n_sp):
            total = total + buf[k]
        return total

    def share_tp(buf, send, recv):
        for k in range(1, n_tp):
            peer = lax.rem(me_t + k, n_tp)
            c = remote(buf.at[me_t], buf.at[me_t], send.at[k], recv.at[me_t], me_s, peer)
            c.start()
            sends.append(c)

    def wait_tp(buf, send, recv):
        for k in range(1, n_tp):
            peer = lax.rem(me_t + k, n_tp)
            remote(buf.at[peer], buf.at[peer], send.at[k], recv.at[peer], me_s, peer).wait_recv()

    share_sp(mod_sp, mod_send, mod_recv)
    for i in (5, 6, 7, 8):
        copies[i].start()
    copies[2].wait()
    gate_part = jnp.dot(placed(0, None), w_mod[2], preferred_element_type=F32)
    for b in range(blocks):
        gate_sp[me_s, b : b + 1, :] = gate_part[:1, b * 128 : (b + 1) * 128]

    piece = width // 16
    n_cross, n_direct = 3, 4
    n_pieces = 2 * n_cross + n_direct
    early = (0, n_cross)
    later = [c + o for c in range(1, n_cross) for o in (0, n_cross)]
    later = later + list(range(2 * n_cross, n_pieces))
    z_side = lax.rem(slab, 2)
    z_mate = me_s + 2 - 4 * z_side

    def wo_rows(c, away_from):
        if c < n_cross:
            start = (side + away_from - 2 * side * away_from) * n_cross * piece + c * piece
        elif c < 2 * n_cross:
            start = (
                2 * n_cross * piece
                + (z_side + away_from - 2 * z_side * away_from) * n_cross * piece
                + (c - n_cross) * piece
            )
        else:
            start = (2 * n_cross + c) * piece
        return pl.ds(pl.multiple_of(start, piece), piece)

    def wo_copy(kind, c, source, shard, rows_at, s, t):
        return remote(
            source.at[rows_at], w_out.at[shard, rows_at],
            wo_send.at[kind, c], wo_recv.at[kind, c], s, t,
        )

    def begin(c):
        c.start()
        sends.append(c)

    def wo_far(c):
        return wo_copy(0, c, out_w, me_t, wo_rows(c, 0), me_s, far)

    def wo_forward(c):
        at_rows = wo_rows(c, 0)
        came = w_out.at[far]
        wo_copy(0, c, came, far, at_rows, me_s, far).wait_recv()
        begin(wo_copy(1, c, came, far, at_rows, me_s, partner))
        if c < 2 * n_cross:
            begin(wo_copy(2, c, came, far, at_rows, mate if c < n_cross else z_mate, me_t))

    def wo_cross(c):
        at_rows = wo_rows(c, 1)
        came = w_out.at[far]
        wo_copy(2, c, came, far, at_rows, mate, me_t).wait_recv()
        begin(wo_copy(3, c, came, far, at_rows, me_s, partner))

    def wo_finish_far():
        for c in range(n_pieces):
            wo_copy(
                1, c, w_out.at[far_partner], far_partner, wo_rows(c, 0), me_s, partner
            ).wait_recv()
        for c in range(2 * n_cross):
            wo_copy(
                3, c, w_out.at[far_partner], far_partner, wo_rows(c, 1), me_s, partner
            ).wait_recv()

    def wo_partner():
        return remote(
            out_w, w_out.at[me_t], wo_send.at[4, 0], wo_recv.at[4, 0], me_s, partner
        )

    for c in early:
        begin(wo_far(c))

    copies[3].wait()
    copies[4].wait()
    copies[11].wait()
    step = 32

    def norm_rows(i, carry):
        at = pl.ds(pl.multiple_of(i * step, step), step)
        v = x_in[at, :].astype(F32)
        r = lax.rsqrt(jnp.mean(v * v, axis=-1, keepdims=True) + EPS)
        x_norm[at, :] = v * r * norm_gain_v[...]
        return carry

    lax.fori_loop(0, (rows + c_rows) // step, norm_rows, 0)

    pair = 2 * GRID_W
    q_col = lax.broadcasted_iota(jnp.int32, (GRID_W, pair), 0)
    k_col = lax.broadcasted_iota(jnp.int32, (GRID_W, pair), 1) % GRID_W
    col0 = jnp.clip(q_col - WIN_COLS // 2, 0, GRID_W - WIN_COLS)
    col_open = (k_col >= col0) & (k_col < col0 + WIN_COLS)
    n_pairs = 2 * WIN_ROWS - 2
    copies[14].wait()
    bias_pad[...] = jnp.zeros_like(bias_pad)
    for h in range(heads):
        bias_pad[h, : 2 * WIN_ROWS - 1, : 2 * WIN_COLS - 1] = bias_v[:, h, :]
    for h in range(half_heads):
        head = side * half_heads + h
        upper = pltpu.roll(bias_pad[head, 1 : n_pairs + 1, :], GRID_W, 1)
        bias_lines[h, :n_pairs, :] = bias_pad[head, :n_pairs, :] + upper
        for a in range(n_pairs):
            line = jnp.broadcast_to(bias_lines[h, a : a + 1, :], (GRID_W, pair))
            rolled = pltpu.roll(line, pair - (WIN_COLS - 1), 1, stride=1, stride_axis=0)
            table[a, h * GRID_W : (h + 1) * GRID_W, :] = jnp.where(col_open, rolled, MASKED)

    mod_tp[me_t] = sum_sp(mod_sp, mod_send, mod_recv)
    share_tp(mod_tp, modt_send, modt_recv)
    for c in later:
        begin(wo_far(c))
    share_sp(gate_sp, gate_send, gate_recv)

    def wait_mod(peer):
        remote(
            mod_tp.at[peer], mod_tp.at[peer], modt_send.at[1], modt_recv.at[peer], me_s, peer
        ).wait_recv()

    pair_cols = 2 * block

    def vec(which, r):
        return jnp.concatenate(
            [
                mod_tp[2 * which + j, 4 * b + r : 4 * b + r + 1, :]
                for j in range(2)
                for b in range(blocks)
            ],
            axis=1,
        )

    def cols_of(which):
        return pl.ds(pl.multiple_of(which * pair_cols, pair_cols), pair_cols)

    def modulate_rows(which, first, count, shift, scale):
        def body(i, carry):
            at = pl.ds(pl.multiple_of(first + i * step, step), step)
            hid[at, cols_of(which)] = (x_norm[at, cols_of(which)] * scale + shift).astype(BF16)
            return carry

        lax.fori_loop(0, count // step, body, 0)

    def modulate_pair(which):
        modulate_rows(which, 0, c_rows, vec(which, 1), 1.0 + vec(which, 3))
        modulate_rows(which, c_rows, rows, vec(which, 0), 1.0 + vec(which, 2))

    def hidden_dot(which, start_row, start_col, count_col):
        return jnp.dot(
            hid[start_row:, cols_of(which)],
            w_qkv[cols_of(which), start_col : start_col + count_col],
            preferred_element_type=F32,
        )

    wait_mod(partner)
    modulate_pair(chip)
    for i in (5, 6, 7):
        copies[i].wait()
    part_kv[...] = hidden_dot(chip, 0, 0, 2 * width)
    part_q[...] = hidden_dot(chip, c_rows, 2 * width, width)
    for c in early:
        wo_forward(c)
    wait_mod(far)
    wait_mod(far_partner)
    head_row = lax.broadcasted_iota(jnp.int32, (width, width), 0) // HEAD_DIM
    head_col = lax.broadcasted_iota(jnp.int32, (width, width), 1) // HEAD_DIM
    same_head = (head_row == head_col).astype(BF16)
    copies[12].wait()
    copies[13].wait()

    def head_scale(p, gain):
        squares = p * p
        high = squares.astype(BF16)
        low = (squares - high.astype(F32)).astype(BF16)
        mean = jnp.dot(high, same_head, preferred_element_type=F32)
        mean = mean + jnp.dot(low, same_head, preferred_element_type=F32)
        mean = mean * (1.0 / HEAD_DIM)
        wide_gain = jnp.concatenate([gain[...]] * heads, axis=1)
        return (p * lax.rsqrt(mean + EPS) * wide_gain).astype(BF16)

    own = pl.ds(rows + pl.multiple_of(side * rows, rows), rows)
    other = pl.ds(rows + pl.multiple_of((1 - side) * rows, rows), rows)

    def split(stage, value):
        for h in range(2):
            stage[h] = value[:, h * half : (h + 1) * half]

    def trade(index, stage, block_all, at):
        c = remote(
            stage.at[1 - side], block_all.at[at], pair_send.at[index], pair_recv.at[index],
            mate, me_t,
        )
        c.start()
        sends.append(c)
        return c

    n_z = n_sp // 2
    z_order = tuple(range(2, n_z)) + (1,)

    def ctx_copy(index, slot, source, shard, block_ctx, s):
        return remote(
            source, block_ctx.at[shard], ctx_send.at[index, slot], ctx_recv.at[index, shard],
            s, me_t,
        )

    at_end = (slab == 0) | (slab == last_slab)
    sends_when = []

    def along_z(index, slot, source, shard, block_ctx, all_direct=False):
        for k in z_order:
            peer = lax.rem(slab + k, n_z)
            c = ctx_copy(index, slot + k, source, shard, block_ctx, 2 * peer + side)
            low = (peer == 0) & (slab >= 2)
            high = (peer == last_slab) & (slab <= last_slab - 2)
            if all_direct:
                begin(c)
                continue
            direct = jnp.logical_not(low | high)
            pl.when(direct)(c.start)
            sends_when.append((direct, c))

    z_pair = lax.div(slab, 2)

    def relay_end(of_side):
        def body():
            for j in range(2):
                shard = 2 * (2 * (1 - z_pair) + j) + of_side
                for index, block_ctx in enumerate((ctx_k, ctx_v)):
                    ctx_copy(index, 0, block_ctx.at[shard], shard, block_ctx, shard).wait_recv()
                    end_copy(index, shard, block_ctx).start()

        pl.when(jnp.logical_not(at_end))(body)
        for j in range(2):
            shard = 2 * (2 * (1 - z_pair) + j) + of_side
            for index, block_ctx in enumerate((ctx_k, ctx_v)):
                sends_when.append((jnp.logical_not(at_end), end_copy(index, shard, block_ctx)))

    def end_copy(index, shard, block_ctx):
        return remote(
            block_ctx.at[shard], block_ctx.at[shard],
            end_send.at[index, shard], ctx_recv.at[index, shard],
            2 * z_pair * last_slab + side, me_t,
        )


    def relay_ctx(index, block_ctx):
        ctx_copy(index, 0, block_ctx.at[mate], mate, block_ctx, mate).wait_recv()
        along_z(index, n_z - 1, block_ctx.at[mate], mate, block_ctx, True)

    lower = rows - GRID_W

    def halo_copies(index, block_all):
        down = remote(
            block_all.at[pl.ds(rows, lower)], block_all.at[pl.ds(3 * rows, lower)],
            halo_send.at[index, 0], halo_recv.at[index, 0], me_s - 2, me_t,
        )
        up = remote(
            block_all.at[pl.ds(2 * rows, rows)], block_all.at[pl.ds(0, rows)],
            halo_send.at[index, 1], halo_recv.at[index, 1], me_s + 2, me_t,
        )
        return down, up

    def halo_start(mine, index, block_all):
        down, up = halo_copies(index, block_all)
        is_low = side == 0 if mine else side == 1

        @pl.when(is_low & (slab > 0))
        def _():
            down.start()

        @pl.when(jnp.logical_not(is_low) & (slab < last_slab))
        def _():
            up.start()

    away = 1 - chip
    modulate_rows(away, 0, c_rows, vec(away, 1), 1.0 + vec(away, 3))
    ctx_both = part_kv[:c_rows, :] + jnp.dot(
        hid[:c_rows, cols_of(away)], w_qkv[cols_of(away), : 2 * width], preferred_element_type=F32
    )
    ctx_keys = head_scale(ctx_both[:, :width], key_gain_v)
    ctx_values = ctx_both[:, width:].astype(BF16)
    split(ck_stage, ctx_keys)
    split(cv_stage, ctx_values)
    for index, (stage, block_ctx) in enumerate(((ck_stage, ctx_k), (cv_stage, ctx_v))):
        begin(ctx_copy(index, 0, stage.at[1 - side], me_s, block_ctx, mate))
        along_z(index, 0, stage.at[side], me_s, block_ctx)
        block_ctx[me_s] = stage[side]
    modulate_rows(away, c_rows, rows, vec(away, 0), 1.0 + vec(away, 2))
    both = part_kv[c_rows:, :] + hidden_dot(away, c_rows, 0, 2 * width)
    keys = head_scale(both[:, :width], key_gain_v)
    split(k_stage, keys)
    k_trade = trade(0, k_stage, k_all, own)
    k_all[own, :] = k_stage[side]
    halo_start(True, 0, k_all)
    split(v_stage, both[:, width:].astype(BF16))
    v_trade = trade(1, v_stage, v_all, own)
    v_all[own, :] = v_stage[side]
    halo_start(True, 1, v_all)
    queries = head_scale(
        part_q[...] + hidden_dot(away, c_rows, 2 * width, width), query_gain_v
    ) * jnp.asarray(HEAD_DIM ** (-0.5), BF16)
    split(q_stage, queries)
    q_own = pl.ds(pl.multiple_of(side * rows, rows), rows)
    q_trade = trade(2, q_stage, q_all, q_own)
    q_all[q_own, :] = q_stage[side]
    begin(wo_partner())
    gate_tp[me_t] = sum_sp(gate_sp, gate_send, gate_recv)
    share_tp(gate_tp, gatet_send, gatet_recv)
    relay_ctx(0, ctx_k)
    relay_ctx(1, ctx_v)
    relay_end(side)
    k_trade.wait_recv()
    halo_start(False, 0, k_all)
    for c in range(1, n_cross):
        wo_forward(c)
    v_trade.wait_recv()
    halo_start(False, 1, v_all)
    def halo_wait(theirs_need):
        below = side == 0 if theirs_need else side == 1
        for index, block_all in enumerate((k_all, v_all)):
            down, up = halo_copies(index, block_all)

            @pl.when(below & (slab < last_slab))
            def _():
                down.wait_recv()

            @pl.when(jnp.logical_not(below) & (slab > 0))
            def _():
                up.wait_recv()

    lane_head = lax.broadcasted_iota(jnp.int32, (GRID_W, half), 1) // HEAD_DIM
    masks = [(lane_head == h).astype(F32) for h in range(half_heads)]
    contract_last = (((1,), (1,)), ((), ()))
    stack = half_heads * GRID_W
    ones = jnp.ones((win, 128), BF16)

    def stacked(i):
        qi = q_all[pl.ds(pl.multiple_of(i * GRID_W, GRID_W), GRID_W), :].astype(F32)
        return jnp.concatenate([(qi * m).astype(BF16) for m in masks], axis=0)

    def score_local(i, held_at, slot):
        start = jnp.where(
            slab == 0,
            jnp.maximum(i, halo),
            jnp.where(slab == last_slab, jnp.minimum(i, halo), i),
        )
        if last_slab == 0:
            start = jnp.int32(halo)
        at = pl.ds(pl.multiple_of(start * GRID_W, GRID_W), win)
        qs = stacked(i)
        q_heads[held_at] = qs
        s = lax.dot_general(qs, k_all[at, :], contract_last, preferred_element_type=F32)
        first = start - i + WIN_ROWS - 1 - halo
        s = s + jnp.concatenate([table[first + 2 * m] for m in range(WIN_ROWS // 2)], axis=1)
        scores[slot] = s
        return at, jnp.max(s, axis=1, keepdims=True)

    def weigh_local(held_at, slot, at, top):
        e = jnp.exp(scores[slot] - top)
        tops[held_at] = jnp.broadcast_to(top, (stack, 128))
        values_at = jnp.concatenate([v_all[at, :], ones], axis=1)
        sums[held_at] = jnp.dot(e.astype(BF16), values_at, preferred_element_type=F32)

    def local_half(which, base):
        first = which * l_rows
        held = score_local(first, base, 0)
        for i in range(l_rows):
            later = None
            if i + 1 < l_rows:
                later = score_local(first + i + 1, base + i + 1, (i + 1) % 2)
            weigh_local(base + i, i % 2, *held)
            held = later

    def ctx_wait(wait_near):
        for index, block_ctx in enumerate((ctx_k, ctx_v)):
            for s in range(n_sp):

                relayed = jnp.logical_not(at_end) & (z_pair != s // 4) & (side == s % 2)

                wanted = (z_pair == s // 4) if wait_near else (z_pair != s // 4)

                @pl.when((s != me_s) & (s != mate) & jnp.logical_not(relayed) & wanted)
                def _():
                    ctx_copy(index, 0, block_ctx.at[s], s, block_ctx, s).wait_recv()

    top_head = lax.broadcasted_iota(jnp.int32, (GRID_W, half), 1) // HEAD_DIM
    half_stack = l_rows * stack
    n_ctx = n_sp * c_rows
    ctx_ones = jnp.ones((n_ctx, 128), BF16)

    n_part = n_ctx // 2
    shards_part = n_sp // 2

    def ctx_scores(base, first_shard, n_keys, exp_all):
        shards = pl.ds(first_shard, n_keys // c_rows)
        qs = q_heads[base : base + l_rows].reshape(half_stack, half)
        scores_ctx[:, :n_keys] = lax.dot_general(
            qs, ctx_k[shards].reshape(n_keys, half), contract_last, preferred_element_type=F32
        )
        fades = []
        for i in range(l_rows):
            at_rows = slice(i * stack, (i + 1) * stack)
            s = scores_ctx[at_rows, :n_keys]
            old = tops[base + i]
            top = jnp.maximum(old, jnp.max(s, axis=1, keepdims=True))
            fade = jnp.exp(old - top)
            fades.append(jnp.concatenate([fade] * ((half + 128) // 128), axis=1))
            if exp_all:
                tops[base + i] = top
            wide_top = jnp.concatenate([top] * (n_keys // 128), axis=1)
            weights[at_rows, :n_keys] = jnp.exp(s - wide_top).astype(BF16)
        values_ctx = jnp.concatenate(
            [ctx_v[shards].reshape(n_keys, half), ctx_ones[:n_keys]], axis=1
        )
        sums_ctx[...] = jnp.dot(
            weights[:, :n_keys], values_ctx, preferred_element_type=F32
        )
        return fades

    def ctx_near(base):
        fades = ctx_scores(base, shards_part * z_pair, n_part, True)
        for i in range(l_rows):
            at_rows = slice(i * stack, (i + 1) * stack)
            sums[base + i] = sums_ctx[at_rows, :] + sums[base + i] * fades[i]

    def finished(o):
        up, down = o[:, :half], o[:, half:]
        num, den = up[:GRID_W], down[:GRID_W]
        for h in range(1, half_heads):
            part_h = slice(h * GRID_W, (h + 1) * GRID_W)
            num = jnp.where(top_head == h, up[part_h], num)
            den = jnp.where(top_head == h, down[part_h], den)
        return (num / den).astype(BF16)

    def ctx_last(base, store):
        fades = ctx_scores(base, shards_part * (1 - z_pair), n_part, False)
        for i in range(l_rows):
            at_rows = slice(i * stack, (i + 1) * stack)
            o = sums_ctx[at_rows, :] + sums[base + i] * fades[i]
            store(i, finished(o))

    def att_copy(index, source, dest, s, t):
        return remote(source, dest, att_send.at[index], att_recv.at[index], s, t)

    def store_theirs(i, value):
        att_slab[i * GRID_W : (i + 1) * GRID_W, :] = value

    def store_mine(i, value):
        att[me_t, side, i * GRID_W : (i + 1) * GRID_W, :] = value

    def ctx_start():
        for i in range(l_rows):
            q_heads[l_rows + i] = stacked(side * l_rows + i)
        qs = q_heads[l_rows : 2 * l_rows].reshape(half_stack, half)
        scores_ctx[...] = lax.dot_general(
            qs, ctx_k[...].reshape(n_ctx, half), contract_last, preferred_element_type=F32
        )
        for i in range(l_rows):
            at_rows = slice(i * stack, (i + 1) * stack)
            s = scores_ctx[at_rows, :]
            top = jnp.broadcast_to(jnp.max(s, axis=1, keepdims=True), (stack, 128))
            tops[l_rows + i] = top
            wide_top = jnp.concatenate([top] * (n_ctx // 128), axis=1)
            weights[at_rows, :] = jnp.exp(s - wide_top).astype(BF16)
        values_ctx = jnp.concatenate([ctx_v[...].reshape(n_ctx, half), ctx_ones], axis=1)
        sums_ctx[...] = jnp.dot(weights[...], values_ctx, preferred_element_type=F32)

    def local_last():
        first = side * l_rows
        held = score_local(first, l_rows, 0)
        for i in range(l_rows):
            later = None
            if i + 1 < l_rows:
                later = score_local(first + i + 1, l_rows + i + 1, (i + 1) % 2)
            at, top = held
            at_rows = slice(i * stack, (i + 1) * stack)
            old = tops[l_rows + i]
            top = jnp.maximum(old, top)
            wide_top = jnp.concatenate([top] * (win // 128), axis=1)
            e = jnp.exp(scores[i % 2] - wide_top)
            values_at = jnp.concatenate([v_all[at, :], ones], axis=1)
            o = jnp.dot(e.astype(BF16), values_at, preferred_element_type=F32)
            fade = jnp.exp(old - top)
            o = o + sums_ctx[at_rows, :] * jnp.concatenate([fade] * ((half + 128) // 128), axis=1)
            store_mine(i, finished(o))
            held = later

    def local_mine():
        halo_wait(False)
        local_half(side, l_rows)

    n_early = len(sends)
    for c in range(n_cross + 1, 2 * n_cross):
        wo_forward(c)
    no_halo = ((slab == 0) & (side == 0)) | ((slab == last_slab) & (side == 1))
    @pl.when(no_halo)
    def _():
        local_mine()
        ctx_wait(True)
        ctx_near(l_rows)

    q_trade.wait_recv()
    halo_wait(True)
    local_half(1 - side, 0)
    @pl.when(jnp.logical_not(no_halo))
    def _():
        ctx_wait(True)

    ctx_near(0)
    ctx_wait(False)
    ctx_last(0, store_theirs)
    begin(att_copy(0, att_slab, att.at[me_t, side], mate, far))
    begin(att_copy(1, att_slab, att.at[me_t, side], mate, me_t))
    @pl.when(no_halo)
    def _():
        ctx_last(l_rows, store_mine)

    @pl.when(jnp.logical_not(no_halo))
    def _():
        ctx_start()
        halo_wait(False)
        local_last()

    begin(att_copy(2, att.at[me_t, side], att.at[me_t, side], me_s, far))
    begin(att_copy(3, att.at[me_t, side], att.at[me_t, side], me_s, partner))

    def arrived(index, shard, part_of):
        return att_copy(index, att.at[shard, part_of], att.at[shard, part_of], me_s, partner)

    def pass_on(index, onto, shard, part_of):
        arrived(index, shard, part_of).wait_recv()
        begin(arrived(onto, shard, part_of))

    for c in range(2 * n_cross, n_pieces):
        wo_forward(c)
    for c in range(2 * n_cross):
        wo_cross(c)
    wait_tp(gate_tp, gatet_send, gatet_recv)
    gate = jnp.concatenate(
        [gate_tp[j, b : b + 1, :] for j in range(n_tp) for b in range(blocks)], axis=1
    )
    copies[8].wait()
    cols = 512

    def project(groups, first_pass, last_pass):
        heads_of = [jnp.concatenate([att[j, 0], att[j, 1]], axis=1) for j in groups]
        for n in range(d // cols):
            at = slice(n * cols, (n + 1) * cols)
            total = None if first_pass else acc[:, at]
            for j, lhs in zip(groups, heads_of):
                term = jnp.dot(lhs, w_out[j, :, at], preferred_element_type=F32)
                term = term.astype(BF16).astype(F32)
                total = term if total is None else total + term
            if last_pass:
                base = x_in[c_rows:, at].astype(F32)
                out[:, at] = (base + gate[:, at] * total).astype(BF16)
            else:
                acc[:, at] = total

    for c in sends[:n_early]:
        c.wait_send()
    for condition, c in sends_when:
        pl.when(condition)(c.wait_send)
    for index, block_all in enumerate((k_all, v_all)):
        down, up = halo_copies(index, block_all)

        @pl.when(slab > 0)
        def _():
            down.wait_send()

        @pl.when(slab < last_slab)
        def _():
            up.wait_send()
    pass_on(1, 5, me_t, 1 - side)
    pass_on(0, 4, far, 1 - side)
    project((me_t,), True, False)
    pass_on(2, 6, far, side)
    odd = core == 1
    @pl.when(odd)
    def _():
        project((far,), False, False)

    remote(
        w_out.at[partner], w_out.at[partner], wo_send.at[4, 0], wo_recv.at[4, 0], me_s, partner
    ).wait_recv()
    arrived(3, partner, side).wait_recv()
    arrived(5, partner, 1 - side).wait_recv()
    @pl.when(odd)
    def _():
        project((partner,), False, False)

    wo_finish_far()
    arrived(4, far_partner, 1 - side).wait_recv()
    arrived(6, far_partner, side).wait_recv()
    @pl.when(odd)
    def _():
        project((far_partner,), False, True)

    @pl.when(jnp.logical_not(odd))
    def _():
        project((far, partner, far_partner), False, True)

    for c in sends[n_early:]:
        c.wait_send()


def per_device(
    latent,
    context,
    condition,
    ctx_condition,
    shift_weight,
    scale_weight,
    gate_weight,
    norm_gain,
    query_weight,
    key_weight,
    value_weight,
    query_gain,
    key_gain,
    offset_bias,
    out_weight,
):
    n_sp, n_tp = lax.axis_size("sp"), lax.axis_size("tp")
    rows, d = latent.shape
    c_rows = context.shape[0]
    width = key_weight.shape[1]
    heads = width // HEAD_DIM
    block = shift_weight.shape[1]
    n_pairs = 2 * WIN_ROWS - 2
    half = width // 2
    half_heads = heads // 2
    blocks = block // 128
    l_rows = rows // GRID_W
    stack = half_heads * GRID_W
    any_spec = pl.BlockSpec(memory_space=pl.ANY)
    vmem_spec = pl.BlockSpec(memory_space=pltpu.VMEM)
    dma = pltpu.SemaphoreType.DMA
    return pl.pallas_call(
        functools.partial(fused_kernel, n_sp, n_tp),
        out_shape=pltpu.VMEM((rows, d), BF16),
        in_specs=[any_spec] * 15,
        out_specs=vmem_spec,
        scratch_shapes=[
            pltpu.VMEM((1, condition.shape[0]), F32),
            pltpu.VMEM((1, condition.shape[0]), F32),
            pltpu.VMEM((1, d), F32),
            pltpu.VMEM((1, HEAD_DIM), F32),
            pltpu.VMEM((1, HEAD_DIM), F32),
            pltpu.VMEM((2 * WIN_ROWS - 1, heads, 2 * WIN_COLS - 1), F32),
            pltpu.VMEM((rows + c_rows, d), BF16),
            pltpu.VMEM((rows + c_rows, d), F32),
            pltpu.VMEM((rows + c_rows, d), BF16),
            pltpu.VMEM((3, shift_weight.shape[0], block), BF16),
            pltpu.VMEM((d, 3 * width), BF16),
            pltpu.VMEM((n_tp, width, d), BF16),
            pltpu.VMEM((n_sp, 4 * blocks, 128), F32),
            pltpu.VMEM((n_tp, 4 * blocks, 128), F32),
            pltpu.VMEM((rows + c_rows, 2 * width), F32),
            pltpu.VMEM((rows, width), F32),
            pltpu.VMEM((n_sp, blocks, 128), F32),
            pltpu.VMEM((n_tp, blocks, 128), F32),
            pltpu.VMEM((rows, d), F32),
            pltpu.VMEM((2, rows, half), BF16),
            pltpu.VMEM((2, rows, half), BF16),
            pltpu.VMEM((2, rows, half), BF16),
            pltpu.VMEM((2, c_rows, half), BF16),
            pltpu.VMEM((2, c_rows, half), BF16),
            pltpu.VMEM((2 * rows, half), BF16),
            pltpu.VMEM((4 * rows, half), BF16),
            pltpu.VMEM((4 * rows, half), BF16),
            pltpu.VMEM((n_sp, c_rows, half), BF16),
            pltpu.VMEM((n_sp, c_rows, half), BF16),
            pltpu.VMEM((heads, 2 * WIN_ROWS, 2 * GRID_W), F32),
            pltpu.VMEM((half_heads, 2 * WIN_ROWS, 2 * GRID_W), F32),
            pltpu.VMEM((n_pairs, half_heads * GRID_W, 2 * GRID_W), F32),
            pltpu.VMEM((2 * l_rows, stack, half), BF16),
            pltpu.VMEM((2, stack, WIN_ROWS * GRID_W), F32),
            pltpu.VMEM((2 * l_rows, stack, 128), F32),
            pltpu.VMEM((2 * l_rows, stack, half + 128), F32),
            pltpu.VMEM((l_rows * stack, n_sp * c_rows), F32),
            pltpu.VMEM((l_rows * stack, n_sp * c_rows), BF16),
            pltpu.VMEM((l_rows * stack, half + 128), F32),
            pltpu.VMEM((rows, half), BF16),
            pltpu.VMEM((n_tp, 2, rows, half), BF16),
            dma((15,)),
            dma((n_sp,)),
            dma((n_sp,)),
            dma((n_tp,)),
            dma((n_tp,)),
            dma((n_sp,)),
            dma((n_sp,)),
            dma((n_tp,)),
            dma((n_tp,)),
            dma((4,)),
            dma((4,)),
            dma((2, 2)),
            dma((2, 2)),
            dma((2, n_sp)),
            dma((2, n_sp)),
            dma((2, n_sp)),
            dma((5, 16)),
            dma((5, 16)),
            dma((7,)),
            dma((7,)),
        ],
        compiler_params=pltpu.CompilerParams(collective_id=0, has_side_effects=True),
        name="fused_block",
    )(
        latent,
        context,
        shift_weight,
        scale_weight,
        gate_weight,
        query_weight,
        key_weight,
        value_weight,
        out_weight,
        condition.reshape(1, -1),
        ctx_condition.reshape(1, -1),
        norm_gain.reshape(1, -1),
        query_gain.reshape(1, -1),
        key_gain.reshape(1, -1),
        offset_bias.transpose(1, 0, 2),
    )


def fused_fits(latent, context, condition, query_weight, n_sp, n_tp):
    rows, c_rows = latent.shape[0] // n_sp, context.shape[0] // n_sp
    width = query_weight.shape[1] // n_tp
    return (
        rows == WIN_ROWS // 2 * GRID_W
        and c_rows % 32 == 0
        and condition.shape[0] // n_sp % 128 == 0
        and condition.shape[0] // n_tp % 256 == 0
        and condition.shape[0] // n_tp <= 1024
        and width == 2 * LANES
        and n_tp == 4
        and n_sp == 8
    )


def solution(mesh):
    in_specs = (
        P("sp", None),
        P("sp", None),
        P("sp"),
        P("sp"),
        P("sp", "tp"),
        P("sp", "tp"),
        P("sp", "tp"),
        P(),
        P(None, "tp"),
        P(None, "tp"),
        P(None, "tp"),
        P(),
        P(),
        P("tp", None, None),
        P("tp", None),
    )
    out_specs = P("sp", None)

    def step(latent, context, condition, ctx_condition, *rest):
        n_sp, n_tp = mesh.shape["sp"], mesh.shape["tp"]
        fits = fused_fits(latent, context, condition, rest[4], n_sp, n_tp)
        body = per_device if fits else per_device_plain
        return jax.shard_map(
            body, mesh=mesh, in_specs=in_specs, out_specs=out_specs, check_vma=False
        )(latent, context, condition, ctx_condition, *rest)

    return step
```
